256 devices in a mesh: tp: 32 (over z, y), dp: 8 (over x, core).
Axes of the slice: x: 4, y: 4, z: 8, core: 2. Of those that a mesh axis runs over, the one named last changes fastest.
Arguments:
- stream: bfloat16 [256, 2048], P('tp', 'dp'), may hold values from -12 to 12
- norm_gain: float32 [2, 2048], P(None, 'dp'), may hold values from 0.1 to 1.9
- w_input: bfloat16 [2, 2048, 2048], P(None, 'dp', 'tp'), may hold values from -0.125 to 0.125
- lam_re: float32 [2, 128, 64], P(None, 'tp'), may hold values from -1 to -0.05
- lam_im: float32 [2, 128, 64], P(None, 'tp'), may hold values from 0 to 6
- log_dt: float32 [2, 128], P(None, 'tp'), may hold values from -3 to 0
- b_re: float32 [2, 128, 64, 16], P(None, 'tp'), may hold values from -1 to 1
- b_im: float32 [2, 128, 64, 16], P(None, 'tp'), may hold values from -1 to 1
- readout_real: float32 [2, 128, 16, 64], P(None, 'tp'), may hold values from -0.5 to 0.5
- readout_imaginary: float32 [2, 128, 16, 64], P(None, 'tp'), may hold values from -0.5 to 0.5
- d_skip: float32 [2, 2048], P(None, 'tp'), may hold values from -4 to 4
- w_val: bfloat16 [2, 2048, 2048], P(None, 'tp', 'dp'), may hold values from -0.375 to 0.375
- w_gate: bfloat16 [2, 2048, 2048], P(None, 'tp', 'dp'), may hold values from -0.375 to 0.375
- state: float32 [2, 256, 128, 128], P(None, 'dp', 'tp'), may hold values from -6 to 6
Outputs:
- stream_out: bfloat16 [256, 2048], P('tp', 'dp')
- states_out: float32 [2, 256, 128, 128], P(None, 'dp', 'tp')
The draws below stay inside these ranges and needn't reach their ends.
All inputs are finite; a program needn't handle non-finite values.
Results may differ from the reference program's by a relative error of at most 0.0064.
Values may be sent and summed in bfloat16 or wider, within the bound.
A program may use at most 64 MiB of HBM per device.

```python
import jax
import jax.numpy as jnp
from jax import lax

D = 2048
CH = 16
STATE = 64
GROUPS = 128
LAYERS = 2
SEQS = 256


def draw_stream(key, part):
    subkeys = jax.random.split(key, 2)
    base_draw = jax.random.normal(subkeys[0], (SEQS, D), jnp.float32)
    block_scale = jnp.exp(jax.random.uniform(subkeys[1], (SEQS, 8), jnp.float32, -1.2, 1.2))
    full_draw = base_draw * jnp.repeat(block_scale, D // 8, axis=1)
    return jnp.clip(full_draw, -12.0, 12.0).astype(jnp.bfloat16)


def level_of(rng, extent, cuts, low, largest):
    loudness, own = 1.0, jax.random.fold_in(rng, 6)
    for dim, shards_of in cuts:
        heights = jnp.exp(jax.random.uniform(jax.random.fold_in(own, dim), (shards_of,), jnp.float32, low / len(cuts), largest / len(cuts)))
        loudness = loudness * jnp.repeat(heights, extent[dim] // shards_of).reshape([-1 if axis == dim else 1 for axis in range(len(extent))])
    return loudness


def bell_draw(rng, shape, scale, limit, cuts=(), held_as=jnp.bfloat16):
    result = scale * jax.random.normal(rng, shape, jnp.float32)
    if cuts:
        result = result * level_of(rng, shape, cuts, -0.22, 0.18)
    return jnp.clip(result, -limit, limit).astype(held_as)


def setup_inputs(seed: int = 0) -> dict:
    keys = jax.random.split(jax.random.key(seed), 15)
    stream = draw_stream(jax.random.fold_in(keys[14], 71), 0)
    norm_gain = jnp.clip(1.0 + 0.18 * jax.random.normal(keys[1], (LAYERS, D), jnp.float32), 0.1, 1.9)
    w_input = bell_draw(keys[2], (LAYERS, D, D), D ** -0.5, 0.125, ((1, 8), (2, 32)))
    lam_re = jnp.clip(-1.0 + 0.95 * jax.random.uniform(keys[3], (LAYERS, GROUPS, STATE), jnp.float32) ** level_of(keys[3], (LAYERS, GROUPS, STATE), ((1, 32),), -0.2, 0.2), -1.0, -0.05)
    lam_im = jnp.clip(6.0 * jax.random.uniform(keys[4], (LAYERS, GROUPS, STATE), jnp.float32) ** level_of(keys[4], (LAYERS, GROUPS, STATE), ((1, 32),), -0.2, 0.2), 0.0, 6.0)
    log_dt = jnp.clip(-3.0 + 3.0 * jax.random.uniform(keys[5], (LAYERS, GROUPS), jnp.float32) ** level_of(keys[5], (LAYERS, GROUPS), ((1, 32),), -0.2, 0.2), -3.0, 0.0)
    b_re = bell_draw(keys[6], (LAYERS, GROUPS, STATE, CH), (2 * CH) ** -0.5, 1.0, ((1, 32),), jnp.float32)
    b_im = bell_draw(keys[7], (LAYERS, GROUPS, STATE, CH), (2 * CH) ** -0.5, 1.0, ((1, 32),), jnp.float32)
    readout_real = bell_draw(keys[8], (LAYERS, GROUPS, CH, STATE), (2 * STATE) ** -0.5, 0.5, ((1, 32),), jnp.float32)
    readout_imaginary = bell_draw(keys[9], (LAYERS, GROUPS, CH, STATE), (2 * STATE) ** -0.5, 0.5, ((1, 32),), jnp.float32)
    d_skip = bell_draw(keys[10], (LAYERS, D), 1.0, 4.0, ((1, 32),), jnp.float32)
    w_val = bell_draw(keys[11], (LAYERS, D, D), (D // 8) ** -0.5, 0.375, ((1, 32), (2, 8)))
    w_gate = bell_draw(keys[12], (LAYERS, D, D), (D // 8) ** -0.5, 0.375, ((1, 32), (2, 8)))
    state = bell_draw(keys[13], (LAYERS, SEQS, GROUPS, 2 * STATE), 1.0, 6.0, ((1, 8), (2, 32)), jnp.float32)
    return {"stream": stream, "norm_gain": norm_gain, "w_input": w_input, "lam_re": lam_re, "lam_im": lam_im, "log_dt": log_dt, "b_re": b_re, "b_im": b_im, "readout_real": readout_real, "readout_imaginary": readout_imaginary, "d_skip": d_skip, "w_val": w_val, "w_gate": w_gate, "state": state}


eps = 1e-06

def advance(inputs, old_state, lam_re, lam_im, log_dt, b_re, b_im, readout_real, readout_imaginary, d_skip):
    upper_bound = lax.Precision.HIGHEST
    count_rows, groups, doubled = old_state.shape
    half_state = doubled // 2
    chans = b_re.shape[-1]
    step_size = jnp.exp(log_dt)[:, None]
    decay = jnp.exp(lam_re * step_size)
    angle = lam_im * step_size
    keep_re = decay * jnp.cos(angle)
    keep_im = decay * jnp.sin(angle)
    denom = lam_re * lam_re + lam_im * lam_im
    ratio_re = ((keep_re - 1.0) * lam_re + keep_im * lam_im) / denom
    ratio_im = (keep_im * lam_re - (keep_re - 1.0) * lam_im) / denom
    drive_re = ratio_re[..., None] * b_re - ratio_im[..., None] * b_im
    drive_im = ratio_re[..., None] * b_im + ratio_im[..., None] * b_re
    grouped = inputs.reshape(count_rows, groups, chans)
    push_re = jnp.einsum('gpc,rgc->rgp', drive_re, grouped, precision=upper_bound)
    push_im = jnp.einsum('gpc,rgc->rgp', drive_im, grouped, precision=upper_bound)
    old_re = old_state[..., :half_state]
    old_im = old_state[..., half_state:]
    updated_real = keep_re * old_re - keep_im * old_im + push_re
    updated_imaginary = keep_re * old_im + keep_im * old_re + push_im
    readout_output = jnp.einsum('aot,mat->mao', readout_real, updated_real, precision=upper_bound) - jnp.einsum('aot,mat->mao', readout_imaginary, updated_imaginary, precision=upper_bound)
    pre_act = readout_output.reshape(count_rows, groups * chans) + d_skip * inputs
    return (pre_act, jnp.concatenate([updated_real, updated_imaginary], axis=-1))

def reference(stream, norm_gain, w_input, lam_re, lam_im, log_dt, b_re, b_im, readout_real, readout_imaginary, d_skip, w_val, w_gate, state):
    collected = []
    for layer_no in range(LAYERS):
        widened = stream.astype(jnp.float32)
        factor = lax.rsqrt(lax.optimization_barrier(jnp.mean(widened * widened, axis=1)) + eps)
        normed = (widened * norm_gain[layer_no]).astype(jnp.bfloat16)
        inputs = factor[:, None] * jnp.dot(normed, w_input[layer_no], preferred_element_type=jnp.float32)
        pre_act, new_state = advance(inputs, state[layer_no], lam_re[layer_no], lam_im[layer_no], log_dt[layer_no], b_re[layer_no], b_im[layer_no], readout_real[layer_no], readout_imaginary[layer_no], d_skip[layer_no])
        mixed = jax.nn.gelu(pre_act).astype(jnp.bfloat16)
        value = jnp.dot(mixed, w_val[layer_no], preferred_element_type=jnp.float32)
        gate = jnp.dot(mixed, w_gate[layer_no], preferred_element_type=jnp.float32)
        stream = (widened + value * jax.nn.sigmoid(gate)).astype(jnp.bfloat16)
        collected.append(new_state)
    return (stream, jnp.stack(collected))
```

```python
import functools

import jax
import jax.numpy as jnp
from jax import lax
from jax.experimental import pallas as pl
from jax.experimental.pallas import tpu as pltpu
from jax.sharding import PartitionSpec as P

EPS = 1e-06
F32 = jnp.float32
BF16 = jnp.bfloat16
HIGHEST = lax.Precision.HIGHEST
NT = (((1,), (1,)), ((), ()))
PLANE_FAR_FIRST = (4, 5, 6, 7, 2, 3, 1, 0)
ROW_FAR_FIRST = (2, 1, 3, 0)


def partner(me, k, n, back=False):
    if n & (n - 1):
        return (me + (n - k if back else k)) % n
    found, bit = 0, 1
    while bit < n:
        mine = (me // bit) % 2
        found = found + (bit * (1 - mine) if k & bit else bit * mine)
        bit *= 2
    return found


def kernel(
    tp, dp, chans,
    stream_ref, gain_ref, w_in_hbm, lam_re_ref, lam_im_ref, log_dt_ref, b_re_hbm, b_im_hbm, c_re_hbm, c_im_hbm, skip_ref,
    w_val_hbm, w_gate_hbm, state_hbm,
    out_ref, state,
    w_in, w_val, w_gate, b_re, b_im, c_re, c_im, drive, read,
    kept, proj, u_keep, masked, from_old, mix_w,
    x_all, part_send, part_recv, sq_send, sq_recv, mix_all, comb_send, comb_own, comb_recv,
    gain_all, far_in, far_val, far_gate, x_far, swap_send, swap_recv, u_send, u_recv, out_send, out_recv,
    load_sem, x_ss, x_rs, part_ss, part_rs, sq_ss, sq_rs, mix_ss, mix_rs, comb_ss, comb_rs,
    gain_ss, gain_rs, far_ss, far_rs, xf_ss, xf_rs, swap_ss, swap_rs, u_ss, u_rs, of_ss, of_rs,
):
    layers = w_in.shape[0]
    me_t, me_d = lax.axis_index("tp"), lax.axis_index("dp")
    rows_t, feats = stream_ref.shape
    rows_d, width = u_keep.shape
    per = rows_d // rows_t
    groups, half = lam_re_ref.shape[1:]
    lanes = state.shape[2]
    sq_width = sq_send.shape[2]
    me_z, me_y = me_t // per, me_t % per

    loads = {}
    for l in range(layers):
        for i, (src, dst) in enumerate(
            (
                (b_re_hbm, b_re), (b_im_hbm, b_im), (c_re_hbm, c_re), (c_im_hbm, c_im), (state_hbm, state),
                (w_in_hbm, w_in), (w_val_hbm, w_val), (w_gate_hbm, w_gate),
            )
        ):
            loads[l, i] = pltpu.make_async_copy(src.at[l], dst.at[l], load_sem.at[l, i])
            loads[l, i].start()

    barrier = pltpu.get_barrier_semaphore()

    def greet(t, d):
        pl.semaphore_signal(barrier, inc=1, device_id={"tp": t, "dp": d}, device_id_type=pl.DeviceIdType.MESH)

    for k in range(1, dp):
        greet(me_t, partner(me_d, k, dp))
    for k in range(1, tp):
        greet(partner(me_t, k, tp), me_d)
    for j in range(1, per):
        for k in range(1, dp):
            greet(me_z * per + partner(me_y, j, per), partner(me_d, k, dp))
    for k in range(dp):

        @pl.when(jnp.logical_or(me_z != me_d, k != me_d))
        def _():
            greet(me_d * per + me_y, k)

    def send(src, dst, ss, rs, t, d):
        return pltpu.make_async_remote_copy(
            src_ref=src, dst_ref=dst, send_sem=ss, recv_sem=rs, device_id={"tp": t, "dp": d},
            device_id_type=pl.DeviceIdType.MESH,
        )

    def x_copy(k):
        to = partner(me_t, k, tp)
        return send(stream_ref, x_all.at[me_t], x_ss.at[to], x_rs.at[me_t], to, me_d)

    def part_copy(to):
        return send(part_send.at[to], part_recv.at[me_d], part_ss.at[to], part_rs.at[me_d], me_t, to)

    def sq_copy(to):
        return send(sq_send.at[to], sq_recv.at[me_d], sq_ss.at[to], sq_rs.at[me_d], me_t, to)

    def mix_copy(to):
        return send(mix_all.at[me_d], mix_all.at[me_d], mix_ss.at[to], mix_rs.at[me_d], me_t, to)

    def comb_copy(to):
        return send(comb_send.at[to], comb_recv.at[me_t], comb_ss.at[to], comb_rs.at[me_t], to, me_d)

    def gain_copy(to):
        return send(gain_all.at[me_d], gain_all.at[me_d], gain_ss.at[to], gain_rs.at[me_d], me_t, to)

    far = ((w_in, far_in), (w_val, far_val), (w_gate, far_gate))

    def far_copy(i, z):
        return send(far[i][0].at[1], far[i][1].at[me_d], far_ss.at[i, z], far_rs.at[i, me_d], z * per + me_y, me_z)

    def xf_copy(y, d):
        return send(x_far.at[me_d, me_y], x_far.at[me_d, me_y], xf_ss.at[d, y], xf_rs.at[me_d, me_y], me_z * per + y, d)

    def of_copy(y, d):
        return send(out_send.at[d, y], out_recv.at[me_d, me_y], of_ss.at[d, y], of_rs.at[me_d, me_y], me_z * per + y, d)

    def swap_copy():
        return send(swap_send, swap_recv, swap_ss, swap_rs, me_d * per + me_y, me_z)

    def u_copy():
        return send(u_send, u_recv, u_ss, u_rs, me_d * per + me_y, me_z)

    def arrival(ref, rs):
        return send(ref, ref, rs, rs, 0, 0)

    def spread(i):
        loads[1, 5 + i].wait()
        for k in reversed(range(dp)):
            z = partner(me_z, k, dp)

            @pl.when(jnp.logical_or(z != me_z, me_z != me_d))
            def _():
                far_copy(i, z).start()

        @pl.when(me_z == me_d)
        def _():
            far[i][1][me_d] = far[i][0][1]

    def spread_wait(i, d):
        @pl.when(jnp.logical_or(d != me_d, me_z != me_d))
        def _():
            arrival(far[i][1].at[d], far_rs.at[i, d]).wait_recv()

    lane_group = lax.broadcasted_iota(jnp.int32, (rows_d, width), 1) // chans
    eye = lax.broadcasted_iota(jnp.int32, (rows_d, sq_width), 0) == lax.broadcasted_iota(jnp.int32, (rows_d, sq_width), 1)
    group_eye = lax.broadcasted_iota(jnp.int32, (groups, groups), 0) == lax.broadcasted_iota(jnp.int32, (groups, groups), 1)
    wide_0 = lax.broadcasted_iota(jnp.int32, (width, width), 0)
    wide_1 = lax.broadcasted_iota(jnp.int32, (width, width), 1)

    def prepare(l):
        step_size = jnp.exp(jnp.sum(jnp.where(group_eye, log_dt_ref[l : l + 1, :], 0.0), axis=1, keepdims=True))
        lam_re, lam_im = lam_re_ref[l], lam_im_ref[l]
        decay = jnp.exp(lam_re * step_size)
        angle = lam_im * step_size
        keep_re = decay * jnp.cos(angle)
        keep_im = decay * jnp.sin(angle)
        denom = lam_re * lam_re + lam_im * lam_im
        ratio_re = ((keep_re - 1.0) * lam_re + keep_im * lam_im) / denom
        ratio_im = (keep_im * lam_re - (keep_re - 1.0) * lam_im) / denom
        keep_a = jnp.concatenate([keep_re, keep_re], axis=1)
        keep_b = jnp.concatenate([-keep_im, keep_im], axis=1)
        for i in range(5):
            loads[l, i].wait()
        for g in range(groups):
            t_re, t_im = b_re[l, g], b_im[l, g]
            r_re, r_im = ratio_re[g : g + 1, :], ratio_im[g : g + 1, :]
            drive[l, pl.ds(g * chans, chans), :] = jnp.concatenate(
                [r_re * t_re - r_im * t_im, r_re * t_im + r_im * t_re], axis=1
            )
        read[l] = jnp.concatenate([c_re[l].reshape(width, half), -c_im[l].reshape(width, half)], axis=1)
        for g in range(groups):
            old = state[l, pl.ds(g, rows_d, stride=groups), :]
            kept[l, pl.ds(g * rows_d, rows_d), :] = (
                keep_a[g : g + 1, :] * old + keep_b[g : g + 1, :] * pltpu.roll(old, lanes // 2, 1)
            )
        proj[...] = lax.dot_general(kept[l], read[l], NT, precision=HIGHEST, preferred_element_type=F32)
        total = jnp.zeros((rows_d, width), F32)
        for g in range(groups):
            total = jnp.where(lane_group == g, proj[pl.ds(g * rows_d, rows_d), :], total)
        full = lax.dot_general(drive[l], read[l], NT, precision=HIGHEST, preferred_element_type=F32)
        mixer = jnp.where(wide_0 // chans == wide_1 // chans, full, 0.0)
        mixer = mixer + jnp.where(wide_0 == wide_1, skip_ref[l : l + 1, :], 0.0)
        return total, mixer

    def update(l, u):
        for g in range(groups):
            masked[pl.ds(g * rows_d, rows_d), :] = jnp.where(lane_group == g, u, 0.0)
        kept[l] = kept[l] + jnp.dot(masked[...], drive[l], precision=HIGHEST, preferred_element_type=F32)
        for g in range(groups):
            state[l, pl.ds(g, rows_d, stride=groups), :] = kept[l, pl.ds(g * rows_d, rows_d), :]

    elsewhere = ((me_z - me_d) * (me_z - me_d) + dp * dp - 1) // (dp * dp)
    pl.semaphore_wait(barrier, tp - 1 + dp - 1 + (per - 1) * (dp - 1) + dp - 1 + elsewhere)

    for k in reversed(range(1, tp)):
        x_copy(k).start()
    gain_all[me_d] = jnp.broadcast_to(gain_ref[1:2, :], (rows_t, feats))
    for k in reversed(range(1, dp)):
        gain_copy(partner(me_d, k, dp)).start()
    spread(0)
    x_all[me_t] = stream_ref[...]
    from_old[...], mix_w[...] = prepare(0)

    loads[0, 5].wait()
    gain = gain_ref[0:1, :]
    own_part = own_sq = None
    for k in reversed(range(dp)):
        to = partner(me_d, k, dp)
        for j in range(per):
            t = to * per + j

            @pl.when(t != me_t)
            def _():
                arrival(x_all.at[t], x_rs.at[t]).wait_recv()

        x = x_all[pl.ds(to * per, per)].astype(F32).reshape(rows_d, feats)
        column = jnp.sum(x * x, axis=1, keepdims=True)
        squares = jnp.sum(jnp.where(eye, column, 0.0), axis=0, keepdims=True)
        product = lax.dot_general((x * gain).astype(BF16), w_in[0], NT, preferred_element_type=F32)
        if k:
            sq_send[to] = jnp.broadcast_to(squares, (8, sq_width))
            sq_copy(to).start()
            part_send[to] = product.astype(BF16)
            part_copy(to).start()
        else:
            own_part, own_sq = product, squares
    spread(1)
    for k in range(1, dp):
        by = partner(me_d, k, dp, True)
        arrival(sq_recv.at[by], sq_rs.at[by]).wait_recv()
        own_sq = own_sq + sq_recv[by][0:1, :]
        arrival(part_recv.at[by], part_rs.at[by]).wait_recv()
        own_part = own_part + part_recv[by].astype(F32)
    square_total = jnp.sum(jnp.where(eye, own_sq, 0.0), axis=1, keepdims=True)
    u = lax.rsqrt(square_total / (feats * dp) + EPS) * own_part
    u_keep[...] = u
    pre = from_old[...] + jnp.dot(u, mix_w[...], precision=HIGHEST, preferred_element_type=F32)
    mix_all[me_d] = jax.nn.gelu(pre).astype(BF16)
    for k in reversed(range(1, dp)):
        mix_copy(partner(me_d, k, dp)).start()
    loads[0, 6].wait()
    loads[0, 7].wait()
    for k in range(dp):
        by = partner(me_d, k, dp, True)
        if k:
            arrival(mix_all.at[by], mix_rs.at[by]).wait_recv()
        mixed = mix_all[by]
        value = jnp.dot(mixed, w_val[0], preferred_element_type=F32)
        gate = jnp.dot(mixed, w_gate[0], preferred_element_type=F32)
        for j in range(per):
            t = by * per + j
            rows = slice(j * rows_t, (j + 1) * rows_t)

            @pl.when(t != me_t)
            def _():
                comb_send[t, :, :feats] = value[rows].astype(BF16)
                comb_send[t, :, feats:] = gate[rows].astype(BF16)
                comb_copy(t).start()

            @pl.when(t == me_t)
            def _():
                comb_own[:, :feats] = value[rows]
                comb_own[:, feats:] = gate[rows]

    spread(2)
    update(0, u_keep[...])
    total, mixer = prepare(1)
    swap_send[:rows_d] = jnp.concatenate([total, total], axis=1)
    swap_send[rows_d:] = jnp.concatenate([mixer, mixer], axis=1)

    @pl.when(me_z != me_d)
    def _():
        swap_copy().start()

    @pl.when(me_z == me_d)
    def _():
        swap_recv[...] = swap_send[...]

    combined = comb_own[...]
    for k in range(1, tp):
        by = partner(me_t, k, tp, True)
        arrival(comb_recv.at[by], comb_rs.at[by]).wait_recv()
        combined = combined + comb_recv[by].astype(F32)
    fresh = (x_all[me_t].astype(F32) + combined[:, :feats] * jax.nn.sigmoid(combined[:, feats:])).astype(BF16)

    x_far[me_d, me_y] = fresh
    for k in PLANE_FAR_FIRST:
        for j in ROW_FAR_FIRST:
            if k or j:
                xf_copy(partner(me_y, j, per), partner(me_d, k, dp)).start()
    for k in range(1, dp):
        by = partner(me_d, k, dp, True)
        arrival(gain_all.at[by], gain_rs.at[by]).wait_recv()

    acc = jnp.zeros((rows_d, width), F32)
    squares = jnp.zeros((rows_d, feats), F32)
    for k in reversed(PLANE_FAR_FIRST):
        by = partner(me_d, k, dp, True)
        spread_wait(0, by)
        for j in reversed(ROW_FAR_FIRST):
            if k or j:
                y = partner(me_y, j, per)
                arrival(x_far.at[by, y], xf_rs.at[by, y]).wait_recv()
        x = x_far[by].astype(F32)
        normed = (x * gain_all[by][None]).astype(BF16).reshape(rows_d, feats)
        x = x.reshape(rows_d, feats)
        squares = squares + x * x
        acc = acc + lax.dot_general(normed, far_in[by], NT, preferred_element_type=F32)
    u = lax.rsqrt(jnp.sum(squares, axis=1, keepdims=True) / (feats * dp) + EPS) * acc
    u_send[...] = jnp.concatenate([u, u], axis=1)

    @pl.when(me_z != me_d)
    def _():
        u_copy().start()
        arrival(swap_recv, swap_rs).wait_recv()

    @pl.when(me_z == me_d)
    def _():
        u_recv[...] = u_send[...]

    pre = swap_recv[:rows_d, :width] + jnp.dot(
        u, swap_recv[rows_d:, :width], precision=HIGHEST, preferred_element_type=F32
    )
    mixed = jax.nn.gelu(pre).astype(BF16)
    for k in PLANE_FAR_FIRST:
        to = partner(me_d, k, dp)
        spread_wait(1, to)
        spread_wait(2, to)
        value = jnp.dot(mixed, far_val[to], preferred_element_type=F32)
        gate = jnp.dot(mixed, far_gate[to], preferred_element_type=F32)
        out_send[to, :, :, :feats] = value.astype(BF16).reshape(per, rows_t, feats)
        out_send[to, :, :, feats:] = gate.astype(BF16).reshape(per, rows_t, feats)
        for j in ROW_FAR_FIRST:
            if k or j:
                of_copy(partner(me_y, j, per), to).start()
    combined = out_send[me_d, me_y].astype(F32)

    @pl.when(me_z != me_d)
    def _():
        arrival(u_recv, u_rs).wait_recv()

    update(1, u_recv[:, :width])
    for k in reversed(PLANE_FAR_FIRST):
        by = partner(me_d, k, dp, True)
        for j in reversed(ROW_FAR_FIRST):
            if k or j:
                y = partner(me_y, j, per)
                arrival(out_recv.at[by, y], of_rs.at[by, y]).wait_recv()
                combined = combined + out_recv[by, y].astype(F32)
    out_ref[...] = (
        x_far[me_d, me_y].astype(F32) + combined[:, :feats] * jax.nn.sigmoid(combined[:, feats:])
    ).astype(BF16)

    for k in range(1, tp):
        x_copy(k).wait_send()
        comb_copy(partner(me_t, k, tp)).wait_send()
    for k in range(1, dp):
        to = partner(me_d, k, dp)
        part_copy(to).wait_send()
        sq_copy(to).wait_send()
        mix_copy(to).wait_send()
        gain_copy(to).wait_send()
    for k in range(dp):
        z = partner(me_z, k, dp)

        @pl.when(jnp.logical_or(z != me_z, me_z != me_d))
        def _():
            for i in range(3):
                far_copy(i, z).wait_send()

    for k in range(dp):
        for j in range(per):
            if k or j:
                xf_copy(partner(me_y, j, per), partner(me_d, k, dp)).wait_send()
                of_copy(partner(me_y, j, per), partner(me_d, k, dp)).wait_send()

    @pl.when(me_z != me_d)
    def _():
        swap_copy().wait_send()
        u_copy().wait_send()


def per_device(
    tp, dp,
    stream, norm_gain, w_input, lam_re, lam_im, log_dt, b_re, b_im, readout_real, readout_imaginary, d_skip,
    w_val, w_gate, state,
):
    layers, feats, width = w_input.shape
    rows_t = stream.shape[0]
    rows_d, groups, lanes = state.shape[1:]
    chans = b_re.shape[-1]
    per = rows_d // rows_t

    turned_in = w_input.swapaxes(1, 2)
    turned_re, turned_im = b_re.swapaxes(2, 3), b_im.swapaxes(2, 3)

    limit = 67043328 - 4 * layers * rows_d * groups * lanes - (256 << 10)
    vmem = pl.BlockSpec(memory_space=pltpu.VMEM)
    hbm = pl.BlockSpec(memory_space=pltpu.HBM)
    sq_width = max(rows_d, 128)
    dma = lambda *shape: pltpu.SemaphoreType.DMA(shape)
    out, states = pl.pallas_call(
        functools.partial(kernel, tp, dp, chans),
        out_shape=(pltpu.VMEM(stream.shape, BF16), pltpu.VMEM((layers, rows_d * groups, lanes), F32)),
        in_specs=[vmem, vmem, hbm, vmem, vmem, vmem, hbm, hbm, hbm, hbm, vmem, hbm, hbm, hbm],
        out_specs=(vmem, vmem),
        scratch_shapes=[
            pltpu.VMEM(turned_in.shape, BF16),
            pltpu.VMEM(w_val.shape, BF16),
            pltpu.VMEM(w_gate.shape, BF16),
            pltpu.VMEM(turned_re.shape, F32),
            pltpu.VMEM(turned_im.shape, F32),
            pltpu.VMEM(readout_real.shape, F32),
            pltpu.VMEM(readout_imaginary.shape, F32),
            pltpu.VMEM((layers, width, lanes), F32),
            pltpu.VMEM((layers, width, lanes), F32),
            pltpu.VMEM((layers, rows_d * groups, lanes), F32),
            pltpu.VMEM((rows_d * groups, width), F32),
            pltpu.VMEM((rows_d, width), F32),
            pltpu.VMEM((rows_d * groups, width), F32),
            pltpu.VMEM((rows_d, width), F32),
            pltpu.VMEM((width, width), F32),
            pltpu.VMEM((tp, rows_t, feats), BF16),
            pltpu.VMEM((dp, rows_d, width), BF16),
            pltpu.VMEM((dp, rows_d, width), BF16),
            pltpu.VMEM((dp, 8, sq_width), F32),
            pltpu.VMEM((dp, 8, sq_width), F32),
            pltpu.VMEM((dp, rows_d, width), BF16),
            pltpu.VMEM((tp, rows_t, 2 * feats), BF16),
            pltpu.VMEM((rows_t, 2 * feats), F32),
            pltpu.VMEM((tp, rows_t, 2 * feats), BF16),
            pltpu.VMEM((dp, rows_t, feats), F32),
            pltpu.VMEM((dp, width, feats), BF16),
            pltpu.VMEM((dp, width, feats), BF16),
            pltpu.VMEM((dp, width, feats), BF16),
            pltpu.VMEM((dp, per, rows_t, feats), BF16),
            pltpu.VMEM((rows_d + width, 128), F32),
            pltpu.VMEM((rows_d + width, 128), F32),
            pltpu.VMEM((rows_d, 128), F32),
            pltpu.VMEM((rows_d, 128), F32),
            pltpu.VMEM((dp, per, rows_t, 2 * feats), BF16),
            pltpu.VMEM((dp, per, rows_t, 2 * feats), BF16),
            dma(layers, 8),
            dma(tp), dma(tp),
            dma(dp), dma(dp),
            dma(dp), dma(dp),
            dma(dp), dma(dp),
            dma(tp), dma(tp),
            dma(dp), dma(dp),
            dma(3, dp), dma(3, dp),
            dma(dp, per), dma(dp, per),
            pltpu.SemaphoreType.DMA, pltpu.SemaphoreType.DMA,
            pltpu.SemaphoreType.DMA, pltpu.SemaphoreType.DMA,
            dma(dp, per), dma(dp, per),
        ],
        compiler_params=pltpu.CompilerParams(collective_id=0, has_side_effects=True, vmem_limit_bytes=limit),
    )(
        stream, norm_gain, turned_in, lam_re, lam_im, log_dt, turned_re, turned_im, readout_real,
        readout_imaginary, d_skip, w_val, w_gate,
        state.reshape(layers, rows_d * groups, lanes),
    )
    return out, states.reshape(state.shape)


def solution(mesh):
    return jax.shard_map(
        functools.partial(per_device, mesh.shape["tp"], mesh.shape["dp"]),
        mesh=mesh,
        in_specs=(
            P("tp", "dp"),
            P(None, "dp"),
            P(None, "dp", "tp"),
            P(None, "tp", None),
            P(None, "tp", None),
            P(None, "tp"),
            P(None, "tp", None, None),
            P(None, "tp", None, None),
            P(None, "tp", None, None),
            P(None, "tp", None, None),
            P(None, "tp"),
            P(None, "tp", "dp"),
            P(None, "tp", "dp"),
            P(None, "dp", "tp", None),
        ),
        out_specs=(P("tp", "dp"), P(None, "dp", "tp", None)),
        check_vma=False,
    )
```

```python
import functools

import jax
import jax.numpy as jnp
from jax import lax
from jax.experimental import pallas as pl
from jax.experimental.pallas import tpu as pltpu
from jax.sharding import PartitionSpec as P

EPS = 1e-06
F32 = jnp.float32
BF16 = jnp.bfloat16
HIGHEST = lax.Precision.HIGHEST
NT = (((1,), (1,)), ((), ()))
PLANE_FAR_FIRST = (4, 5, 6, 7, 2, 3, 1, 0)
ROW_FAR_FIRST = (2, 1, 3, 0)


def partner(me, k, n, back=False):
    if n & (n - 1):
        return (me + (n - k if back else k)) % n
    found, bit = 0, 1
    while bit < n:
        mine = (me // bit) % 2
        found = found + (bit * (1 - mine) if k & bit else bit * mine)
        bit *= 2
    return found


def kernel(
    tp, dp, chans,
    stream_hbm, gain_hbm, w_in_hbm, lam_re_hbm, lam_im_hbm, log_dt_hbm, b_re_hbm, b_im_hbm, c_re_hbm, c_im_hbm, skip_hbm,
    w_val_hbm, w_gate_hbm, state_hbm,
    out_ref, state,
    stream_ref, gain_ref, lam_re_ref, lam_im_ref, log_dt_ref, skip_ref, own_w, b_re, b_im, c_re, c_im, drive, read,
    kept, proj, u_keep, masked, from_old, mix_w,
    x_all, part_send, part_recv, sq_send, sq_recv, mix_all, comb_send, comb_own, comb_recv,
    gain_all, col_w, far_w, x_far, swap_send, swap_recv, u_send, u_recv, out_send, out_recv,
    small_sem, load_sem, x_ss, x_rs, part_ss, part_rs, sq_ss, sq_rs, mix_ss, mix_rs, comb_ss, comb_rs,
    gain_ss, gain_rs, col_ss, col_rs, row_ss, row_rs, xf_ss, xf_rs, swap_ss, swap_rs, u_ss, u_rs, of_ss, of_rs,
):
    layers = w_in_hbm.shape[0]
    me_t, me_d = lax.axis_index("tp"), lax.axis_index("dp")
    rows_t, feats = stream_ref.shape
    rows_d, width = u_keep.shape
    per = rows_d // rows_t
    groups, half = lam_re_ref.shape[1:]
    lanes = state.shape[2]
    sq_width = sq_send.shape[2]
    me_z, me_y = me_t // per, me_t % per

    barrier = pltpu.get_barrier_semaphore()

    def greet(t, d):
        pl.semaphore_signal(barrier, inc=1, device_id={"tp": t, "dp": d}, device_id_type=pl.DeviceIdType.MESH)

    for k in range(1, dp):
        greet(me_t, partner(me_d, k, dp))
    for k in range(1, tp):
        greet(partner(me_t, k, tp), me_d)
    for j in range(1, per):
        for k in range(1, dp):
            greet(me_z * per + partner(me_y, j, per), partner(me_d, k, dp))

    @pl.when(me_z != me_d)
    def _():
        greet(me_d * per + me_y, me_z)

    smalls = []
    for i, (src, dst) in enumerate(
        (
            (stream_hbm, stream_ref), (gain_hbm, gain_ref), (lam_re_hbm, lam_re_ref), (lam_im_hbm, lam_im_ref),
            (log_dt_hbm, log_dt_ref), (skip_hbm, skip_ref),
        )
    ):
        smalls.append(pltpu.make_async_copy(src, dst, small_sem.at[i]))
        smalls[i].start()
    loads = {}
    for l in range(layers):
        weights = own_w if l == 0 else col_w.at[me_z]
        for i, (src, dst) in enumerate(
            (
                (b_re_hbm, b_re.at[l]), (b_im_hbm, b_im.at[l]), (c_re_hbm, c_re.at[l]), (c_im_hbm, c_im.at[l]),
                (state_hbm, state.at[l]), (w_in_hbm, weights.at[0]), (w_val_hbm, weights.at[1]),
                (w_gate_hbm, weights.at[2]),
            )
        ):
            loads[l, i] = pltpu.make_async_copy(src.at[l], dst, load_sem.at[l, i])
            loads[l, i].start()

    def send(src, dst, ss, rs, t, d):
        return pltpu.make_async_remote_copy(
            src_ref=src, dst_ref=dst, send_sem=ss, recv_sem=rs, device_id={"tp": t, "dp": d},
            device_id_type=pl.DeviceIdType.MESH,
        )

    def x_copy(k):
        to = partner(me_t, k, tp)
        return send(stream_ref, x_all.at[me_t], x_ss.at[to], x_rs.at[me_t], to, me_d)

    def part_copy(to):
        return send(part_send.at[to], part_recv.at[me_d], part_ss.at[to], part_rs.at[me_d], me_t, to)

    def sq_copy(to):
        return send(sq_send.at[to], sq_recv.at[me_d], sq_ss.at[to], sq_rs.at[me_d], me_t, to)

    def mix_copy(to):
        return send(mix_all.at[me_d], mix_all.at[me_d], mix_ss.at[to], mix_rs.at[me_d], me_t, to)

    def comb_copy(to):
        return send(comb_send.at[to], comb_recv.at[me_t], comb_ss.at[to], comb_rs.at[me_t], to, me_d)

    def gain_copy(to):
        return send(gain_all.at[me_d], gain_all.at[me_d], gain_ss.at[to], gain_rs.at[me_d], me_t, to)

    def col_copy(side, i):
        sign = 1 - 2 * side
        home = lax.rem(me_z - sign * min(i - 1, 2) + 2 * dp, dp)
        to = lax.rem(me_z + sign * (2 if i == 4 else 1) + dp, dp)
        part = col_w.at[home]
        if i == 4:
            part = part.at[:, pl.ds(side * (width // 2), width // 2)]
        return send(part, part, col_ss.at[side, i - 1], col_rs.at[side, i - 1], to * per + me_y, me_d)

    def col_wait(side, i):
        home = lax.rem(me_z - (1 - 2 * side) * i + 2 * dp, dp)
        part = col_w.at[home]
        if i == 4:
            part = part.at[:, pl.ds(side * (width // 2), width // 2)]
        arrival(part, col_rs.at[side, i - 1]).wait_recv()

    def row_copy(z, i):
        some = pl.ds(0, 1) if i == 0 else pl.ds(1, 2)
        return send(col_w.at[z, some], far_w.at[me_d, some], row_ss.at[i, z], row_rs.at[i, me_d], me_t, z)

    def row_wait(d, i):
        some = pl.ds(0, 1) if i == 0 else pl.ds(1, 2)
        arrival(far_w.at[d, some], row_rs.at[i, d]).wait_recv()

    def row_start(step):
        for i in range(2):
            z = lax.rem(me_z + step + dp, dp)

            @pl.when(z != me_d)
            def _():
                row_copy(z, i).start()

    def xf_copy(y, d):
        return send(x_far.at[me_d, me_y], x_far.at[me_d, me_y], xf_ss.at[d, y], xf_rs.at[me_d, me_y], me_z * per + y, d)

    def of_copy(y, d):
        return send(out_send.at[d, y], out_recv.at[me_d, me_y], of_ss.at[d, y], of_rs.at[me_d, me_y], me_z * per + y, d)

    def swap_copy():
        return send(swap_send, swap_recv, swap_ss, swap_rs, me_d * per + me_y, me_z)

    def u_copy():
        return send(u_send, u_recv, u_ss, u_rs, me_d * per + me_y, me_z)

    def arrival(ref, rs):
        return send(ref, ref, rs, rs, 0, 0)

    lane_group = lax.broadcasted_iota(jnp.int32, (rows_d, width), 1) // chans
    eye = lax.broadcasted_iota(jnp.int32, (rows_d, sq_width), 0) == lax.broadcasted_iota(jnp.int32, (rows_d, sq_width), 1)
    group_eye = lax.broadcasted_iota(jnp.int32, (groups, groups), 0) == lax.broadcasted_iota(jnp.int32, (groups, groups), 1)
    wide_0 = lax.broadcasted_iota(jnp.int32, (width, width), 0)
    wide_1 = lax.broadcasted_iota(jnp.int32, (width, width), 1)

    def prepare(l):
        step_size = jnp.exp(jnp.sum(jnp.where(group_eye, log_dt_ref[l : l + 1, :], 0.0), axis=1, keepdims=True))
        lam_re, lam_im = lam_re_ref[l], lam_im_ref[l]
        decay = jnp.exp(lam_re * step_size)
        angle = lam_im * step_size
        keep_re = decay * jnp.cos(angle)
        keep_im = decay * jnp.sin(angle)
        denom = lam_re * lam_re + lam_im * lam_im
        ratio_re = ((keep_re - 1.0) * lam_re + keep_im * lam_im) / denom
        ratio_im = (keep_im * lam_re - (keep_re - 1.0) * lam_im) / denom
        keep_a = jnp.concatenate([keep_re, keep_re], axis=1)
        keep_b = jnp.concatenate([-keep_im, keep_im], axis=1)
        for i in range(5):
            loads[l, i].wait()
        for g in range(groups):
            t_re, t_im = b_re[l, g], b_im[l, g]
            r_re, r_im = ratio_re[g : g + 1, :], ratio_im[g : g + 1, :]
            drive[l, pl.ds(g * chans, chans), :] = jnp.concatenate(
                [r_re * t_re - r_im * t_im, r_re * t_im + r_im * t_re], axis=1
            )
        read[l] = jnp.concatenate([c_re[l].reshape(width, half), -c_im[l].reshape(width, half)], axis=1)
        for g in range(groups):
            old = state[l, pl.ds(g, rows_d, stride=groups), :]
            kept[l, pl.ds(g * rows_d, rows_d), :] = (
                keep_a[g : g + 1, :] * old + keep_b[g : g + 1, :] * pltpu.roll(old, lanes // 2, 1)
            )
        proj[...] = lax.dot_general(kept[l], read[l], NT, precision=HIGHEST, preferred_element_type=F32)
        total = jnp.zeros((rows_d, width), F32)
        for g in range(groups):
            total = jnp.where(lane_group == g, proj[pl.ds(g * rows_d, rows_d), :], total)
        full = lax.dot_general(drive[l], read[l], NT, precision=HIGHEST, preferred_element_type=F32)
        mixer = jnp.where(wide_0 // chans == wide_1 // chans, full, 0.0)
        mixer = mixer + jnp.where(wide_0 == wide_1, skip_ref[l : l + 1, :], 0.0)
        return total, mixer

    def update(l, u):
        for g in range(groups):
            masked[pl.ds(g * rows_d, rows_d), :] = jnp.where(lane_group == g, u, 0.0)
        kept[l] = kept[l] + jnp.dot(masked[...], drive[l], precision=HIGHEST, preferred_element_type=F32)
        for g in range(groups):
            state[l, pl.ds(g, rows_d, stride=groups), :] = kept[l, pl.ds(g * rows_d, rows_d), :]

    elsewhere = ((me_z - me_d) * (me_z - me_d) + dp * dp - 1) // (dp * dp)
    pl.semaphore_wait(barrier, tp - 1 + dp - 1 + (per - 1) * (dp - 1) + elsewhere)

    smalls[0].wait()
    for k in reversed(range(1, tp)):
        x_copy(k).start()
    smalls[1].wait()
    gain_all[me_d] = jnp.broadcast_to(gain_ref[1:2, :], (rows_t, feats))
    for k in reversed(range(1, dp)):
        gain_copy(partner(me_d, k, dp)).start()
    for i in range(5, 8):
        loads[1, i].wait()
    for side in range(2):
        col_copy(side, 1).start()
    x_all[me_t] = stream_ref[...]
    for small in smalls[2:]:
        small.wait()
    from_old[...], mix_w[...] = prepare(0)

    loads[0, 5].wait()
    gain = gain_ref[0:1, :]
    own_part = own_sq = None
    for k in reversed(range(dp)):
        if k == 1:
            for side in range(2):
                col_wait(side, 1)
                col_copy(side, 2).start()
        to = partner(me_d, k, dp)
        for j in range(per):
            t = to * per + j

            @pl.when(t != me_t)
            def _():
                arrival(x_all.at[t], x_rs.at[t]).wait_recv()

        x = x_all[pl.ds(to * per, per)].astype(F32).reshape(rows_d, feats)
        column = jnp.sum(x * x, axis=1, keepdims=True)
        squares = jnp.sum(jnp.where(eye, column, 0.0), axis=0, keepdims=True)
        product = lax.dot_general((x * gain).astype(BF16), own_w[0], NT, preferred_element_type=F32)
        if k:
            sq_send[to] = jnp.broadcast_to(squares, (8, sq_width))
            sq_copy(to).start()
            part_send[to] = product.astype(BF16)
            part_copy(to).start()
        else:
            own_part, own_sq = product, squares
    for k in range(1, dp):
        by = partner(me_d, k, dp, True)
        arrival(sq_recv.at[by], sq_rs.at[by]).wait_recv()
        own_sq = own_sq + sq_recv[by][0:1, :]
        arrival(part_recv.at[by], part_rs.at[by]).wait_recv()
        own_part = own_part + part_recv[by].astype(F32)
    square_total = jnp.sum(jnp.where(eye, own_sq, 0.0), axis=1, keepdims=True)
    u = lax.rsqrt(square_total / (feats * dp) + EPS) * own_part
    u_keep[...] = u
    pre = from_old[...] + jnp.dot(u, mix_w[...], precision=HIGHEST, preferred_element_type=F32)
    mix_all[me_d] = jax.nn.gelu(pre).astype(BF16)
    for k in reversed(range(1, dp)):
        mix_copy(partner(me_d, k, dp)).start()
    for side in range(2):
        col_wait(side, 2)
        col_copy(side, 3).start()
        col_copy(side, 4).start()
    loads[0, 6].wait()
    loads[0, 7].wait()
    for k in range(dp):
        by = partner(me_d, k, dp, True)
        if k:
            arrival(mix_all.at[by], mix_rs.at[by]).wait_recv()
        mixed = mix_all[by]
        value = jnp.dot(mixed, own_w[1], preferred_element_type=F32)
        gate = jnp.dot(mixed, own_w[2], preferred_element_type=F32)
        for j in range(per):
            t = by * per + j
            rows = slice(j * rows_t, (j + 1) * rows_t)

            @pl.when(t != me_t)
            def _():
                comb_send[t, :, :feats] = value[rows].astype(BF16)
                comb_send[t, :, feats:] = gate[rows].astype(BF16)
                comb_copy(t).start()

            @pl.when(t == me_t)
            def _():
                comb_own[:, :feats] = value[rows]
                comb_own[:, feats:] = gate[rows]

    for step in (0, 1, -1, 2, -2):
        row_start(step)
    update(0, u_keep[...])
    total, mixer = prepare(1)
    swap_send[:rows_d] = jnp.concatenate([total, total], axis=1)
    swap_send[rows_d:] = jnp.concatenate([mixer, mixer], axis=1)

    @pl.when(me_z != me_d)
    def _():
        swap_copy().start()

    @pl.when(me_z == me_d)
    def _():
        swap_recv[...] = swap_send[...]

    for side in range(2):
        col_wait(side, 3)
        col_wait(side, 4)
    for step in (3, -3, 4):
        row_start(step)
    for k in range(1, tp):
        x_copy(k).wait_send()
    for k in range(1, dp):
        to = partner(me_d, k, dp)
        part_copy(to).wait_send()
        sq_copy(to).wait_send()
        mix_copy(to).wait_send()
        gain_copy(to).wait_send()
    for side in range(2):
        for i in range(1, 5):
            col_copy(side, i).wait_send()

    combined = comb_own[...]
    for k in range(1, tp):
        by = partner(me_t, k, tp, True)
        arrival(comb_recv.at[by], comb_rs.at[by]).wait_recv()
        combined = combined + comb_recv[by].astype(F32)
    fresh = (x_all[me_t].astype(F32) + combined[:, :feats] * jax.nn.sigmoid(combined[:, feats:])).astype(BF16)

    x_far[me_d, me_y] = fresh
    for k in PLANE_FAR_FIRST:
        for j in ROW_FAR_FIRST:
            if k or j:
                xf_copy(partner(me_y, j, per), partner(me_d, k, dp)).start()
    for k in range(1, tp):
        comb_copy(partner(me_t, k, tp)).wait_send()

    @pl.when(me_z != me_d)
    def _():
        swap_copy().wait_send()

    for k in range(1, dp):
        by = partner(me_d, k, dp, True)
        arrival(gain_all.at[by], gain_rs.at[by]).wait_recv()

    acc = jnp.zeros((rows_d, width), F32)
    squares = jnp.zeros((rows_d, feats), F32)
    for k in reversed(PLANE_FAR_FIRST):
        by = partner(me_d, k, dp, True)
        if k:
            row_wait(by, 0)
        weights = far_w.at[by] if k else col_w.at[me_d]
        for j in reversed(ROW_FAR_FIRST):
            if k or j:
                y = partner(me_y, j, per)
                arrival(x_far.at[by, y], xf_rs.at[by, y]).wait_recv()
        x = x_far[by].astype(F32)
        normed = (x * gain_all[by][None]).astype(BF16).reshape(rows_d, feats)
        x = x.reshape(rows_d, feats)
        squares = squares + x * x
        acc = acc + lax.dot_general(normed, weights[0], NT, preferred_element_type=F32)
    u = lax.rsqrt(jnp.sum(squares, axis=1, keepdims=True) / (feats * dp) + EPS) * acc
    u_send[...] = jnp.concatenate([u, u], axis=1)

    @pl.when(me_z != me_d)
    def _():
        u_copy().start()
        arrival(swap_recv, swap_rs).wait_recv()

    @pl.when(me_z == me_d)
    def _():
        u_recv[...] = u_send[...]

    pre = swap_recv[:rows_d, :width] + jnp.dot(
        u, swap_recv[rows_d:, :width], precision=HIGHEST, preferred_element_type=F32
    )
    mixed = jax.nn.gelu(pre).astype(BF16)
    for k in PLANE_FAR_FIRST:
        to = partner(me_d, k, dp)
        if k:
            row_wait(to, 1)
        weights = far_w.at[to] if k else col_w.at[me_d]
        value = jnp.dot(mixed, weights[1], preferred_element_type=F32)
        gate = jnp.dot(mixed, weights[2], preferred_element_type=F32)
        out_send[to, :, :, :feats] = value.astype(BF16).reshape(per, rows_t, feats)
        out_send[to, :, :, feats:] = gate.astype(BF16).reshape(per, rows_t, feats)
        for j in ROW_FAR_FIRST:
            if k or j:
                of_copy(partner(me_y, j, per), to).start()
    for k in range(dp):
        for j in range(per):
            if k or j:
                xf_copy(partner(me_y, j, per), partner(me_d, k, dp)).wait_send()
    combined = out_send[me_d, me_y].astype(F32)

    @pl.when(me_z != me_d)
    def _():
        arrival(u_recv, u_rs).wait_recv()

    update(1, u_recv[:, :width])
    for k in reversed(PLANE_FAR_FIRST):
        by = partner(me_d, k, dp, True)
        for j in reversed(ROW_FAR_FIRST):
            if k or j:
                y = partner(me_y, j, per)
                arrival(out_recv.at[by, y], of_rs.at[by, y]).wait_recv()
                combined = combined + out_recv[by, y].astype(F32)
    out_ref[...] = (
        x_far[me_d, me_y].astype(F32) + combined[:, :feats] * jax.nn.sigmoid(combined[:, feats:])
    ).astype(BF16)

    for k in range(dp):
        for j in range(per):
            if k or j:
                of_copy(partner(me_y, j, per), partner(me_d, k, dp)).wait_send()
    for k in range(1, dp):
        for i in range(2):
            row_copy(partner(me_d, k, dp), i).wait_send()

    @pl.when(me_z != me_d)
    def _():
        u_copy().wait_send()


def per_device(
    tp, dp,
    stream, norm_gain, w_input, lam_re, lam_im, log_dt, b_re, b_im, readout_real, readout_imaginary, d_skip,
    w_val, w_gate, state,
):
    layers, feats, width = w_input.shape
    rows_t = stream.shape[0]
    rows_d, groups, lanes = state.shape[1:]
    chans = b_re.shape[-1]
    per = rows_d // rows_t

    turned_in = w_input.swapaxes(1, 2)
    turned_re, turned_im = b_re.swapaxes(2, 3), b_im.swapaxes(2, 3)

    limit = 67043328 - 4 * layers * rows_d * groups * lanes - (256 << 10)
    vmem = pl.BlockSpec(memory_space=pltpu.VMEM)
    hbm = pl.BlockSpec(memory_space=pltpu.HBM)
    sq_width = max(rows_d, 128)
    dma = lambda *shape: pltpu.SemaphoreType.DMA(shape)
    out, states = pl.pallas_call(
        functools.partial(kernel, tp, dp, chans),
        out_shape=(pltpu.VMEM(stream.shape, BF16), pltpu.VMEM((layers, rows_d * groups, lanes), F32)),
        in_specs=[hbm] * 14,
        out_specs=(vmem, vmem),
        scratch_shapes=[
            pltpu.VMEM(stream.shape, BF16),
            pltpu.VMEM(norm_gain.shape, F32),
            pltpu.VMEM(lam_re.shape, F32),
            pltpu.VMEM(lam_im.shape, F32),
            pltpu.VMEM(log_dt.shape, F32),
            pltpu.VMEM(d_skip.shape, F32),
            pltpu.VMEM((3, width, feats), BF16),
            pltpu.VMEM(turned_re.shape, F32),
            pltpu.VMEM(turned_im.shape, F32),
            pltpu.VMEM(readout_real.shape, F32),
            pltpu.VMEM(readout_imaginary.shape, F32),
            pltpu.VMEM((layers, width, lanes), F32),
            pltpu.VMEM((layers, width, lanes), F32),
            pltpu.VMEM((layers, rows_d * groups, lanes), F32),
            pltpu.VMEM((rows_d * groups, width), F32),
            pltpu.VMEM((rows_d, width), F32),
            pltpu.VMEM((rows_d * groups, width), F32),
            pltpu.VMEM((rows_d, width), F32),
            pltpu.VMEM((width, width), F32),
            pltpu.VMEM((tp, rows_t, feats), BF16),
            pltpu.VMEM((dp, rows_d, width), BF16),
            pltpu.VMEM((dp, rows_d, width), BF16),
            pltpu.VMEM((dp, 8, sq_width), F32),
            pltpu.VMEM((dp, 8, sq_width), F32),
            pltpu.VMEM((dp, rows_d, width), BF16),
            pltpu.VMEM((tp, rows_t, 2 * feats), BF16),
            pltpu.VMEM((rows_t, 2 * feats), F32),
            pltpu.VMEM((tp, rows_t, 2 * feats), BF16),
            pltpu.VMEM((dp, rows_t, feats), F32),
            pltpu.VMEM((dp, 3, width, feats), BF16),
            pltpu.VMEM((dp, 3, width, feats), BF16),
            pltpu.VMEM((dp, per, rows_t, feats), BF16),
            pltpu.VMEM((rows_d + width, 128), F32),
            pltpu.VMEM((rows_d + width, 128), F32),
            pltpu.VMEM((rows_d, 128), F32),
            pltpu.VMEM((rows_d, 128), F32),
            pltpu.VMEM((dp, per, rows_t, 2 * feats), BF16),
            pltpu.VMEM((dp, per, rows_t, 2 * feats), BF16),
            dma(6), dma(layers, 8),
            dma(tp), dma(tp),
            dma(dp), dma(dp),
            dma(dp), dma(dp),
            dma(dp), dma(dp),
            dma(tp), dma(tp),
            dma(dp), dma(dp),
            dma(2, 4), dma(2, 4),
            dma(2, dp), dma(2, dp),
            dma(dp, per), dma(dp, per),
            pltpu.SemaphoreType.DMA, pltpu.SemaphoreType.DMA,
            pltpu.SemaphoreType.DMA, pltpu.SemaphoreType.DMA,
            dma(dp, per), dma(dp, per),
        ],
        compiler_params=pltpu.CompilerParams(collective_id=0, has_side_effects=True, vmem_limit_bytes=limit),
    )(
        stream, norm_gain, turned_in, lam_re, lam_im, log_dt, turned_re, turned_im, readout_real,
        readout_imaginary, d_skip, w_val, w_gate,
        state.reshape(layers, rows_d * groups, lanes),
    )
    return out, states.reshape(state.shape)


def solution(mesh):
    return jax.shard_map(
        functools.partial(per_device, mesh.shape["tp"], mesh.shape["dp"]),
        mesh=mesh,
        in_specs=(
            P("tp", "dp"),
            P(None, "dp"),
            P(None, "dp", "tp"),
            P(None, "tp", None),
            P(None, "tp", None),
            P(None, "tp"),
            P(None, "tp", None, None),
            P(None, "tp", None, None),
            P(None, "tp", None, None),
            P(None, "tp", None, None),
            P(None, "tp"),
            P(None, "tp", "dp"),
            P(None, "tp", "dp"),
            P(None, "dp", "tp", None),
        ),
        out_specs=(P("tp", "dp"), P(None, "dp", "tp", None)),
        check_vma=False,
    )
```

```python
import functools

import jax
import jax.numpy as jnp
from jax import lax
from jax.experimental import pallas as pl
from jax.experimental.pallas import tpu as pltpu
from jax.sharding import PartitionSpec as P

EPS = 1e-06
F32 = jnp.float32
BF16 = jnp.bfloat16
HIGHEST = lax.Precision.HIGHEST
NT = (((1,), (1,)), ((), ()))
PLANE_FAR_FIRST = (4, 5, 6, 7, 2, 3, 1, 0)
ROW_FAR_FIRST = (2, 1, 3, 0)


def partner(me, k, n, back=False):
    if n & (n - 1):
        return (me + (n - k if back else k)) % n
    found, bit = 0, 1
    while bit < n:
        mine = (me // bit) % 2
        found = found + (bit * (1 - mine) if k & bit else bit * mine)
        bit *= 2
    return found


def kernel(
    tp, dp, chans,
    stream_hbm, gain_hbm, w_in_hbm, lam_re_hbm, lam_im_hbm, log_dt_hbm, b_re_hbm, b_im_hbm, c_re_hbm, c_im_hbm, skip_hbm,
    w_val_hbm, w_gate_hbm, state_hbm,
    out_ref, state,
    stream_ref, gain_ref, lam_re_ref, lam_im_ref, log_dt_ref, skip_ref, own_w, b_re, b_im, c_re, c_im, drive, read,
    kept, proj, u_keep, masked, from_old, mix_w,
    x_all, part_send, part_recv, sq_send, sq_recv, mix_all, near_own, near_send, near_recv, comb_send, comb_own, comb_recv,
    gain_all, col_in, col_out, far_in, x_far, swap_send, swap_recv, u_send, u_recv, mix_far, out_send, out_recv,
    small_sem, load_sem, x_ss, x_rs, part_ss, part_rs, sq_ss, sq_rs, mix_ss, mix_rs, near_ss, near_rs, comb_ss, comb_rs,
    gain_ss, gain_rs, col_ss, col_rs, row_ss, row_rs, xf_ss, xf_rs, swap_ss, swap_rs, u_ss, u_rs, mf_ss, mf_rs, of_ss, of_rs,
):
    layers = w_in_hbm.shape[0]
    me_t, me_d = lax.axis_index("tp"), lax.axis_index("dp")
    rows_t, feats = stream_ref.shape
    rows_d, width = u_keep.shape
    per = rows_d // rows_t
    groups, half = lam_re_ref.shape[1:]
    lanes = state.shape[2]
    sq_width = sq_send.shape[2]
    me_z, me_y = me_t // per, me_t % per

    barrier = pltpu.get_barrier_semaphore()

    def greet(t, d):
        pl.semaphore_signal(barrier, inc=1, device_id={"tp": t, "dp": d}, device_id_type=pl.DeviceIdType.MESH)

    for k in range(1, dp):
        greet(me_t, partner(me_d, k, dp))
    for k in range(1, tp):
        greet(partner(me_t, k, tp), me_d)
    for j in range(1, per):
        for k in range(1, dp):
            greet(me_z * per + partner(me_y, j, per), partner(me_d, k, dp))

    @pl.when(me_z != me_d)
    def _():
        greet(me_d * per + me_y, me_z)

    smalls = []
    for i, (src, dst) in enumerate(
        (
            (stream_hbm, stream_ref), (gain_hbm, gain_ref), (lam_re_hbm, lam_re_ref), (lam_im_hbm, lam_im_ref),
            (log_dt_hbm, log_dt_ref), (skip_hbm, skip_ref),
        )
    ):
        smalls.append(pltpu.make_async_copy(src, dst, small_sem.at[i]))
        smalls[i].start()
    loads = {}
    for l in range(layers):
        weights = (
            [own_w.at[i] for i in range(3)] if l == 0 else [col_in.at[me_z], col_out.at[me_z, 0], col_out.at[me_z, 1]]
        )
        for i, (src, dst) in enumerate(
            (
                (b_re_hbm, b_re.at[l]), (b_im_hbm, b_im.at[l]), (c_re_hbm, c_re.at[l]), (c_im_hbm, c_im.at[l]),
                (state_hbm, state.at[l]), (w_in_hbm, weights[0]), (w_val_hbm, weights[1]), (w_gate_hbm, weights[2]),
            )
        ):
            loads[l, i] = pltpu.make_async_copy(src.at[l], dst, load_sem.at[l, i])
            loads[l, i].start()

    def send(src, dst, ss, rs, t, d):
        return pltpu.make_async_remote_copy(
            src_ref=src, dst_ref=dst, send_sem=ss, recv_sem=rs, device_id={"tp": t, "dp": d},
            device_id_type=pl.DeviceIdType.MESH,
        )

    def x_copy(k):
        to = partner(me_t, k, tp)
        return send(stream_ref, x_all.at[me_t], x_ss.at[to], x_rs.at[me_t], to, me_d)

    def part_copy(to):
        return send(part_send.at[to], part_recv.at[me_d], part_ss.at[to], part_rs.at[me_d], me_t, to)

    def sq_copy(to):
        return send(sq_send.at[to], sq_recv.at[me_d], sq_ss.at[to], sq_rs.at[me_d], me_t, to)

    def mix_copy(to):
        return send(mix_all.at[me_d], mix_all.at[me_d], mix_ss.at[to], mix_rs.at[me_d], me_t, to)

    def near_copy(z, y):
        return send(
            near_send.at[z, y], near_recv.at[z, me_y], near_ss.at[z, y], near_rs.at[z, me_y], me_z * per + y, me_d
        )

    def comb_copy(z):
        return send(comb_send.at[z], comb_recv.at[me_z], comb_ss.at[z], comb_rs.at[me_z], z * per + me_y, me_d)

    def gain_copy(to):
        return send(gain_all.at[me_d], gain_all.at[me_d], gain_ss.at[to], gain_rs.at[me_d], me_t, to)

    def col_part(what, home, side, i):
        if what:
            return col_out.at[home, :, pl.ds(side * (width // 2), width // 2)] if i == 4 else col_out.at[home]
        return col_in.at[home, pl.ds(side * (width // 2), width // 2)] if i == 4 else col_in.at[home]

    def col_copy(what, side, i):
        sign = 1 - 2 * side
        home = lax.rem(me_z - sign * min(i - 1, 2) + 2 * dp, dp)
        to = lax.rem(me_z + sign * (2 if i == 4 else 1) + dp, dp)
        part = col_part(what, home, side, i)
        return send(part, part, col_ss.at[what, side, i - 1], col_rs.at[what, side, i - 1], to * per + me_y, me_d)

    def col_start(what, *hops):
        for i in hops:
            for side in range(2):
                col_copy(what, side, i).start()

    def col_wait(what, *hops):
        for i in hops:
            for side in range(2):
                home = lax.rem(me_z - (1 - 2 * side) * i + 2 * dp, dp)
                arrival(col_part(what, home, side, i), col_rs.at[what, side, i - 1]).wait_recv()

    def row_copy(z):
        return send(col_in.at[z], far_in.at[me_d], row_ss.at[z], row_rs.at[me_d], me_t, z)

    def mf_copy(to):
        return send(mix_far.at[me_d], mix_far.at[me_d], mf_ss.at[to], mf_rs.at[me_d], me_t, to)

    def xf_copy(y, d):
        return send(x_far.at[me_d, me_y], x_far.at[me_d, me_y], xf_ss.at[d, y], xf_rs.at[me_d, me_y], me_z * per + y, d)

    def of_copy(y):
        return send(out_send.at[y], out_recv.at[me_y], of_ss.at[y], of_rs.at[me_y], me_z * per + y, me_d)

    def swap_copy():
        return send(swap_send, swap_recv, swap_ss, swap_rs, me_d * per + me_y, me_z)

    def u_copy():
        return send(u_send, u_recv, u_ss, u_rs, me_d * per + me_y, me_z)

    def arrival(ref, rs):
        return send(ref, ref, rs, rs, 0, 0)

    lane_group = lax.broadcasted_iota(jnp.int32, (rows_d, width), 1) // chans
    eye = lax.broadcasted_iota(jnp.int32, (rows_d, sq_width), 0) == lax.broadcasted_iota(jnp.int32, (rows_d, sq_width), 1)
    group_eye = lax.broadcasted_iota(jnp.int32, (groups, groups), 0) == lax.broadcasted_iota(jnp.int32, (groups, groups), 1)
    wide_0 = lax.broadcasted_iota(jnp.int32, (width, width), 0)
    wide_1 = lax.broadcasted_iota(jnp.int32, (width, width), 1)

    def prepare(l):
        step_size = jnp.exp(jnp.sum(jnp.where(group_eye, log_dt_ref[l : l + 1, :], 0.0), axis=1, keepdims=True))
        lam_re, lam_im = lam_re_ref[l], lam_im_ref[l]
        decay = jnp.exp(lam_re * step_size)
        angle = lam_im * step_size
        keep_re = decay * jnp.cos(angle)
        keep_im = decay * jnp.sin(angle)
        denom = lam_re * lam_re + lam_im * lam_im
        ratio_re = ((keep_re - 1.0) * lam_re + keep_im * lam_im) / denom
        ratio_im = (keep_im * lam_re - (keep_re - 1.0) * lam_im) / denom
        keep_a = jnp.concatenate([keep_re, keep_re], axis=1)
        keep_b = jnp.concatenate([-keep_im, keep_im], axis=1)
        for i in range(5):
            loads[l, i].wait()
        for g in range(groups):
            t_re, t_im = b_re[l, g], b_im[l, g]
            r_re, r_im = ratio_re[g : g + 1, :], ratio_im[g : g + 1, :]
            drive[l, pl.ds(g * chans, chans), :] = jnp.concatenate(
                [r_re * t_re - r_im * t_im, r_re * t_im + r_im * t_re], axis=1
            )
        read[l] = jnp.concatenate([c_re[l].reshape(width, half), -c_im[l].reshape(width, half)], axis=1)
        for g in range(groups):
            old = state[l, pl.ds(g, rows_d, stride=groups), :]
            kept[l, pl.ds(g * rows_d, rows_d), :] = (
                keep_a[g : g + 1, :] * old + keep_b[g : g + 1, :] * pltpu.roll(old, lanes // 2, 1)
            )
        proj[...] = lax.dot_general(kept[l], read[l], NT, precision=HIGHEST, preferred_element_type=F32)
        total = jnp.zeros((rows_d, width), F32)
        for g in range(groups):
            total = jnp.where(lane_group == g, proj[pl.ds(g * rows_d, rows_d), :], total)
        full = lax.dot_general(drive[l], read[l], NT, precision=HIGHEST, preferred_element_type=F32)
        mixer = jnp.where(wide_0 // chans == wide_1 // chans, full, 0.0)
        mixer = mixer + jnp.where(wide_0 == wide_1, skip_ref[l : l + 1, :], 0.0)
        return total, mixer

    def update(l, u):
        for g in range(groups):
            masked[pl.ds(g * rows_d, rows_d), :] = jnp.where(lane_group == g, u, 0.0)
        kept[l] = kept[l] + jnp.dot(masked[...], drive[l], precision=HIGHEST, preferred_element_type=F32)
        for g in range(groups):
            state[l, pl.ds(g, rows_d, stride=groups), :] = kept[l, pl.ds(g * rows_d, rows_d), :]

    elsewhere = ((me_z - me_d) * (me_z - me_d) + dp * dp - 1) // (dp * dp)
    pl.semaphore_wait(barrier, tp - 1 + dp - 1 + (per - 1) * (dp - 1) + elsewhere)

    smalls[0].wait()
    for k in reversed(range(1, tp)):
        x_copy(k).start()
    smalls[1].wait()
    gain_all[me_d] = jnp.broadcast_to(gain_ref[1:2, :], (rows_t, feats))
    for k in reversed(range(1, dp)):
        gain_copy(partner(me_d, k, dp)).start()
    loads[1, 5].wait()
    col_start(0, 1)
    x_all[me_t] = stream_ref[...]
    for small in smalls[2:]:
        small.wait()
    from_old[...], mix_w[...] = prepare(0)

    loads[0, 5].wait()
    gain = gain_ref[0:1, :]
    own_part = own_sq = None
    for k in reversed(range(dp)):
        if k == 6:
            col_wait(0, 1)
            col_start(0, 2)
        to = partner(me_d, k, dp)
        for j in range(per):
            t = to * per + j

            @pl.when(t != me_t)
            def _():
                arrival(x_all.at[t], x_rs.at[t]).wait_recv()

        x = x_all[pl.ds(to * per, per)].astype(F32).reshape(rows_d, feats)
        column = jnp.sum(x * x, axis=1, keepdims=True)
        squares = jnp.sum(jnp.where(eye, column, 0.0), axis=0, keepdims=True)
        product = lax.dot_general((x * gain).astype(BF16), own_w[0], NT, preferred_element_type=F32)
        if k:
            sq_send[to] = jnp.broadcast_to(squares, (8, sq_width))
            sq_copy(to).start()
            part_send[to] = product.astype(BF16)
            part_copy(to).start()
        else:
            own_part, own_sq = product, squares
    loads[1, 6].wait()
    loads[1, 7].wait()
    col_start(1, 1)
    for k in range(1, dp):
        by = partner(me_d, k, dp, True)
        arrival(sq_recv.at[by], sq_rs.at[by]).wait_recv()
        own_sq = own_sq + sq_recv[by][0:1, :]
        arrival(part_recv.at[by], part_rs.at[by]).wait_recv()
        own_part = own_part + part_recv[by].astype(F32)
        if k == 2:
            col_wait(0, 2)
            col_start(0, 3, 4)
    square_total = jnp.sum(jnp.where(eye, own_sq, 0.0), axis=1, keepdims=True)
    u = lax.rsqrt(square_total / (feats * dp) + EPS) * own_part
    u_keep[...] = u
    pre = from_old[...] + jnp.dot(u, mix_w[...], precision=HIGHEST, preferred_element_type=F32)
    mix_all[me_d] = jax.nn.gelu(pre).astype(BF16)
    for k in reversed(range(1, dp)):
        mix_copy(partner(me_d, k, dp)).start()
    loads[0, 6].wait()
    loads[0, 7].wait()
    for k in range(dp):
        by = partner(me_d, k, dp, True)
        if k:
            arrival(mix_all.at[by], mix_rs.at[by]).wait_recv()
        mixed = mix_all[by]
        value = jnp.dot(mixed, own_w[1], preferred_element_type=F32)
        gate = jnp.dot(mixed, own_w[2], preferred_element_type=F32)
        near_own[by, :, :, :feats] = value.reshape(per, rows_t, feats)
        near_own[by, :, :, feats:] = gate.reshape(per, rows_t, feats)
        near_send[by, :, :, :feats] = value.astype(BF16).reshape(per, rows_t, feats)
        near_send[by, :, :, feats:] = gate.astype(BF16).reshape(per, rows_t, feats)
        for j in ROW_FAR_FIRST:
            if j:
                near_copy(by, partner(me_y, j, per)).start()

    def gather_near(k):
        z = partner(me_d, k, dp, True)
        total = near_own[z, me_y]
        for j in range(1, per):
            y = partner(me_y, j, per)
            arrival(near_recv.at[z, y], near_rs.at[z, y]).wait_recv()
            total = total + near_recv[z, y].astype(F32)

        @pl.when(z != me_z)
        def _():
            comb_send[z] = total.astype(BF16)
            comb_copy(z).start()

        @pl.when(z == me_z)
        def _():
            comb_own[...] = total

    col_wait(0, 3, 4)
    for k in reversed(range(1, dp)):
        row_copy(partner(me_d, k, dp)).start()
    for k in range(4):
        gather_near(k)
    update(0, u_keep[...])
    total, mixer = prepare(1)
    swap_send[:rows_d] = jnp.concatenate([total, total], axis=1)
    swap_send[rows_d:] = jnp.concatenate([mixer, mixer], axis=1)

    @pl.when(me_z != me_d)
    def _():
        swap_copy().start()

    @pl.when(me_z == me_d)
    def _():
        swap_recv[...] = swap_send[...]

    for k in range(4, dp):
        gather_near(k)
    for k in range(1, tp):
        x_copy(k).wait_send()
    for k in range(1, dp):
        to = partner(me_d, k, dp)
        part_copy(to).wait_send()
        sq_copy(to).wait_send()
        mix_copy(to).wait_send()
        gain_copy(to).wait_send()
    for side in range(2):
        for i in range(1, 5):
            col_copy(0, side, i).wait_send()

    col_wait(1, 1)
    col_start(1, 2)
    combined = comb_own[...]
    for k in range(1, dp):
        by = partner(me_z, k, dp, True)
        arrival(comb_recv.at[by], comb_rs.at[by]).wait_recv()
        combined = combined + comb_recv[by].astype(F32)
    fresh = (x_all[me_t].astype(F32) + combined[:, :feats] * jax.nn.sigmoid(combined[:, feats:])).astype(BF16)

    x_far[me_d, me_y] = fresh
    for k in PLANE_FAR_FIRST:
        for j in ROW_FAR_FIRST:
            if k or j:
                xf_copy(partner(me_y, j, per), partner(me_d, k, dp)).start()
    for k in range(1, dp):
        comb_copy(partner(me_z, k, dp)).wait_send()
    for k in range(dp):
        for j in range(1, per):
            near_copy(k, partner(me_y, j, per)).wait_send()

    @pl.when(me_z != me_d)
    def _():
        swap_copy().wait_send()

    for k in range(1, dp):
        by = partner(me_d, k, dp, True)
        arrival(gain_all.at[by], gain_rs.at[by]).wait_recv()

    acc = jnp.zeros((rows_d, width), F32)
    squares = jnp.zeros((rows_d, feats), F32)
    for k in reversed(PLANE_FAR_FIRST):
        by = partner(me_d, k, dp, True)
        if k == 3:
            col_wait(1, 2)
            col_start(1, 3, 4)
        if k:
            arrival(far_in.at[by], row_rs.at[by]).wait_recv()
        weights = far_in.at[by] if k else col_in.at[me_d]
        for j in reversed(ROW_FAR_FIRST):
            if k or j:
                y = partner(me_y, j, per)
                arrival(x_far.at[by, y], xf_rs.at[by, y]).wait_recv()
        x = x_far[by].astype(F32)
        normed = (x * gain_all[by][None]).astype(BF16).reshape(rows_d, feats)
        x = x.reshape(rows_d, feats)
        squares = squares + x * x
        acc = acc + lax.dot_general(normed, weights[...], NT, preferred_element_type=F32)
    u = lax.rsqrt(jnp.sum(squares, axis=1, keepdims=True) / (feats * dp) + EPS) * acc
    u_send[...] = jnp.concatenate([u, u], axis=1)

    @pl.when(me_z != me_d)
    def _():
        u_copy().start()
        arrival(swap_recv, swap_rs).wait_recv()

    @pl.when(me_z == me_d)
    def _():
        u_recv[...] = u_send[...]

    pre = swap_recv[:rows_d, :width] + jnp.dot(
        u, swap_recv[rows_d:, :width], precision=HIGHEST, preferred_element_type=F32
    )
    mix_far[me_d] = jax.nn.gelu(pre).astype(BF16)
    for k in PLANE_FAR_FIRST:
        if k:
            mf_copy(partner(me_d, k, dp)).start()
    col_wait(1, 3, 4)
    for k in range(dp):
        for j in range(per):
            if k or j:
                xf_copy(partner(me_y, j, per), partner(me_d, k, dp)).wait_send()
    for k in range(1, dp):
        row_copy(partner(me_d, k, dp)).wait_send()
    for side in range(2):
        for i in range(1, 5):
            col_copy(1, side, i).wait_send()
    value = jnp.zeros((rows_d, feats), F32)
    gate = jnp.zeros((rows_d, feats), F32)
    for k in reversed(PLANE_FAR_FIRST):
        by = partner(me_d, k, dp, True)
        if k:
            arrival(mix_far.at[by], mf_rs.at[by]).wait_recv()
        mixed = mix_far[by]
        value = value + jnp.dot(mixed, col_out[by, 0], preferred_element_type=F32)
        gate = gate + jnp.dot(mixed, col_out[by, 1], preferred_element_type=F32)
    near_own[0, :, :, :feats] = value.reshape(per, rows_t, feats)
    near_own[0, :, :, feats:] = gate.reshape(per, rows_t, feats)
    out_send[:, :, :feats] = value.astype(BF16).reshape(per, rows_t, feats)
    out_send[:, :, feats:] = gate.astype(BF16).reshape(per, rows_t, feats)
    for j in ROW_FAR_FIRST:
        if j:
            of_copy(partner(me_y, j, per)).start()

    @pl.when(me_z != me_d)
    def _():
        arrival(u_recv, u_rs).wait_recv()

    update(1, u_recv[:, :width])
    combined = near_own[0, me_y]
    for j in reversed(ROW_FAR_FIRST):
        if j:
            y = partner(me_y, j, per)
            arrival(out_recv.at[y], of_rs.at[y]).wait_recv()
            combined = combined + out_recv[y].astype(F32)
    out_ref[...] = (
        x_far[me_d, me_y].astype(F32) + combined[:, :feats] * jax.nn.sigmoid(combined[:, feats:])
    ).astype(BF16)

    for k in range(1, dp):
        mf_copy(partner(me_d, k, dp)).wait_send()
    for j in range(1, per):
        of_copy(partner(me_y, j, per)).wait_send()

    @pl.when(me_z != me_d)
    def _():
        u_copy().wait_send()


def per_device(
    tp, dp,
    stream, norm_gain, w_input, lam_re, lam_im, log_dt, b_re, b_im, readout_real, readout_imaginary, d_skip,
    w_val, w_gate, state,
):
    layers, feats, width = w_input.shape
    rows_t = stream.shape[0]
    rows_d, groups, lanes = state.shape[1:]
    chans = b_re.shape[-1]
    per = rows_d // rows_t

    turned_in = w_input.swapaxes(1, 2)
    turned_re, turned_im = b_re.swapaxes(2, 3), b_im.swapaxes(2, 3)

    limit = 67043328 - 4 * layers * rows_d * groups * lanes - (256 << 10)
    vmem = pl.BlockSpec(memory_space=pltpu.VMEM)
    hbm = pl.BlockSpec(memory_space=pltpu.HBM)
    sq_width = max(rows_d, 128)
    dma = lambda *shape: pltpu.SemaphoreType.DMA(shape)
    out, states = pl.pallas_call(
        functools.partial(kernel, tp, dp, chans),
        out_shape=(pltpu.VMEM(stream.shape, BF16), pltpu.VMEM((layers, rows_d * groups, lanes), F32)),
        in_specs=[hbm] * 14,
        out_specs=(vmem, vmem),
        scratch_shapes=[
            pltpu.VMEM(stream.shape, BF16),
            pltpu.VMEM(norm_gain.shape, F32),
            pltpu.VMEM(lam_re.shape, F32),
            pltpu.VMEM(lam_im.shape, F32),
            pltpu.VMEM(log_dt.shape, F32),
            pltpu.VMEM(d_skip.shape, F32),
            pltpu.VMEM((3, width, feats), BF16),
            pltpu.VMEM(turned_re.shape, F32),
            pltpu.VMEM(turned_im.shape, F32),
            pltpu.VMEM(readout_real.shape, F32),
            pltpu.VMEM(readout_imaginary.shape, F32),
            pltpu.VMEM((layers, width, lanes), F32),
            pltpu.VMEM((layers, width, lanes), F32),
            pltpu.VMEM((layers, rows_d * groups, lanes), F32),
            pltpu.VMEM((rows_d * groups, width), F32),
            pltpu.VMEM((rows_d, width), F32),
            pltpu.VMEM((rows_d * groups, width), F32),
            pltpu.VMEM((rows_d, width), F32),
            pltpu.VMEM((width, width), F32),
            pltpu.VMEM((tp, rows_t, feats), BF16),
            pltpu.VMEM((dp, rows_d, width), BF16),
            pltpu.VMEM((dp, rows_d, width), BF16),
            pltpu.VMEM((dp, 8, sq_width), F32),
            pltpu.VMEM((dp, 8, sq_width), F32),
            pltpu.VMEM((dp, rows_d, width), BF16),
            pltpu.VMEM((dp, per, rows_t, 2 * feats), F32),
            pltpu.VMEM((dp, per, rows_t, 2 * feats), BF16),
            pltpu.VMEM((dp, per, rows_t, 2 * feats), BF16),
            pltpu.VMEM((dp, rows_t, 2 * feats), BF16),
            pltpu.VMEM((rows_t, 2 * feats), F32),
            pltpu.VMEM((dp, rows_t, 2 * feats), BF16),
            pltpu.VMEM((dp, rows_t, feats), F32),
            pltpu.VMEM((dp, width, feats), BF16),
            pltpu.VMEM((dp, 2, width, feats), BF16),
            pltpu.VMEM((dp, width, feats), BF16),
            pltpu.VMEM((dp, per, rows_t, feats), BF16),
            pltpu.VMEM((rows_d + width, 128), F32),
            pltpu.VMEM((rows_d + width, 128), F32),
            pltpu.VMEM((rows_d, 128), F32),
            pltpu.VMEM((rows_d, 128), F32),
            pltpu.VMEM((dp, rows_d, width), BF16),
            pltpu.VMEM((per, rows_t, 2 * feats), BF16),
            pltpu.VMEM((per, rows_t, 2 * feats), BF16),
            dma(6), dma(layers, 8),
            dma(tp), dma(tp),
            dma(dp), dma(dp),
            dma(dp), dma(dp),
            dma(dp), dma(dp),
            dma(dp, per), dma(dp, per),
            dma(dp), dma(dp),
            dma(dp), dma(dp),
            dma(2, 2, 4), dma(2, 2, 4),
            dma(dp), dma(dp),
            dma(dp, per), dma(dp, per),
            pltpu.SemaphoreType.DMA, pltpu.SemaphoreType.DMA,
            pltpu.SemaphoreType.DMA, pltpu.SemaphoreType.DMA,
            dma(dp), dma(dp),
            dma(per), dma(per),
        ],
        compiler_params=pltpu.CompilerParams(collective_id=0, has_side_effects=True, vmem_limit_bytes=limit),
    )(
        stream, norm_gain, turned_in, lam_re, lam_im, log_dt, turned_re, turned_im, readout_real,
        readout_imaginary, d_skip, w_val, w_gate,
        state.reshape(layers, rows_d * groups, lanes),
    )
    return out, states.reshape(state.shape)


def solution(mesh):
    return jax.shard_map(
        functools.partial(per_device, mesh.shape["tp"], mesh.shape["dp"]),
        mesh=mesh,
        in_specs=(
            P("tp", "dp"),
            P(None, "dp"),
            P(None, "dp", "tp"),
            P(None, "tp", None),
            P(None, "tp", None),
            P(None, "tp"),
            P(None, "tp", None, None),
            P(None, "tp", None, None),
            P(None, "tp", None, None),
            P(None, "tp", None, None),
            P(None, "tp"),
            P(None, "tp", "dp"),
            P(None, "tp", "dp"),
            P(None, "dp", "tp", None),
        ),
        out_specs=(P("tp", "dp"), P(None, "dp", "tp", None)),
        check_vma=False,
    )
```

```python
import functools

import jax
import jax.numpy as jnp
from jax import lax
from jax.experimental import pallas as pl
from jax.experimental.pallas import tpu as pltpu
from jax.sharding import PartitionSpec as P

EPS = 1e-06
F32 = jnp.float32
BF16 = jnp.bfloat16
HIGHEST = lax.Precision.HIGHEST
NT = (((1,), (1,)), ((), ()))
PLANE_FAR_FIRST = (4, 5, 6, 7, 2, 3, 1, 0)
ROW_FAR_FIRST = (2, 1, 3, 0)


def partner(me, k, n, back=False):
    if n & (n - 1):
        return (me + (n - k if back else k)) % n
    found, bit = 0, 1
    while bit < n:
        mine = (me // bit) % 2
        found = found + (bit * (1 - mine) if k & bit else bit * mine)
        bit *= 2
    return found


def kernel(
    tp, dp, chans,
    stream_hbm, gain_hbm, w_in_hbm, lam_re_hbm, lam_im_hbm, log_dt_hbm, b_re_hbm, b_im_hbm, c_re_hbm, c_im_hbm, skip_hbm,
    w_val_hbm, w_gate_hbm, state_hbm,
    out_ref, state,
    stream_ref, gain_ref, lam_re_ref, lam_im_ref, log_dt_ref, skip_ref, own_w, b_re, b_im, c_re, c_im, drive, read,
    kept, proj, u_keep, masked, from_old, mix_w,
    x_all, near_in, mix_all, near_own, near_send, near_recv, comb_send, comb_own, comb_recv,
    gain_all, col_in, col_out, far_in, x_far, swap_send, swap_recv, u_send, u_recv, mix_far, out_send, out_recv,
    small_sem, load_sem, x_ss, x_rs, in_ss, in_rs, mix_ss, mix_rs, near_ss, near_rs, comb_ss, comb_rs,
    gain_ss, gain_rs, col_ss, col_rs, row_ss, row_rs, xf_ss, xf_rs, swap_ss, swap_rs, u_ss, u_rs, mf_ss, mf_rs, of_ss, of_rs,
):
    layers = w_in_hbm.shape[0]
    me_t, me_d = lax.axis_index("tp"), lax.axis_index("dp")
    rows_t, feats = stream_ref.shape
    rows_d, width = u_keep.shape
    per = rows_d // rows_t
    groups, half = lam_re_ref.shape[1:]
    lanes = state.shape[2]
    me_z, me_y = me_t // per, me_t % per

    barrier = pltpu.get_barrier_semaphore()

    def greet(t, d):
        pl.semaphore_signal(barrier, inc=1, device_id={"tp": t, "dp": d}, device_id_type=pl.DeviceIdType.MESH)

    @pl.when(me_z != me_d)
    def _():
        for k in range(dp):
            for j in range(per):
                greet(me_d * per + j, partner(me_d, k, dp))

    for k in range(1, dp):
        greet(partner(me_z, k, dp) * per + me_y, me_d)
    for k in range(dp):
        for j in range(per):
            if k or j:
                greet(me_z * per + partner(me_y, j, per), partner(me_d, k, dp))

    smalls = []
    for i, (src, dst) in enumerate(
        (
            (stream_hbm, stream_ref), (gain_hbm, gain_ref), (lam_re_hbm, lam_re_ref), (lam_im_hbm, lam_im_ref),
            (log_dt_hbm, log_dt_ref), (skip_hbm, skip_ref),
        )
    ):
        smalls.append(pltpu.make_async_copy(src, dst, small_sem.at[i]))
        smalls[i].start()
    loads = {}
    for l in range(layers):
        weights = (
            [own_w.at[i] for i in range(3)] if l == 0 else [col_in.at[me_z], col_out.at[me_z, 0], col_out.at[me_z, 1]]
        )
        for i, (src, dst) in enumerate(
            (
                (b_re_hbm, b_re.at[l]), (b_im_hbm, b_im.at[l]), (c_re_hbm, c_re.at[l]), (c_im_hbm, c_im.at[l]),
                (state_hbm, state.at[l]), (w_in_hbm, weights[0]), (w_val_hbm, weights[1]), (w_gate_hbm, weights[2]),
            )
        ):
            loads[l, i] = pltpu.make_async_copy(src.at[l], dst, load_sem.at[l, i])
            loads[l, i].start()

    def send(src, dst, ss, rs, t, d):
        return pltpu.make_async_remote_copy(
            src_ref=src, dst_ref=dst, send_sem=ss, recv_sem=rs, device_id={"tp": t, "dp": d},
            device_id_type=pl.DeviceIdType.MESH,
        )

    def x_copy(t):
        return send(stream_ref, x_all.at[me_d, me_y], x_ss.at[t], x_rs.at[me_d, me_y], t, me_z)

    def in_copy(to):
        return send(own_w.at[0], near_in.at[me_d], in_ss.at[to], in_rs.at[me_d], me_t, to)

    def mix_copy(to):
        return send(mix_all.at[me_d], mix_all.at[me_d], mix_ss.at[to], mix_rs.at[me_d], me_t, to)

    def near_copy(z, y):
        return send(
            near_send.at[z, y], near_recv.at[z, me_y], near_ss.at[z, y], near_rs.at[z, me_y], me_z * per + y, me_d
        )

    def comb_copy(z):
        return send(comb_send.at[z], comb_recv.at[me_z], comb_ss.at[z], comb_rs.at[me_z], z * per + me_y, me_d)

    def gain_copy(to):
        return send(gain_all.at[me_d], gain_all.at[me_d], gain_ss.at[to], gain_rs.at[me_d], me_t, to)

    def col_part(what, home, side, i):
        if what:
            return col_out.at[home, :, pl.ds(side * (width // 2), width // 2)] if i == 4 else col_out.at[home]
        return col_in.at[home, pl.ds(side * (width // 2), width // 2)] if i == 4 else col_in.at[home]

    def col_copy(what, side, i):
        sign = 1 - 2 * side
        home = lax.rem(me_z - sign * min(i - 1, 2) + 2 * dp, dp)
        to = lax.rem(me_z + sign * (2 if i == 4 else 1) + dp, dp)
        part = col_part(what, home, side, i)
        return send(part, part, col_ss.at[what, side, i - 1], col_rs.at[what, side, i - 1], to * per + me_y, me_d)

    def col_start(what, *hops):
        for i in hops:
            for side in range(2):
                col_copy(what, side, i).start()

    def col_wait(what, *hops):
        for i in hops:
            for side in range(2):
                home = lax.rem(me_z - (1 - 2 * side) * i + 2 * dp, dp)
                arrival(col_part(what, home, side, i), col_rs.at[what, side, i - 1]).wait_recv()

    def row_copy(z):
        return send(col_in.at[z], far_in.at[me_d], row_ss.at[z], row_rs.at[me_d], me_t, z)

    def mf_copy(to):
        return send(mix_far.at[me_d], mix_far.at[me_d], mf_ss.at[to], mf_rs.at[me_d], me_t, to)

    def xf_copy(y, d):
        return send(x_far.at[me_d, me_y], x_far.at[me_d, me_y], xf_ss.at[d, y], xf_rs.at[me_d, me_y], me_z * per + y, d)

    def of_copy(y):
        return send(out_send.at[y], out_recv.at[me_y], of_ss.at[y], of_rs.at[me_y], me_z * per + y, me_d)

    def swap_copy():
        return send(swap_send, swap_recv, swap_ss, swap_rs, me_d * per + me_y, me_z)

    def u_copy():
        return send(u_send, u_recv, u_ss, u_rs, me_d * per + me_y, me_z)

    def arrival(ref, rs):
        return send(ref, ref, rs, rs, 0, 0)

    lane_group = lax.broadcasted_iota(jnp.int32, (rows_d, width), 1) // chans
    group_eye = lax.broadcasted_iota(jnp.int32, (groups, groups), 0) == lax.broadcasted_iota(jnp.int32, (groups, groups), 1)
    wide_0 = lax.broadcasted_iota(jnp.int32, (width, width), 0)
    wide_1 = lax.broadcasted_iota(jnp.int32, (width, width), 1)

    def prepare(l):
        step_size = jnp.exp(jnp.sum(jnp.where(group_eye, log_dt_ref[l : l + 1, :], 0.0), axis=1, keepdims=True))
        lam_re, lam_im = lam_re_ref[l], lam_im_ref[l]
        decay = jnp.exp(lam_re * step_size)
        angle = lam_im * step_size
        keep_re = decay * jnp.cos(angle)
        keep_im = decay * jnp.sin(angle)
        denom = lam_re * lam_re + lam_im * lam_im
        ratio_re = ((keep_re - 1.0) * lam_re + keep_im * lam_im) / denom
        ratio_im = (keep_im * lam_re - (keep_re - 1.0) * lam_im) / denom
        keep_a = jnp.concatenate([keep_re, keep_re], axis=1)
        keep_b = jnp.concatenate([-keep_im, keep_im], axis=1)
        for i in range(5):
            loads[l, i].wait()
        for g in range(groups):
            t_re, t_im = b_re[l, g], b_im[l, g]
            r_re, r_im = ratio_re[g : g + 1, :], ratio_im[g : g + 1, :]
            drive[l, pl.ds(g * chans, chans), :] = jnp.concatenate(
                [r_re * t_re - r_im * t_im, r_re * t_im + r_im * t_re], axis=1
            )
        read[l] = jnp.concatenate([c_re[l].reshape(width, half), -c_im[l].reshape(width, half)], axis=1)
        for g in range(groups):
            old = state[l, pl.ds(g, rows_d, stride=groups), :]
            kept[l, pl.ds(g * rows_d, rows_d), :] = (
                keep_a[g : g + 1, :] * old + keep_b[g : g + 1, :] * pltpu.roll(old, lanes // 2, 1)
            )
        proj[...] = lax.dot_general(kept[l], read[l], NT, precision=HIGHEST, preferred_element_type=F32)
        total = jnp.zeros((rows_d, width), F32)
        for g in range(groups):
            total = jnp.where(lane_group == g, proj[pl.ds(g * rows_d, rows_d), :], total)
        full = lax.dot_general(drive[l], read[l], NT, precision=HIGHEST, preferred_element_type=F32)
        mixer = jnp.where(wide_0 // chans == wide_1 // chans, full, 0.0)
        mixer = mixer + jnp.where(wide_0 == wide_1, skip_ref[l : l + 1, :], 0.0)
        return total, mixer

    def update(l, u):
        for g in range(groups):
            masked[pl.ds(g * rows_d, rows_d), :] = jnp.where(lane_group == g, u, 0.0)
        kept[l] = kept[l] + jnp.dot(masked[...], drive[l], precision=HIGHEST, preferred_element_type=F32)
        for g in range(groups):
            state[l, pl.ds(g, rows_d, stride=groups), :] = kept[l, pl.ds(g * rows_d, rows_d), :]

    pl.semaphore_wait(barrier, per * dp - 1 + dp - 1 + (dp - 1) * per)

    smalls[0].wait()
    for k in reversed(range(1, tp)):
        x_copy(partner(me_t, k, tp)).start()

    @pl.when(me_z != me_d)
    def _():
        x_copy(me_t).start()

    @pl.when(me_z == me_d)
    def _():
        x_all[me_d, me_y] = stream_ref[...]

    smalls[1].wait()
    for l in range(layers):
        gain_all[me_d, l] = jnp.broadcast_to(gain_ref[l : l + 1, :], (rows_t, feats))
    loads[0, 5].wait()
    for k in reversed(range(1, dp)):
        gain_copy(partner(me_d, k, dp)).start()
        in_copy(partner(me_d, k, dp)).start()
    loads[1, 5].wait()
    col_start(0, 1)
    for small in smalls[2:]:
        small.wait()
    from_old[...], mix_w[...] = prepare(0)

    acc = jnp.zeros((rows_d, width), F32)
    squares = jnp.zeros((rows_d, feats), F32)
    for k in reversed(PLANE_FAR_FIRST):
        if k == 7:
            col_wait(0, 1)
            col_start(0, 2)
        by = partner(me_d, k, dp, True)
        if k:
            arrival(gain_all.at[by], gain_rs.at[by]).wait_recv()
            arrival(near_in.at[by], in_rs.at[by]).wait_recv()
        for j in range(per):
            y = partner(me_y, j, per)
            if k or j:
                arrival(x_all.at[by, y], x_rs.at[by, y]).wait_recv()
            else:

                @pl.when(me_z != me_d)
                def _():
                    arrival(x_all.at[by, y], x_rs.at[by, y]).wait_recv()

        weights = near_in.at[by] if k else own_w.at[0]
        x = x_all[by].astype(F32)
        normed = (x * gain_all[by, 0][None]).astype(BF16).reshape(rows_d, feats)
        x = x.reshape(rows_d, feats)
        squares = squares + x * x
        acc = acc + lax.dot_general(normed, weights[...], NT, preferred_element_type=F32)
    u = lax.rsqrt(jnp.sum(squares, axis=1, keepdims=True) / (feats * dp) + EPS) * acc
    u_keep[...] = u
    pre = from_old[...] + jnp.dot(u, mix_w[...], precision=HIGHEST, preferred_element_type=F32)
    mix_all[me_d] = jax.nn.gelu(pre).astype(BF16)
    for k in reversed(range(1, dp)):
        mix_copy(partner(me_d, k, dp)).start()
    loads[1, 6].wait()
    loads[1, 7].wait()
    col_start(1, 1)
    loads[0, 6].wait()
    loads[0, 7].wait()
    for k in range(dp):
        if k == 2:
            col_wait(0, 2)
            col_start(0, 3, 4)
        by = partner(me_d, k, dp, True)
        if k:
            arrival(mix_all.at[by], mix_rs.at[by]).wait_recv()
        mixed = mix_all[by]
        value = jnp.dot(mixed, own_w[1], preferred_element_type=F32)
        gate = jnp.dot(mixed, own_w[2], preferred_element_type=F32)
        near_own[by, :, :, :feats] = value.reshape(per, rows_t, feats)
        near_own[by, :, :, feats:] = gate.reshape(per, rows_t, feats)
        near_send[by, :, :, :feats] = value.astype(BF16).reshape(per, rows_t, feats)
        near_send[by, :, :, feats:] = gate.astype(BF16).reshape(per, rows_t, feats)
        for j in ROW_FAR_FIRST:
            if j:
                near_copy(by, partner(me_y, j, per)).start()

    def gather_near(k):
        z = partner(me_d, k, dp, True)
        total = near_own[z, me_y]
        for j in range(1, per):
            y = partner(me_y, j, per)
            arrival(near_recv.at[z, y], near_rs.at[z, y]).wait_recv()
            total = total + near_recv[z, y].astype(F32)

        @pl.when(z != me_z)
        def _():
            comb_send[z] = total.astype(BF16)
            comb_copy(z).start()

        @pl.when(z == me_z)
        def _():
            comb_own[...] = total

    for k in range(4):
        gather_near(k)
    col_wait(1, 1)
    col_start(1, 2)
    update(0, u_keep[...])
    total, mixer = prepare(1)
    swap_send[:rows_d] = jnp.concatenate([total, total], axis=1)
    swap_send[rows_d:] = jnp.concatenate([mixer, mixer], axis=1)

    @pl.when(me_z != me_d)
    def _():
        swap_copy().start()

    @pl.when(me_z == me_d)
    def _():
        swap_recv[...] = swap_send[...]

    for k in range(4, dp):
        gather_near(k)
    for k in range(1, tp):
        x_copy(partner(me_t, k, tp)).wait_send()

    @pl.when(me_z != me_d)
    def _():
        x_copy(me_t).wait_send()

    for k in range(1, dp):
        to = partner(me_d, k, dp)
        in_copy(to).wait_send()
        mix_copy(to).wait_send()
        gain_copy(to).wait_send()
    for side in range(2):
        for i in range(1, 5):
            col_copy(0, side, i).wait_send()

    col_wait(0, 3, 4)
    for k in reversed(range(1, dp)):
        row_copy(partner(me_d, k, dp)).start()
    combined = comb_own[...]
    for k in range(1, dp):
        by = partner(me_z, k, dp, True)
        arrival(comb_recv.at[by], comb_rs.at[by]).wait_recv()
        combined = combined + comb_recv[by].astype(F32)
    fresh = (stream_ref[...].astype(F32) + combined[:, :feats] * jax.nn.sigmoid(combined[:, feats:])).astype(BF16)

    x_far[me_d, me_y] = fresh
    for k in PLANE_FAR_FIRST:
        for j in ROW_FAR_FIRST:
            if k or j:
                xf_copy(partner(me_y, j, per), partner(me_d, k, dp)).start()
    col_wait(1, 2)
    col_start(1, 3, 4)
    for k in range(1, dp):
        comb_copy(partner(me_z, k, dp)).wait_send()
    for k in range(dp):
        for j in range(1, per):
            near_copy(k, partner(me_y, j, per)).wait_send()

    @pl.when(me_z != me_d)
    def _():
        swap_copy().wait_send()

    acc = jnp.zeros((rows_d, width), F32)
    squares = jnp.zeros((rows_d, feats), F32)
    for k in reversed(PLANE_FAR_FIRST):
        by = partner(me_d, k, dp, True)
        if k:
            arrival(far_in.at[by], row_rs.at[by]).wait_recv()
        weights = far_in.at[by] if k else col_in.at[me_d]
        for j in reversed(ROW_FAR_FIRST):
            if k or j:
                y = partner(me_y, j, per)
                arrival(x_far.at[by, y], xf_rs.at[by, y]).wait_recv()
        x = x_far[by].astype(F32)
        normed = (x * gain_all[by, 1][None]).astype(BF16).reshape(rows_d, feats)
        x = x.reshape(rows_d, feats)
        squares = squares + x * x
        acc = acc + lax.dot_general(normed, weights[...], NT, preferred_element_type=F32)
    u = lax.rsqrt(jnp.sum(squares, axis=1, keepdims=True) / (feats * dp) + EPS) * acc
    u_send[...] = jnp.concatenate([u, u], axis=1)

    @pl.when(me_z != me_d)
    def _():
        u_copy().start()
        arrival(swap_recv, swap_rs).wait_recv()

    @pl.when(me_z == me_d)
    def _():
        u_recv[...] = u_send[...]

    pre = swap_recv[:rows_d, :width] + jnp.dot(
        u, swap_recv[rows_d:, :width], precision=HIGHEST, preferred_element_type=F32
    )
    mix_far[me_d] = jax.nn.gelu(pre).astype(BF16)
    for k in PLANE_FAR_FIRST:
        if k:
            mf_copy(partner(me_d, k, dp)).start()
    col_wait(1, 3, 4)
    for k in range(dp):
        for j in range(per):
            if k or j:
                xf_copy(partner(me_y, j, per), partner(me_d, k, dp)).wait_send()
    for k in range(1, dp):
        row_copy(partner(me_d, k, dp)).wait_send()
    for side in range(2):
        for i in range(1, 5):
            col_copy(1, side, i).wait_send()
    value = jnp.zeros((rows_d, feats), F32)
    gate = jnp.zeros((rows_d, feats), F32)
    for k in reversed(PLANE_FAR_FIRST):
        by = partner(me_d, k, dp, True)
        if k:
            arrival(mix_far.at[by], mf_rs.at[by]).wait_recv()
        mixed = mix_far[by]
        value = value + jnp.dot(mixed, col_out[by, 0], preferred_element_type=F32)
        gate = gate + jnp.dot(mixed, col_out[by, 1], preferred_element_type=F32)
    near_own[0, :, :, :feats] = value.reshape(per, rows_t, feats)
    near_own[0, :, :, feats:] = gate.reshape(per, rows_t, feats)
    out_send[:, :, :feats] = value.astype(BF16).reshape(per, rows_t, feats)
    out_send[:, :, feats:] = gate.astype(BF16).reshape(per, rows_t, feats)
    for j in ROW_FAR_FIRST:
        if j:
            of_copy(partner(me_y, j, per)).start()

    @pl.when(me_z != me_d)
    def _():
        arrival(u_recv, u_rs).wait_recv()

    update(1, u_recv[:, :width])
    combined = near_own[0, me_y]
    for j in reversed(ROW_FAR_FIRST):
        if j:
            y = partner(me_y, j, per)
            arrival(out_recv.at[y], of_rs.at[y]).wait_recv()
            combined = combined + out_recv[y].astype(F32)
    out_ref[...] = (
        x_far[me_d, me_y].astype(F32) + combined[:, :feats] * jax.nn.sigmoid(combined[:, feats:])
    ).astype(BF16)

    for k in range(1, dp):
        mf_copy(partner(me_d, k, dp)).wait_send()
    for j in range(1, per):
        of_copy(partner(me_y, j, per)).wait_send()

    @pl.when(me_z != me_d)
    def _():
        u_copy().wait_send()


def per_device(
    tp, dp,
    stream, norm_gain, w_input, lam_re, lam_im, log_dt, b_re, b_im, readout_real, readout_imaginary, d_skip,
    w_val, w_gate, state,
):
    layers, feats, width = w_input.shape
    rows_t = stream.shape[0]
    rows_d, groups, lanes = state.shape[1:]
    chans = b_re.shape[-1]
    per = rows_d // rows_t

    turned_in = w_input.swapaxes(1, 2)
    turned_re, turned_im = b_re.swapaxes(2, 3), b_im.swapaxes(2, 3)

    limit = 67043328 - 4 * layers * rows_d * groups * lanes - (256 << 10)
    vmem = pl.BlockSpec(memory_space=pltpu.VMEM)
    hbm = pl.BlockSpec(memory_space=pltpu.HBM)
    dma = lambda *shape: pltpu.SemaphoreType.DMA(shape)
    out, states = pl.pallas_call(
        functools.partial(kernel, tp, dp, chans),
        out_shape=(pltpu.VMEM(stream.shape, BF16), pltpu.VMEM((layers, rows_d * groups, lanes), F32)),
        in_specs=[hbm] * 14,
        out_specs=(vmem, vmem),
        scratch_shapes=[
            pltpu.VMEM(stream.shape, BF16),
            pltpu.VMEM(norm_gain.shape, F32),
            pltpu.VMEM(lam_re.shape, F32),
            pltpu.VMEM(lam_im.shape, F32),
            pltpu.VMEM(log_dt.shape, F32),
            pltpu.VMEM(d_skip.shape, F32),
            pltpu.VMEM((3, width, feats), BF16),
            pltpu.VMEM(turned_re.shape, F32),
            pltpu.VMEM(turned_im.shape, F32),
            pltpu.VMEM(readout_real.shape, F32),
            pltpu.VMEM(readout_imaginary.shape, F32),
            pltpu.VMEM((layers, width, lanes), F32),
            pltpu.VMEM((layers, width, lanes), F32),
            pltpu.VMEM((layers, rows_d * groups, lanes), F32),
            pltpu.VMEM((rows_d * groups, width), F32),
            pltpu.VMEM((rows_d, width), F32),
            pltpu.VMEM((rows_d * groups, width), F32),
            pltpu.VMEM((rows_d, width), F32),
            pltpu.VMEM((width, width), F32),
            pltpu.VMEM((dp, per, rows_t, feats), BF16),
            pltpu.VMEM((dp, width, feats), BF16),
            pltpu.VMEM((dp, rows_d, width), BF16),
            pltpu.VMEM((dp, per, rows_t, 2 * feats), F32),
            pltpu.VMEM((dp, per, rows_t, 2 * feats), BF16),
            pltpu.VMEM((dp, per, rows_t, 2 * feats), BF16),
            pltpu.VMEM((dp, rows_t, 2 * feats), BF16),
            pltpu.VMEM((rows_t, 2 * feats), F32),
            pltpu.VMEM((dp, rows_t, 2 * feats), BF16),
            pltpu.VMEM((dp, layers, rows_t, feats), F32),
            pltpu.VMEM((dp, width, feats), BF16),
            pltpu.VMEM((dp, 2, width, feats), BF16),
            pltpu.VMEM((dp, width, feats), BF16),
            pltpu.VMEM((dp, per, rows_t, feats), BF16),
            pltpu.VMEM((rows_d + width, 128), F32),
            pltpu.VMEM((rows_d + width, 128), F32),
            pltpu.VMEM((rows_d, 128), F32),
            pltpu.VMEM((rows_d, 128), F32),
            pltpu.VMEM((dp, rows_d, width), BF16),
            pltpu.VMEM((per, rows_t, 2 * feats), BF16),
            pltpu.VMEM((per, rows_t, 2 * feats), BF16),
            dma(6), dma(layers, 8),
            dma(tp), dma(dp, per),
            dma(dp), dma(dp),
            dma(dp), dma(dp),
            dma(dp, per), dma(dp, per),
            dma(dp), dma(dp),
            dma(dp), dma(dp),
            dma(2, 2, 4), dma(2, 2, 4),
            dma(dp), dma(dp),
            dma(dp, per), dma(dp, per),
            pltpu.SemaphoreType.DMA, pltpu.SemaphoreType.DMA,
            pltpu.SemaphoreType.DMA, pltpu.SemaphoreType.DMA,
            dma(dp), dma(dp),
            dma(per), dma(per),
        ],
        compiler_params=pltpu.CompilerParams(collective_id=0, has_side_effects=True, vmem_limit_bytes=limit),
    )(
        stream, norm_gain, turned_in, lam_re, lam_im, log_dt, turned_re, turned_im, readout_real,
        readout_imaginary, d_skip, w_val, w_gate,
        state.reshape(layers, rows_d * groups, lanes),
    )
    return out, states.reshape(state.shape)


def solution(mesh):
    return jax.shard_map(
        functools.partial(per_device, mesh.shape["tp"], mesh.shape["dp"]),
        mesh=mesh,
        in_specs=(
            P("tp", "dp"),
            P(None, "dp"),
            P(None, "dp", "tp"),
            P(None, "tp", None),
            P(None, "tp", None),
            P(None, "tp"),
            P(None, "tp", None, None),
            P(None, "tp", None, None),
            P(None, "tp", None, None),
            P(None, "tp", None, None),
            P(None, "tp"),
            P(None, "tp", "dp"),
            P(None, "tp", "dp"),
            P(None, "dp", "tp", None),
        ),
        out_specs=(P("tp", "dp"), P(None, "dp", "tp", None)),
        check_vma=False,
    )
```

```python
import functools

import jax
import jax.numpy as jnp
from jax import lax
from jax.experimental import pallas as pl
from jax.experimental.pallas import tpu as pltpu
from jax.sharding import PartitionSpec as P

EPS = 1e-06
F32 = jnp.float32
BF16 = jnp.bfloat16
HIGHEST = lax.Precision.HIGHEST
NT = (((1,), (1,)), ((), ()))
PLANE_FAR_FIRST = (4, 5, 6, 7, 2, 3, 1, 0)
ROW_FAR_FIRST = (2, 1, 3, 0)


def partner(me, k, n, back=False):
    if n & (n - 1):
        return (me + (n - k if back else k)) % n
    found, bit = 0, 1
    while bit < n:
        mine = (me // bit) % 2
        found = found + (bit * (1 - mine) if k & bit else bit * mine)
        bit *= 2
    return found


def kernel(
    tp, dp, chans,
    stream_hbm, gain_hbm, w_in_hbm, lam_re_hbm, lam_im_hbm, log_dt_hbm, b_re_hbm, b_im_hbm, c_re_hbm, c_im_hbm, skip_hbm,
    w_val_hbm, w_gate_hbm, state_hbm,
    out_ref, state,
    stream_ref, gain_ref, lam_re_ref, lam_im_ref, log_dt_ref, skip_ref, own_w, b_re, b_im, c_re, c_im, drive, read,
    kept, proj, u_keep, masked, from_old, mix_w,
    x_all, near_in, mix_all, near_own, near_send, near_recv, comb_send, comb_own, comb_recv,
    gain_all, col_in, col_out, far_in, x_far, swap_send, swap_recv, u_send, u_recv, mix_far, out_send, out_recv,
    small_sem, load_sem, x_ss, x_rs, in_ss, in_rs, mix_ss, mix_rs, near_ss, near_rs, comb_ss, comb_rs,
    gain_ss, gain_rs, col_ss, col_rs, row_ss, row_rs, xf_ss, xf_rs, swap_ss, swap_rs, u_ss, u_rs, mf_ss, of_ss, of_rs,
):
    layers = w_in_hbm.shape[0]
    me_t, me_d = lax.axis_index("tp"), lax.axis_index("dp")
    rows_t, feats = stream_ref.shape
    rows_d, width = u_keep.shape
    per = rows_d // rows_t
    groups, half = lam_re_ref.shape[1:]
    lanes = state.shape[2]
    me_z, me_y = me_t // per, me_t % per

    barrier = pltpu.get_barrier_semaphore()

    def greet(t, d):
        pl.semaphore_signal(barrier, inc=1, device_id={"tp": t, "dp": d}, device_id_type=pl.DeviceIdType.MESH)

    @pl.when(me_z != me_d)
    def _():
        for k in range(dp):
            for j in range(per):
                greet(me_d * per + j, partner(me_d, k, dp))

    for k in range(1, dp):
        greet(partner(me_z, k, dp) * per + me_y, me_d)
    for k in range(dp):
        for j in range(per):
            if k or j:
                greet(me_z * per + partner(me_y, j, per), partner(me_d, k, dp))

    smalls = []
    for i, (src, dst) in enumerate(
        (
            (stream_hbm, stream_ref), (gain_hbm, gain_ref), (lam_re_hbm, lam_re_ref), (lam_im_hbm, lam_im_ref),
            (log_dt_hbm, log_dt_ref), (skip_hbm, skip_ref),
        )
    ):
        smalls.append(pltpu.make_async_copy(src, dst, small_sem.at[i]))
        smalls[i].start()
    loads = {}
    for i, (src, dst) in enumerate(
        (
            (w_in_hbm.at[0], own_w.at[0]), (w_in_hbm.at[1], col_in.at[me_z]), (b_re_hbm, b_re), (b_im_hbm, b_im),
            (c_re_hbm, c_re), (c_im_hbm, c_im), (state_hbm, state), (w_val_hbm.at[0], own_w.at[1]),
            (w_gate_hbm.at[0], own_w.at[2]), (w_val_hbm.at[1], col_out.at[me_z, 0]),
            (w_gate_hbm.at[1], col_out.at[me_z, 1]),
        )
    ):
        loads[i] = pltpu.make_async_copy(src, dst, load_sem.at[i])
        loads[i].start()

    def send(src, dst, ss, rs, t, d):
        return pltpu.make_async_remote_copy(
            src_ref=src, dst_ref=dst, send_sem=ss, recv_sem=rs, device_id={"tp": t, "dp": d},
            device_id_type=pl.DeviceIdType.MESH,
        )

    def x_copy(t):
        return send(stream_ref, x_all.at[me_d * per + me_y], x_ss, x_rs.at[me_d], t, me_z)

    def in_copy(to):
        return send(own_w.at[0], near_in.at[me_d], in_ss, in_rs, me_t, to)

    def mix_copy(to):
        return send(mix_all.at[me_d], mix_all.at[me_d], mix_ss, mix_rs.at[me_d], me_t, to)

    def near_copy(z, y):
        return send(
            near_send.at[z, y], near_recv.at[z, me_y], near_ss, near_rs.at[z], me_z * per + y, me_d
        )

    def comb_copy(z):
        return send(comb_send.at[z], comb_recv.at[me_z], comb_ss, comb_rs, z * per + me_y, me_d)

    def gain_copy(to):
        return send(gain_all.at[me_d], gain_all.at[me_d], gain_ss, gain_rs, me_t, to)

    def col_part(what, home, side, i):
        if what:
            return col_out.at[home, :, pl.ds(side * (width // 2), width // 2)] if i == 4 else col_out.at[home]
        return col_in.at[home, pl.ds(side * (width // 2), width // 2)] if i == 4 else col_in.at[home]

    def col_copy(what, side, i):
        sign = 1 - 2 * side
        home = lax.rem(me_z - sign * min(i - 1, 2) + 2 * dp, dp)
        to = lax.rem(me_z + sign * (2 if i == 4 else 1) + dp, dp)
        part = col_part(what, home, side, i)
        return send(part, part, col_ss.at[what], col_rs.at[what, min(i, 3) - 1], to * per + me_y, me_d)

    def col_start(what, *hops):
        for i in hops:
            for side in range(2):
                col_copy(what, side, i).start()

    def col_wait(what, hop):
        blocks = pl.ds(0, 3 if hop == 3 else 2)
        arrival((col_out if what else col_in).at[blocks], col_rs.at[what, hop - 1]).wait_recv()

    def row_copy(z):
        return send(col_in.at[z], far_in.at[me_d], row_ss, row_rs, me_t, z)

    def mf_copy(to):
        return send(mix_far.at[me_d], mix_far.at[me_d], mf_ss, mix_rs.at[me_d], me_t, to)

    def xf_copy(y, d):
        mine = x_far.at[me_d * per + me_y]
        return send(mine, mine, xf_ss, xf_rs.at[me_d], me_z * per + y, d)

    def of_copy(y):
        return send(out_send.at[y], out_recv.at[me_y], of_ss, of_rs, me_z * per + y, me_d)

    def swap_copy():
        return send(swap_send, swap_recv, swap_ss, swap_rs, me_d * per + me_y, me_z)

    def u_copy():
        return send(u_send, u_recv, u_ss, u_rs, me_d * per + me_y, me_z)

    def arrival(ref, rs):
        return send(ref, ref, rs, rs, 0, 0)

    def sent(ref, ss):
        send(ref, ref, ss, ss, 0, 0).wait_send()

    lane_group = lax.broadcasted_iota(jnp.int32, (rows_d, width), 1) // chans
    group_eye = lax.broadcasted_iota(jnp.int32, (groups, groups), 0) == lax.broadcasted_iota(jnp.int32, (groups, groups), 1)
    wide_0 = lax.broadcasted_iota(jnp.int32, (width, width), 0)
    wide_1 = lax.broadcasted_iota(jnp.int32, (width, width), 1)

    def prepare(l):
        step_size = jnp.exp(jnp.sum(jnp.where(group_eye, log_dt_ref[l : l + 1, :], 0.0), axis=1, keepdims=True))
        lam_re, lam_im = lam_re_ref[l], lam_im_ref[l]
        decay = jnp.exp(lam_re * step_size)
        angle = lam_im * step_size
        keep_re = decay * jnp.cos(angle)
        keep_im = decay * jnp.sin(angle)
        denom = lam_re * lam_re + lam_im * lam_im
        ratio_re = ((keep_re - 1.0) * lam_re + keep_im * lam_im) / denom
        ratio_im = (keep_im * lam_re - (keep_re - 1.0) * lam_im) / denom
        keep_a = jnp.concatenate([keep_re, keep_re], axis=1)
        keep_b = jnp.concatenate([-keep_im, keep_im], axis=1)
        if l == 0:
            for i in range(2, 7):
                loads[i].wait()
        for g in range(groups):
            t_re, t_im = b_re[l, g], b_im[l, g]
            r_re, r_im = ratio_re[g : g + 1, :], ratio_im[g : g + 1, :]
            drive[l, pl.ds(g * chans, chans), :] = jnp.concatenate(
                [r_re * t_re - r_im * t_im, r_re * t_im + r_im * t_re], axis=1
            )
        read[l] = jnp.concatenate([c_re[l].reshape(width, half), -c_im[l].reshape(width, half)], axis=1)
        for g in range(groups):
            old = state[l, pl.ds(g, rows_d, stride=groups), :]
            kept[l, pl.ds(g * rows_d, rows_d), :] = (
                keep_a[g : g + 1, :] * old + keep_b[g : g + 1, :] * pltpu.roll(old, lanes // 2, 1)
            )
        proj[...] = lax.dot_general(kept[l], read[l], NT, precision=HIGHEST, preferred_element_type=F32)
        total = jnp.zeros((rows_d, width), F32)
        for g in range(groups):
            total = jnp.where(lane_group == g, proj[pl.ds(g * rows_d, rows_d), :], total)
        full = lax.dot_general(drive[l], read[l], NT, precision=HIGHEST, preferred_element_type=F32)
        mixer = jnp.where(wide_0 // chans == wide_1 // chans, full, 0.0)
        mixer = mixer + jnp.where(wide_0 == wide_1, skip_ref[l : l + 1, :], 0.0)
        return total, mixer

    def update(l, u):
        for g in range(groups):
            masked[pl.ds(g * rows_d, rows_d), :] = jnp.where(lane_group == g, u, 0.0)
        kept[l] = kept[l] + jnp.dot(masked[...], drive[l], precision=HIGHEST, preferred_element_type=F32)
        for g in range(groups):
            state[l, pl.ds(g, rows_d, stride=groups), :] = kept[l, pl.ds(g * rows_d, rows_d), :]

    pl.semaphore_wait(barrier, per * dp - 1 + dp - 1 + (dp - 1) * per)

    smalls[0].wait()
    for k in reversed(range(1, tp)):
        x_copy(partner(me_t, k, tp)).start()

    @pl.when(me_z != me_d)
    def _():
        x_copy(me_t).start()

    @pl.when(me_z == me_d)
    def _():
        x_all[me_d * per + me_y] = stream_ref[...]

    smalls[1].wait()
    for l in range(layers):
        gain_all[me_d, l] = jnp.broadcast_to(gain_ref[l : l + 1, :], (rows_t, feats))
    loads[0].wait()
    for k in reversed(range(1, dp)):
        gain_copy(partner(me_d, k, dp)).start()
        in_copy(partner(me_d, k, dp)).start()
    loads[1].wait()
    col_start(0, 1)
    for small in smalls[2:]:
        small.wait()
    from_old[...], mix_w[...] = prepare(0)

    acc = jnp.zeros((rows_d, width), F32)
    squares = jnp.zeros((rows_d, feats), F32)
    for k in reversed(PLANE_FAR_FIRST):
        if k == 7:
            col_wait(0, 1)
            col_start(0, 2)
        by = partner(me_d, k, dp, True)
        if k:
            arrival(x_all.at[pl.ds(0, per)], x_rs.at[by]).wait_recv()
        else:

            @pl.when(me_z != me_d)
            def _():
                arrival(x_all.at[pl.ds(0, per)], x_rs.at[by]).wait_recv()

            @pl.when(me_z == me_d)
            def _():
                arrival(x_all.at[pl.ds(0, per - 1)], x_rs.at[by]).wait_recv()

            arrival(gain_all.at[pl.ds(0, dp - 1)], gain_rs).wait_recv()
            arrival(near_in.at[pl.ds(0, dp - 1)], in_rs).wait_recv()
        weights = near_in.at[by] if k else own_w.at[0]
        x = x_all[pl.ds(by * per, per)].astype(F32)
        normed = (x * gain_all[by, 0][None]).astype(BF16).reshape(rows_d, feats)
        x = x.reshape(rows_d, feats)
        squares = squares + x * x
        acc = acc + lax.dot_general(normed, weights[...], NT, preferred_element_type=F32)
    u = lax.rsqrt(jnp.sum(squares, axis=1, keepdims=True) / (feats * dp) + EPS) * acc
    u_keep[...] = u
    pre = from_old[...] + jnp.dot(u, mix_w[...], precision=HIGHEST, preferred_element_type=F32)
    mix_all[me_d] = jax.nn.gelu(pre).astype(BF16)
    for k in reversed(range(1, dp)):
        mix_copy(partner(me_d, k, dp)).start()
    loads[9].wait()
    loads[10].wait()
    col_start(1, 1)
    loads[7].wait()
    loads[8].wait()
    for k in range(dp):
        if k == 2:
            col_wait(0, 2)
            col_start(0, 3, 4)
        by = partner(me_d, k, dp, True)
        if k:
            arrival(mix_all.at[by], mix_rs.at[by]).wait_recv()
        mixed = mix_all[by]
        value = jnp.dot(mixed, own_w[1], preferred_element_type=F32)
        gate = jnp.dot(mixed, own_w[2], preferred_element_type=F32)
        near_own[by, :, :, :feats] = value.reshape(per, rows_t, feats)
        near_own[by, :, :, feats:] = gate.reshape(per, rows_t, feats)
        near_send[by, :, :, :feats] = value.astype(BF16).reshape(per, rows_t, feats)
        near_send[by, :, :, feats:] = gate.astype(BF16).reshape(per, rows_t, feats)
        for j in ROW_FAR_FIRST:
            if j:
                near_copy(by, partner(me_y, j, per)).start()

    def gather_near(k):
        z = partner(me_d, k, dp, True)
        total = near_own[z, me_y]
        arrival(near_recv.at[z, pl.ds(0, per - 1)], near_rs.at[z]).wait_recv()
        for j in range(1, per):
            total = total + near_recv[z, partner(me_y, j, per)].astype(F32)

        @pl.when(z != me_z)
        def _():
            comb_send[z] = total.astype(BF16)
            comb_copy(z).start()

        @pl.when(z == me_z)
        def _():
            comb_own[...] = total

    for k in range(4):
        gather_near(k)
    col_wait(1, 1)
    col_start(1, 2)
    update(0, u_keep[...])
    total, mixer = prepare(1)
    swap_send[:rows_d] = jnp.concatenate([total, total], axis=1)
    swap_send[rows_d:] = jnp.concatenate([mixer, mixer], axis=1)

    @pl.when(me_z != me_d)
    def _():
        swap_copy().start()

    @pl.when(me_z == me_d)
    def _():
        swap_recv[...] = swap_send[...]

    for k in range(4, dp):
        gather_near(k)
    @pl.when(me_z != me_d)
    def _():
        sent(x_all, x_ss)

    @pl.when(me_z == me_d)
    def _():
        sent(x_all.at[pl.ds(0, tp - 1)], x_ss)

    sent(near_in.at[pl.ds(0, dp - 1)], in_ss)
    sent(mix_all.at[pl.ds(0, dp - 1)], mix_ss)
    sent(gain_all.at[pl.ds(0, dp - 1)], gain_ss)
    sent(col_in.at[pl.ds(0, 7)], col_ss.at[0])
    col_wait(0, 3)
    for k in reversed(range(1, dp)):
        row_copy(partner(me_d, k, dp)).start()
    combined = comb_own[...]
    arrival(comb_recv.at[pl.ds(0, dp - 1)], comb_rs).wait_recv()
    for k in range(1, dp):
        combined = combined + comb_recv[partner(me_z, k, dp)].astype(F32)
    fresh = (stream_ref[...].astype(F32) + combined[:, :feats] * jax.nn.sigmoid(combined[:, feats:])).astype(BF16)

    x_far[me_d * per + me_y] = fresh
    for k in PLANE_FAR_FIRST:
        for j in ROW_FAR_FIRST:
            if k or j:
                xf_copy(partner(me_y, j, per), partner(me_d, k, dp)).start()
    col_wait(1, 2)
    col_start(1, 3, 4)
    sent(comb_send.at[pl.ds(0, dp - 1)], comb_ss)
    sent(near_send.at[:, pl.ds(0, per - 1)], near_ss)

    @pl.when(me_z != me_d)
    def _():
        swap_copy().wait_send()

    acc = jnp.zeros((rows_d, width), F32)
    squares = jnp.zeros((rows_d, feats), F32)
    for k in reversed(PLANE_FAR_FIRST):
        by = partner(me_d, k, dp, True)
        arrival(x_far.at[pl.ds(0, per if k else per - 1)], xf_rs.at[by]).wait_recv()
        if k == 1:
            arrival(far_in.at[pl.ds(0, dp - 1)], row_rs).wait_recv()
        weights = far_in.at[by] if k else col_in.at[me_d]
        x = x_far[pl.ds(by * per, per)].astype(F32)
        normed = (x * gain_all[by, 1][None]).astype(BF16).reshape(rows_d, feats)
        x = x.reshape(rows_d, feats)
        squares = squares + x * x
        acc = acc + lax.dot_general(normed, weights[...], NT, preferred_element_type=F32)
    u = lax.rsqrt(jnp.sum(squares, axis=1, keepdims=True) / (feats * dp) + EPS) * acc
    u_send[...] = jnp.concatenate([u, u], axis=1)

    @pl.when(me_z != me_d)
    def _():
        u_copy().start()
        arrival(swap_recv, swap_rs).wait_recv()

    @pl.when(me_z == me_d)
    def _():
        u_recv[...] = u_send[...]

    pre = swap_recv[:rows_d, :width] + jnp.dot(
        u, swap_recv[rows_d:, :width], precision=HIGHEST, preferred_element_type=F32
    )
    mix_far[me_d] = jax.nn.gelu(pre).astype(BF16)
    for k in PLANE_FAR_FIRST:
        if k:
            mf_copy(partner(me_d, k, dp)).start()
    col_wait(1, 3)
    sent(x_far.at[pl.ds(0, tp - 1)], xf_ss)
    sent(far_in.at[pl.ds(0, dp - 1)], row_ss)
    sent(col_out.at[pl.ds(0, 7)], col_ss.at[1])
    value = jnp.zeros((rows_d, feats), F32)
    gate = jnp.zeros((rows_d, feats), F32)
    for k in reversed(PLANE_FAR_FIRST):
        by = partner(me_d, k, dp, True)
        if k:
            arrival(mix_far.at[by], mix_rs.at[by]).wait_recv()
        mixed = mix_far[by]
        value = value + jnp.dot(mixed, col_out[by, 0], preferred_element_type=F32)
        gate = gate + jnp.dot(mixed, col_out[by, 1], preferred_element_type=F32)
    near_own[0, :, :, :feats] = value.reshape(per, rows_t, feats)
    near_own[0, :, :, feats:] = gate.reshape(per, rows_t, feats)
    out_send[:, :, :feats] = value.astype(BF16).reshape(per, rows_t, feats)
    out_send[:, :, feats:] = gate.astype(BF16).reshape(per, rows_t, feats)
    for j in ROW_FAR_FIRST:
        if j:
            of_copy(partner(me_y, j, per)).start()

    @pl.when(me_z != me_d)
    def _():
        arrival(u_recv, u_rs).wait_recv()

    update(1, u_recv[:, :width])
    combined = near_own[0, me_y]
    arrival(out_recv.at[pl.ds(0, per - 1)], of_rs).wait_recv()
    for j in range(1, per):
        combined = combined + out_recv[partner(me_y, j, per)].astype(F32)
    out_ref[...] = (
        x_far[me_d * per + me_y].astype(F32) + combined[:, :feats] * jax.nn.sigmoid(combined[:, feats:])
    ).astype(BF16)

    sent(mix_far.at[pl.ds(0, dp - 1)], mf_ss)
    sent(out_send.at[pl.ds(0, per - 1)], of_ss)

    @pl.when(me_z != me_d)
    def _():
        u_copy().wait_send()


def per_device(
    tp, dp,
    stream, norm_gain, w_input, lam_re, lam_im, log_dt, b_re, b_im, readout_real, readout_imaginary, d_skip,
    w_val, w_gate, state,
):
    layers, feats, width = w_input.shape
    rows_t = stream.shape[0]
    rows_d, groups, lanes = state.shape[1:]
    chans = b_re.shape[-1]
    per = rows_d // rows_t

    turned_in = w_input.swapaxes(1, 2)
    turned_re, turned_im = b_re.swapaxes(2, 3), b_im.swapaxes(2, 3)

    limit = 67043328 - 4 * layers * rows_d * groups * lanes - (256 << 10)
    vmem = pl.BlockSpec(memory_space=pltpu.VMEM)
    hbm = pl.BlockSpec(memory_space=pltpu.HBM)
    one = pltpu.SemaphoreType.DMA
    dma = lambda *shape: one(shape)
    out, states = pl.pallas_call(
        functools.partial(kernel, tp, dp, chans),
        out_shape=(pltpu.VMEM(stream.shape, BF16), pltpu.VMEM((layers, rows_d * groups, lanes), F32)),
        in_specs=[hbm] * 14,
        out_specs=(vmem, vmem),
        scratch_shapes=[
            pltpu.VMEM(stream.shape, BF16),
            pltpu.VMEM(norm_gain.shape, F32),
            pltpu.VMEM(lam_re.shape, F32),
            pltpu.VMEM(lam_im.shape, F32),
            pltpu.VMEM(log_dt.shape, F32),
            pltpu.VMEM(d_skip.shape, F32),
            pltpu.VMEM((3, width, feats), BF16),
            pltpu.VMEM(turned_re.shape, F32),
            pltpu.VMEM(turned_im.shape, F32),
            pltpu.VMEM(readout_real.shape, F32),
            pltpu.VMEM(readout_imaginary.shape, F32),
            pltpu.VMEM((layers, width, lanes), F32),
            pltpu.VMEM((layers, width, lanes), F32),
            pltpu.VMEM((layers, rows_d * groups, lanes), F32),
            pltpu.VMEM((rows_d * groups, width), F32),
            pltpu.VMEM((rows_d, width), F32),
            pltpu.VMEM((rows_d * groups, width), F32),
            pltpu.VMEM((rows_d, width), F32),
            pltpu.VMEM((width, width), F32),
            pltpu.VMEM((tp, rows_t, feats), BF16),
            pltpu.VMEM((dp, width, feats), BF16),
            pltpu.VMEM((dp, rows_d, width), BF16),
            pltpu.VMEM((dp, per, rows_t, 2 * feats), F32),
            pltpu.VMEM((dp, per, rows_t, 2 * feats), BF16),
            pltpu.VMEM((dp, per, rows_t, 2 * feats), BF16),
            pltpu.VMEM((dp, rows_t, 2 * feats), BF16),
            pltpu.VMEM((rows_t, 2 * feats), F32),
            pltpu.VMEM((dp, rows_t, 2 * feats), BF16),
            pltpu.VMEM((dp, layers, rows_t, feats), F32),
            pltpu.VMEM((dp, width, feats), BF16),
            pltpu.VMEM((dp, 2, width, feats), BF16),
            pltpu.VMEM((dp, width, feats), BF16),
            pltpu.VMEM((tp, rows_t, feats), BF16),
            pltpu.VMEM((rows_d + width, 128), F32),
            pltpu.VMEM((rows_d + width, 128), F32),
            pltpu.VMEM((rows_d, 128), F32),
            pltpu.VMEM((rows_d, 128), F32),
            pltpu.VMEM((dp, rows_d, width), BF16),
            pltpu.VMEM((per, rows_t, 2 * feats), BF16),
            pltpu.VMEM((per, rows_t, 2 * feats), BF16),
            dma(6), dma(11),
            one, dma(dp),
            one, one,
            one, dma(dp),
            one, dma(dp),
            one, one,
            one, one,
            dma(2), dma(2, 3),
            one, one,
            one, dma(dp),
            one, one,
            one, one,
            one, one, one,
        ],
        compiler_params=pltpu.CompilerParams(collective_id=0, has_side_effects=True, vmem_limit_bytes=limit),
    )(
        stream, norm_gain, turned_in, lam_re, lam_im, log_dt, turned_re, turned_im, readout_real,
        readout_imaginary, d_skip, w_val, w_gate,
        state.reshape(layers, rows_d * groups, lanes),
    )
    return out, states.reshape(state.shape)


def solution(mesh):
    return jax.shard_map(
        functools.partial(per_device, mesh.shape["tp"], mesh.shape["dp"]),
        mesh=mesh,
        in_specs=(
            P("tp", "dp"),
            P(None, "dp"),
            P(None, "dp", "tp"),
            P(None, "tp", None),
            P(None, "tp", None),
            P(None, "tp"),
            P(None, "tp", None, None),
            P(None, "tp", None, None),
            P(None, "tp", None, None),
            P(None, "tp", None, None),
            P(None, "tp"),
            P(None, "tp", "dp"),
            P(None, "tp", "dp"),
            P(None, "dp", "tp", None),
        ),
        out_specs=(P("tp", "dp"), P(None, "dp", "tp", None)),
        check_vma=False,
    )
```

```python
import functools

import jax
import jax.numpy as jnp
from jax import lax
from jax.experimental import pallas as pl
from jax.experimental.pallas import tpu as pltpu
from jax.sharding import PartitionSpec as P

EPS = 1e-06
F32 = jnp.float32
BF16 = jnp.bfloat16
HIGHEST = lax.Precision.HIGHEST
NT = (((1,), (1,)), ((), ()))
PLANE_FAR_FIRST = (4, 5, 6, 7, 2, 3, 1, 0)
ROW_FAR_FIRST = (2, 1, 3, 0)


def partner(me, k, n, back=False):
    if n & (n - 1):
        return (me + (n - k if back else k)) % n
    found, bit = 0, 1
    while bit < n:
        mine = (me // bit) % 2
        found = found + (bit * (1 - mine) if k & bit else bit * mine)
        bit *= 2
    return found


def ring_far_first(n, m):
    others = [(a, b) for a in range(n) for b in range(m) if a or b]
    return sorted(others, key=lambda o: -min(o[0], n - o[0]) - min(o[1], m - o[1]))


def kernel(
    tp, dp, chans,
    stream_hbm, gain_hbm, w_in_hbm, lam_re_hbm, lam_im_hbm, log_dt_hbm, b_re_hbm, b_im_hbm, c_re_hbm, c_im_hbm, skip_hbm,
    w_val_hbm, w_gate_hbm, state_hbm,
    out_ref, state,
    stream_ref, gain_ref, lam_re_ref, lam_im_ref, log_dt_ref, skip_ref, own_w, b_re, b_im, c_re, c_im, drive, read,
    kept, proj, u_keep, masked, from_old, mix_w,
    x_all, near_in, mix_all, near_own, near_send, near_recv, comb_send, comb_own, comb_recv,
    gain_all, col_in, col_out, far_in, x_far, swap_send, swap_recv, u_send, u_recv, mix_far, out_send, out_recv,
    small_sem, load_sem, x_ss, x_rs, in_ss, in_rs, mix_ss, mix_rs, near_ss, near_rs, comb_ss, comb_rs,
    gain_ss, gain_rs, col_ss, col_rs, row_ss, row_rs, xf_ss, xf_rs, swap_ss, swap_rs, u_ss, u_rs, mf_ss, of_ss, of_rs,
):
    layers = w_in_hbm.shape[0]
    me_t, me_d = lax.axis_index("tp"), lax.axis_index("dp")
    rows_t, feats = stream_ref.shape
    rows_d, width = u_keep.shape
    per = rows_d // rows_t
    groups, half = lam_re_ref.shape[1:]
    lanes = state.shape[2]
    me_z, me_y = me_t // per, me_t % per

    barrier = pltpu.get_barrier_semaphore()

    def greet(t, d):
        pl.semaphore_signal(barrier, inc=1, device_id={"tp": t, "dp": d}, device_id_type=pl.DeviceIdType.MESH)

    @pl.when(me_z != me_d)
    def _():
        for k in range(dp):
            for j in range(per):
                greet(me_d * per + j, partner(me_d, k, dp))

    for k in range(1, dp):
        greet(partner(me_z, k, dp) * per + me_y, me_d)
    for k in range(dp):
        for j in range(per):
            if k or j:
                greet(me_z * per + partner(me_y, j, per), partner(me_d, k, dp))

    smalls = []
    for i, (src, dst) in enumerate(
        (
            (stream_hbm, stream_ref), (gain_hbm, gain_ref), (lam_re_hbm, lam_re_ref), (lam_im_hbm, lam_im_ref),
            (log_dt_hbm, log_dt_ref), (skip_hbm, skip_ref),
        )
    ):
        smalls.append(pltpu.make_async_copy(src, dst, small_sem.at[i]))
        smalls[i].start()
    loads = {}
    for i, (src, dst) in enumerate(
        (
            (w_in_hbm.at[0], own_w.at[0]), (w_in_hbm.at[1], col_in.at[me_z]), (b_re_hbm, b_re), (b_im_hbm, b_im),
            (c_re_hbm, c_re), (c_im_hbm, c_im), (state_hbm, state), (w_val_hbm.at[0], own_w.at[1]),
            (w_gate_hbm.at[0], own_w.at[2]), (w_val_hbm.at[1], col_out.at[me_z, 0]),
            (w_gate_hbm.at[1], col_out.at[me_z, 1]),
        )
    ):
        loads[i] = pltpu.make_async_copy(src, dst, load_sem.at[i])
        loads[i].start()

    def send(src, dst, ss, rs, t, d):
        return pltpu.make_async_remote_copy(
            src_ref=src, dst_ref=dst, send_sem=ss, recv_sem=rs, device_id={"tp": t, "dp": d},
            device_id_type=pl.DeviceIdType.MESH,
        )

    def x_copy(t):
        return send(stream_ref, x_all.at[me_d * per + me_y], x_ss, x_rs.at[me_d], t, me_z)

    def in_copy(to):
        return send(own_w.at[0], near_in.at[me_d], in_ss, in_rs, me_t, to)

    def mix_copy(to):
        return send(mix_all.at[me_d], mix_all.at[me_d], mix_ss, mix_rs.at[me_d], me_t, to)

    def near_copy(z, y):
        return send(
            near_send.at[z, y], near_recv.at[z, me_y], near_ss, near_rs.at[z], me_z * per + y, me_d
        )

    def comb_copy(z):
        return send(comb_send.at[z], comb_recv.at[me_z], comb_ss, comb_rs, z * per + me_y, me_d)

    def gain_copy(to):
        return send(gain_all.at[me_d], gain_all.at[me_d], gain_ss, gain_rs, me_t, to)

    def col_part(what, home, side, i):
        if what:
            return col_out.at[home, :, pl.ds(side * (width // 2), width // 2)] if i == 4 else col_out.at[home]
        return col_in.at[home, pl.ds(side * (width // 2), width // 2)] if i == 4 else col_in.at[home]

    def col_copy(what, side, i):
        sign = 1 - 2 * side
        home = lax.rem(me_z - sign * min(i - 1, 2) + 2 * dp, dp)
        to = lax.rem(me_z + sign * (2 if i == 4 else 1) + dp, dp)
        part = col_part(what, home, side, i)
        return send(part, part, col_ss.at[what], col_rs.at[what, min(i, 3) - 1], to * per + me_y, me_d)

    def col_start(what, *hops):
        for i in hops:
            for side in range(2):
                col_copy(what, side, i).start()

    def col_wait(what, hop):
        blocks = pl.ds(0, 3 if hop == 3 else 2)
        arrival((col_out if what else col_in).at[blocks], col_rs.at[what, hop - 1]).wait_recv()

    def row_copy(z):
        return send(col_in.at[z], far_in.at[me_d], row_ss, row_rs, me_t, z)

    def mf_copy(to):
        return send(mix_far.at[me_d], mix_far.at[me_d], mf_ss, mix_rs.at[me_d], me_t, to)

    def xf_copy(y, d):
        mine = x_far.at[me_d * per + me_y]
        return send(mine, mine, xf_ss, xf_rs.at[me_d], me_z * per + y, d)

    def of_copy(y):
        return send(out_send.at[y], out_recv.at[me_y], of_ss, of_rs, me_z * per + y, me_d)

    def swap_copy():
        return send(swap_send, swap_recv, swap_ss, swap_rs, me_d * per + me_y, me_z)

    def u_copy():
        return send(u_send, u_recv, u_ss, u_rs, me_d * per + me_y, me_z)

    def arrival(ref, rs):
        return send(ref, ref, rs, rs, 0, 0)

    def sent(ref, ss):
        send(ref, ref, ss, ss, 0, 0).wait_send()

    lane_group = lax.broadcasted_iota(jnp.int32, (rows_d, width), 1) // chans
    group_eye = lax.broadcasted_iota(jnp.int32, (groups, groups), 0) == lax.broadcasted_iota(jnp.int32, (groups, groups), 1)
    wide_0 = lax.broadcasted_iota(jnp.int32, (width, width), 0)
    wide_1 = lax.broadcasted_iota(jnp.int32, (width, width), 1)

    def prepare(l):
        step_size = jnp.exp(jnp.sum(jnp.where(group_eye, log_dt_ref[l : l + 1, :], 0.0), axis=1, keepdims=True))
        lam_re, lam_im = lam_re_ref[l], lam_im_ref[l]
        decay = jnp.exp(lam_re * step_size)
        angle = lam_im * step_size
        keep_re = decay * jnp.cos(angle)
        keep_im = decay * jnp.sin(angle)
        denom = lam_re * lam_re + lam_im * lam_im
        ratio_re = ((keep_re - 1.0) * lam_re + keep_im * lam_im) / denom
        ratio_im = (keep_im * lam_re - (keep_re - 1.0) * lam_im) / denom
        keep_a = jnp.concatenate([keep_re, keep_re], axis=1)
        keep_b = jnp.concatenate([-keep_im, keep_im], axis=1)
        if l == 0:
            for i in range(2, 7):
                loads[i].wait()
        for g in range(groups):
            t_re, t_im = b_re[l, g], b_im[l, g]
            r_re, r_im = ratio_re[g : g + 1, :], ratio_im[g : g + 1, :]
            drive[l, pl.ds(g * chans, chans), :] = jnp.concatenate(
                [r_re * t_re - r_im * t_im, r_re * t_im + r_im * t_re], axis=1
            )
        read[l] = jnp.concatenate([c_re[l].reshape(width, half), -c_im[l].reshape(width, half)], axis=1)
        for g in range(groups):
            old = state[l, pl.ds(g, rows_d, stride=groups), :]
            kept[l, pl.ds(g * rows_d, rows_d), :] = (
                keep_a[g : g + 1, :] * old + keep_b[g : g + 1, :] * pltpu.roll(old, lanes // 2, 1)
            )
        proj[...] = lax.dot_general(kept[l], read[l], NT, precision=HIGHEST, preferred_element_type=F32)
        total = jnp.zeros((rows_d, width), F32)
        for g in range(groups):
            total = jnp.where(lane_group == g, proj[pl.ds(g * rows_d, rows_d), :], total)
        full = lax.dot_general(drive[l], read[l], NT, precision=HIGHEST, preferred_element_type=F32)
        mixer = jnp.where(wide_0 // chans == wide_1 // chans, full, 0.0)
        mixer = mixer + jnp.where(wide_0 == wide_1, skip_ref[l : l + 1, :], 0.0)
        return total, mixer

    def update(l, u):
        for g in range(groups):
            masked[pl.ds(g * rows_d, rows_d), :] = jnp.where(lane_group == g, u, 0.0)
        kept[l] = kept[l] + jnp.dot(masked[...], drive[l], precision=HIGHEST, preferred_element_type=F32)
        for g in range(groups):
            state[l, pl.ds(g, rows_d, stride=groups), :] = kept[l, pl.ds(g * rows_d, rows_d), :]

    pl.semaphore_wait(barrier, per * dp - 1 + dp - 1 + (dp - 1) * per)

    smalls[0].wait()
    for a, b in ring_far_first(dp, per):
        x_copy(lax.rem(me_z + a, dp) * per + lax.rem(me_y + b, per)).start()

    @pl.when(me_z != me_d)
    def _():
        x_copy(me_t).start()

    @pl.when(me_z == me_d)
    def _():
        x_all[me_d * per + me_y] = stream_ref[...]

    smalls[1].wait()
    for l in range(layers):
        gain_all[me_d, l] = jnp.broadcast_to(gain_ref[l : l + 1, :], (rows_t, feats))
    loads[0].wait()
    for k in PLANE_FAR_FIRST:
        if k:
            gain_copy(partner(me_d, k, dp)).start()
            in_copy(partner(me_d, k, dp)).start()
    loads[1].wait()
    col_start(0, 1)
    for small in smalls[2:]:
        small.wait()
    from_old[...], mix_w[...] = prepare(0)

    acc = jnp.zeros((rows_d, width), F32)
    squares = jnp.zeros((rows_d, feats), F32)
    for k in reversed(PLANE_FAR_FIRST):
        if k == 7:
            col_wait(0, 1)
            col_start(0, 2)
        by = partner(me_d, k, dp, True)
        if k:
            arrival(x_all.at[pl.ds(0, per)], x_rs.at[by]).wait_recv()
        else:

            @pl.when(me_z != me_d)
            def _():
                arrival(x_all.at[pl.ds(0, per)], x_rs.at[by]).wait_recv()

            @pl.when(me_z == me_d)
            def _():
                arrival(x_all.at[pl.ds(0, per - 1)], x_rs.at[by]).wait_recv()

            arrival(gain_all.at[pl.ds(0, dp - 1)], gain_rs).wait_recv()
            arrival(near_in.at[pl.ds(0, dp - 1)], in_rs).wait_recv()
        weights = near_in.at[by] if k else own_w.at[0]
        x = x_all[pl.ds(by * per, per)].astype(F32)
        normed = (x * gain_all[by, 0][None]).astype(BF16).reshape(rows_d, feats)
        x = x.reshape(rows_d, feats)
        squares = squares + x * x
        acc = acc + lax.dot_general(normed, weights[...], NT, preferred_element_type=F32)
    u = lax.rsqrt(jnp.sum(squares, axis=1, keepdims=True) / (feats * dp) + EPS) * acc
    u_keep[...] = u
    pre = from_old[...] + jnp.dot(u, mix_w[...], precision=HIGHEST, preferred_element_type=F32)
    mix_all[me_d] = jax.nn.gelu(pre).astype(BF16)
    for k in PLANE_FAR_FIRST:
        if k:
            mix_copy(partner(me_d, k, dp)).start()
    loads[9].wait()
    loads[10].wait()
    col_start(1, 1)
    loads[7].wait()
    loads[8].wait()
    for k in reversed(PLANE_FAR_FIRST):
        if k == 3:
            col_wait(0, 2)
            col_start(0, 3, 4)
        by = partner(me_d, k, dp, True)
        if k:
            arrival(mix_all.at[by], mix_rs.at[by]).wait_recv()
        mixed = mix_all[by]
        value = jnp.dot(mixed, own_w[1], preferred_element_type=F32)
        gate = jnp.dot(mixed, own_w[2], preferred_element_type=F32)
        near_own[by, :, :, :feats] = value.reshape(per, rows_t, feats)
        near_own[by, :, :, feats:] = gate.reshape(per, rows_t, feats)
        near_send[by, :, :, :feats] = value.astype(BF16).reshape(per, rows_t, feats)
        near_send[by, :, :, feats:] = gate.astype(BF16).reshape(per, rows_t, feats)
        for j in ROW_FAR_FIRST:
            if j:
                near_copy(by, partner(me_y, j, per)).start()

    def gather_near(k):
        z = partner(me_d, k, dp, True)
        total = near_own[z, me_y]
        arrival(near_recv.at[z, pl.ds(0, per - 1)], near_rs.at[z]).wait_recv()
        for j in range(1, per):
            total = total + near_recv[z, partner(me_y, j, per)].astype(F32)

        @pl.when(z != me_z)
        def _():
            comb_send[z] = total.astype(BF16)
            comb_copy(z).start()

        @pl.when(z == me_z)
        def _():
            comb_own[...] = total

    gather_near(0)
    gather_near(1)
    update(0, u_keep[...])
    total, mixer = prepare(1)
    swap_send[:rows_d] = jnp.concatenate([total, total], axis=1)
    swap_send[rows_d:] = jnp.concatenate([mixer, mixer], axis=1)

    @pl.when(me_z != me_d)
    def _():
        swap_copy().start()

    @pl.when(me_z == me_d)
    def _():
        swap_recv[...] = swap_send[...]

    for k in reversed(PLANE_FAR_FIRST[:6]):
        gather_near(k)
    col_wait(1, 1)
    col_start(1, 2)
    @pl.when(me_z != me_d)
    def _():
        sent(x_all, x_ss)

    @pl.when(me_z == me_d)
    def _():
        sent(x_all.at[pl.ds(0, tp - 1)], x_ss)

    sent(near_in.at[pl.ds(0, dp - 1)], in_ss)
    sent(mix_all.at[pl.ds(0, dp - 1)], mix_ss)
    sent(gain_all.at[pl.ds(0, dp - 1)], gain_ss)
    sent(col_in.at[pl.ds(0, 7)], col_ss.at[0])
    col_wait(0, 3)
    for k in reversed(range(1, dp)):
        row_copy(partner(me_d, k, dp)).start()
    combined = comb_own[...]
    arrival(comb_recv.at[pl.ds(0, dp - 1)], comb_rs).wait_recv()
    for k in range(1, dp):
        combined = combined + comb_recv[partner(me_z, k, dp)].astype(F32)
    fresh = (stream_ref[...].astype(F32) + combined[:, :feats] * jax.nn.sigmoid(combined[:, feats:])).astype(BF16)

    x_far[me_d * per + me_y] = fresh
    for k in PLANE_FAR_FIRST:
        for j in ROW_FAR_FIRST:
            if k or j:
                xf_copy(partner(me_y, j, per), partner(me_d, k, dp)).start()
    col_wait(1, 2)
    col_start(1, 3, 4)
    sent(comb_send.at[pl.ds(0, dp - 1)], comb_ss)
    sent(near_send.at[:, pl.ds(0, per - 1)], near_ss)

    @pl.when(me_z != me_d)
    def _():
        swap_copy().wait_send()

    acc = jnp.zeros((rows_d, width), F32)
    squares = jnp.zeros((rows_d, feats), F32)
    for k in reversed(PLANE_FAR_FIRST):
        by = partner(me_d, k, dp, True)
        arrival(x_far.at[pl.ds(0, per if k else per - 1)], xf_rs.at[by]).wait_recv()
        if k == 1:
            arrival(far_in.at[pl.ds(0, dp - 1)], row_rs).wait_recv()
        weights = far_in.at[by] if k else col_in.at[me_d]
        x = x_far[pl.ds(by * per, per)].astype(F32)
        normed = (x * gain_all[by, 1][None]).astype(BF16).reshape(rows_d, feats)
        x = x.reshape(rows_d, feats)
        squares = squares + x * x
        acc = acc + lax.dot_general(normed, weights[...], NT, preferred_element_type=F32)
    u = lax.rsqrt(jnp.sum(squares, axis=1, keepdims=True) / (feats * dp) + EPS) * acc
    u_send[...] = jnp.concatenate([u, u], axis=1)

    @pl.when(me_z != me_d)
    def _():
        u_copy().start()
        arrival(swap_recv, swap_rs).wait_recv()

    @pl.when(me_z == me_d)
    def _():
        u_recv[...] = u_send[...]

    pre = swap_recv[:rows_d, :width] + jnp.dot(
        u, swap_recv[rows_d:, :width], precision=HIGHEST, preferred_element_type=F32
    )
    mix_far[me_d] = jax.nn.gelu(pre).astype(BF16)
    for k in PLANE_FAR_FIRST:
        if k:
            mf_copy(partner(me_d, k, dp)).start()
    col_wait(1, 3)
    sent(x_far.at[pl.ds(0, tp - 1)], xf_ss)
    sent(far_in.at[pl.ds(0, dp - 1)], row_ss)
    sent(col_out.at[pl.ds(0, 7)], col_ss.at[1])
    value = jnp.zeros((rows_d, feats), F32)
    gate = jnp.zeros((rows_d, feats), F32)
    for k in reversed(PLANE_FAR_FIRST):
        by = partner(me_d, k, dp, True)
        if k:
            arrival(mix_far.at[by], mix_rs.at[by]).wait_recv()
        mixed = mix_far[by]
        value = value + jnp.dot(mixed, col_out[by, 0], preferred_element_type=F32)
        gate = gate + jnp.dot(mixed, col_out[by, 1], preferred_element_type=F32)
    near_own[0, :, :, :feats] = value.reshape(per, rows_t, feats)
    near_own[0, :, :, feats:] = gate.reshape(per, rows_t, feats)
    out_send[:, :, :feats] = value.astype(BF16).reshape(per, rows_t, feats)
    out_send[:, :, feats:] = gate.astype(BF16).reshape(per, rows_t, feats)
    for j in ROW_FAR_FIRST:
        if j:
            of_copy(partner(me_y, j, per)).start()

    @pl.when(me_z != me_d)
    def _():
        arrival(u_recv, u_rs).wait_recv()

    update(1, u_recv[:, :width])
    combined = near_own[0, me_y]
    arrival(out_recv.at[pl.ds(0, per - 1)], of_rs).wait_recv()
    for j in range(1, per):
        combined = combined + out_recv[partner(me_y, j, per)].astype(F32)
    out_ref[...] = (
        x_far[me_d * per + me_y].astype(F32) + combined[:, :feats] * jax.nn.sigmoid(combined[:, feats:])
    ).astype(BF16)

    sent(mix_far.at[pl.ds(0, dp - 1)], mf_ss)
    sent(out_send.at[pl.ds(0, per - 1)], of_ss)

    @pl.when(me_z != me_d)
    def _():
        u_copy().wait_send()


def put(out_ref, states_ref, out_hbm, states_hbm, sems):
    copies = [
        pltpu.make_async_copy(states_ref, states_hbm, sems.at[0]),
        pltpu.make_async_copy(out_ref, out_hbm, sems.at[1]),
    ]
    for copy in copies:
        copy.start()
    for copy in copies:
        copy.wait()


def per_device(
    tp, dp,
    stream, norm_gain, w_input, lam_re, lam_im, log_dt, b_re, b_im, readout_real, readout_imaginary, d_skip,
    w_val, w_gate, state,
):
    layers, feats, width = w_input.shape
    rows_t = stream.shape[0]
    rows_d, groups, lanes = state.shape[1:]
    chans = b_re.shape[-1]
    per = rows_d // rows_t

    turned_in = w_input.swapaxes(1, 2)
    turned_re, turned_im = b_re.swapaxes(2, 3), b_im.swapaxes(2, 3)

    limit = 67043328 - 4 * layers * rows_d * groups * lanes - (256 << 10)
    vmem = pl.BlockSpec(memory_space=pltpu.VMEM)
    hbm = pl.BlockSpec(memory_space=pltpu.HBM)
    one = pltpu.SemaphoreType.DMA
    dma = lambda *shape: one(shape)
    out, states = pl.pallas_call(
        functools.partial(kernel, tp, dp, chans),
        out_shape=(pltpu.VMEM(stream.shape, BF16), pltpu.VMEM((layers, rows_d * groups, lanes), F32)),
        in_specs=[hbm] * 14,
        out_specs=(vmem, vmem),
        scratch_shapes=[
            pltpu.VMEM(stream.shape, BF16),
            pltpu.VMEM(norm_gain.shape, F32),
            pltpu.VMEM(lam_re.shape, F32),
            pltpu.VMEM(lam_im.shape, F32),
            pltpu.VMEM(log_dt.shape, F32),
            pltpu.VMEM(d_skip.shape, F32),
            pltpu.VMEM((3, width, feats), BF16),
            pltpu.VMEM(turned_re.shape, F32),
            pltpu.VMEM(turned_im.shape, F32),
            pltpu.VMEM(readout_real.shape, F32),
            pltpu.VMEM(readout_imaginary.shape, F32),
            pltpu.VMEM((layers, width, lanes), F32),
            pltpu.VMEM((layers, width, lanes), F32),
            pltpu.VMEM((layers, rows_d * groups, lanes), F32),
            pltpu.VMEM((rows_d * groups, width), F32),
            pltpu.VMEM((rows_d, width), F32),
            pltpu.VMEM((rows_d * groups, width), F32),
            pltpu.VMEM((rows_d, width), F32),
            pltpu.VMEM((width, width), F32),
            pltpu.VMEM((tp, rows_t, feats), BF16),
            pltpu.VMEM((dp, width, feats), BF16),
            pltpu.VMEM((dp, rows_d, width), BF16),
            pltpu.VMEM((dp, per, rows_t, 2 * feats), F32),
            pltpu.VMEM((dp, per, rows_t, 2 * feats), BF16),
            pltpu.VMEM((dp, per, rows_t, 2 * feats), BF16),
            pltpu.VMEM((dp, rows_t, 2 * feats), BF16),
            pltpu.VMEM((rows_t, 2 * feats), F32),
            pltpu.VMEM((dp, rows_t, 2 * feats), BF16),
            pltpu.VMEM((dp, layers, rows_t, feats), F32),
            pltpu.VMEM((dp, width, feats), BF16),
            pltpu.VMEM((dp, 2, width, feats), BF16),
            pltpu.VMEM((dp, width, feats), BF16),
            pltpu.VMEM((tp, rows_t, feats), BF16),
            pltpu.VMEM((rows_d + width, 128), F32),
            pltpu.VMEM((rows_d + width, 128), F32),
            pltpu.VMEM((rows_d, 128), F32),
            pltpu.VMEM((rows_d, 128), F32),
            pltpu.VMEM((dp, rows_d, width), BF16),
            pltpu.VMEM((per, rows_t, 2 * feats), BF16),
            pltpu.VMEM((per, rows_t, 2 * feats), BF16),
            dma(6), dma(11),
            one, dma(dp),
            one, one,
            one, dma(dp),
            one, dma(dp),
            one, one,
            one, one,
            dma(2), dma(2, 3),
            one, one,
            one, dma(dp),
            one, one,
            one, one,
            one, one, one,
        ],
        compiler_params=pltpu.CompilerParams(collective_id=0, has_side_effects=True, vmem_limit_bytes=limit),
    )(
        stream, norm_gain, turned_in, lam_re, lam_im, log_dt, turned_re, turned_im, readout_real,
        readout_imaginary, d_skip, w_val, w_gate,
        state.reshape(layers, rows_d * groups, lanes),
    )
    out, states = pl.pallas_call(
        put,
        out_shape=(jax.ShapeDtypeStruct(out.shape, BF16), jax.ShapeDtypeStruct(states.shape, F32)),
        in_specs=[vmem, vmem],
        out_specs=(hbm, hbm),
        scratch_shapes=[dma(2)],
        compiler_params=pltpu.CompilerParams(vmem_limit_bytes=1 << 20),
    )(out, states)
    return out, states.reshape(state.shape)


def solution(mesh):
    return jax.shard_map(
        functools.partial(per_device, mesh.shape["tp"], mesh.shape["dp"]),
        mesh=mesh,
        in_specs=(
            P("tp", "dp"),
            P(None, "dp"),
            P(None, "dp", "tp"),
            P(None, "tp", None),
            P(None, "tp", None),
            P(None, "tp"),
            P(None, "tp", None, None),
            P(None, "tp", None, None),
            P(None, "tp", None, None),
            P(None, "tp", None, None),
            P(None, "tp"),
            P(None, "tp", "dp"),
            P(None, "tp", "dp"),
            P(None, "dp", "tp", None),
        ),
        out_specs=(P("tp", "dp"), P(None, "dp", "tp", None)),
        check_vma=False,
    )
```

```python
import functools

import jax
import jax.numpy as jnp
from jax import lax
from jax.experimental import pallas as pl
from jax.experimental.pallas import tpu as pltpu
from jax.sharding import PartitionSpec as P

EPS = 1e-06
F32 = jnp.float32
BF16 = jnp.bfloat16
HIGHEST = lax.Precision.HIGHEST
NT = (((1,), (1,)), ((), ()))
PLANE_FAR_FIRST = (4, 5, 6, 7, 2, 3, 1, 0)
ROW_FAR_FIRST = (2, 1, 3, 0)


def partner(me, k, n, back=False):
    if n & (n - 1):
        return (me + (n - k if back else k)) % n
    found, bit = 0, 1
    while bit < n:
        mine = (me // bit) % 2
        found = found + (bit * (1 - mine) if k & bit else bit * mine)
        bit *= 2
    return found


def ring_far_first(n, m):
    others = [(a, b) for a in range(n) for b in range(m) if a or b]
    return sorted(others, key=lambda o: -min(o[0], n - o[0]) - min(o[1], m - o[1]))


def kernel(
    tp, dp, chans,
    stream_hbm, gain_hbm, w_in_hbm, lam_re_hbm, lam_im_hbm, log_dt_hbm, b_re_hbm, b_im_hbm, c_re_hbm, c_im_hbm, skip_hbm,
    w_val_hbm, w_gate_hbm, state_hbm,
    out_ref, state,
    stream_ref, gain_ref, lam_re_ref, lam_im_ref, log_dt_ref, skip_ref, own_w, b_re, b_im, c_re, c_im, drive, read,
    kept, proj, u_keep, masked, from_old, mix_w,
    x_all, x_old, near_in, mix_out, mix_all, near_recv, out_own,
    gain_all, col_in, col_out, col_now, x_keep, part_send, part_recv, swap_send, swap_recv, u_send, u_recv, mix_far, out_send, out_recv,
    small_sem, load_sem, x_ss, x_rs, old_ss, old_rs, in_ss, in_rs, mix_ss, mix_rs, near_ss, near_rs,
    gain_ss, gain_rs, col_ss, col_rs, part_ss, part_rs, swap_ss, swap_rs, u_ss, u_rs, mf_ss, of_ss, of_rs,
):
    layers = w_in_hbm.shape[0]
    me_t, me_d = lax.axis_index("tp"), lax.axis_index("dp")
    rows_t, feats = stream_ref.shape
    rows_d, width = u_keep.shape
    per = rows_d // rows_t
    groups, half = lam_re_ref.shape[1:]
    lanes = state.shape[2]
    me_z, me_y = me_t // per, me_t % per

    barrier = pltpu.get_barrier_semaphore()

    def greet(t, d):
        pl.semaphore_signal(barrier, inc=1, device_id={"tp": t, "dp": d}, device_id_type=pl.DeviceIdType.MESH)

    @pl.when(me_z != me_d)
    def _():
        for k in range(dp):
            for j in range(per):
                greet(me_d * per + j, partner(me_d, k, dp))

    for hop in (1, -1, 2, -2):
        greet(lax.rem(me_z + hop + dp, dp) * per + me_y, me_d)
    for k in range(dp):
        for j in range(per):
            if k or j:
                greet(me_z * per + partner(me_y, j, per), partner(me_d, k, dp))

    smalls = []
    for i, (src, dst) in enumerate(
        (
            (stream_hbm, stream_ref), (gain_hbm, gain_ref), (lam_re_hbm, lam_re_ref), (lam_im_hbm, lam_im_ref),
            (log_dt_hbm, log_dt_ref), (skip_hbm, skip_ref),
        )
    ):
        smalls.append(pltpu.make_async_copy(src, dst, small_sem.at[i]))
        smalls[i].start()
    loads = {}
    for i, (src, dst) in enumerate(
        (
            (w_in_hbm.at[0], own_w), (w_in_hbm.at[1], col_in.at[me_z]), (b_re_hbm, b_re), (b_im_hbm, b_im),
            (c_re_hbm, c_re), (c_im_hbm, c_im), (state_hbm, state), (w_val_hbm.at[0], col_now.at[me_z, 0]),
            (w_gate_hbm.at[0], col_now.at[me_z, 1]), (w_val_hbm.at[1], col_out.at[me_z, 0]),
            (w_gate_hbm.at[1], col_out.at[me_z, 1]),
        )
    ):
        loads[i] = pltpu.make_async_copy(src, dst, load_sem.at[i])
        loads[i].start()

    def send(src, dst, ss, rs, t, d):
        return pltpu.make_async_remote_copy(
            src_ref=src, dst_ref=dst, send_sem=ss, recv_sem=rs, device_id={"tp": t, "dp": d},
            device_id_type=pl.DeviceIdType.MESH,
        )

    def x_copy(t):
        return send(stream_ref, x_all.at[me_d * per + me_y], x_ss, x_rs.at[me_d], t, me_z)

    def in_copy(to):
        return send(own_w, near_in.at[me_d], in_ss, in_rs, me_t, to)

    def old_copy(y):
        return send(stream_ref, x_old.at[me_y], old_ss, old_rs, me_z * per + y, me_d)

    def mix_copy(to):
        return send(mix_out, mix_all.at[me_z], mix_ss, mix_rs.at[me_z], me_d * per + me_y, to)

    def near_copy(y):
        return send(near_recv.at[me_y], near_recv.at[me_y], near_ss, near_rs, me_z * per + y, me_d)

    def gain_copy(to):
        return send(gain_all.at[me_d], gain_all.at[me_d], gain_ss, gain_rs, me_t, to)

    def col_part(what, home, side, i):
        rows = pl.ds(side * (width // 2), width // 2)
        if what == 1:
            held = col_out.at[home]
            return held.at[:, rows] if i == 4 else held
        held = col_now.at[home, what - 2] if what else col_in.at[home]
        return held.at[rows] if i == 4 else held

    def col_copy(what, side, i):
        sign = 1 - 2 * side
        home = lax.rem(me_z - sign * min(i - 1, 2) + 2 * dp, dp)
        to = lax.rem(me_z + sign * (2 if i == 4 else 1) + dp, dp)
        part = col_part(what, home, side, i)
        return send(part, part, col_ss.at[what], col_rs.at[what, min(i, 3) - 1], to * per + me_y, me_d)

    def col_start(what, *hops):
        for i in hops:
            for side in range(2):
                col_copy(what, side, i).start()

    def col_wait(what, hop):
        blocks = pl.ds(0, 3 if hop == 3 else 2)
        held = (col_in.at[blocks], col_out.at[blocks], col_now.at[blocks, 0], col_now.at[blocks, 1])[what]
        arrival(held, col_rs.at[what, hop - 1]).wait_recv()

    def part_copy(to):
        return send(part_send.at[to], part_recv.at[me_d], part_ss, part_rs, me_t, to)

    def mf_copy(to):
        return send(mix_far.at[me_d], mix_far.at[me_d], mf_ss, mix_rs.at[me_d], me_t, to)

    def of_copy(y):
        return send(out_send.at[y], out_recv.at[me_y], of_ss, of_rs, me_z * per + y, me_d)

    def swap_copy():
        return send(swap_send, swap_recv, swap_ss, swap_rs, me_d * per + me_y, me_z)

    def u_copy():
        return send(u_send, u_recv, u_ss, u_rs, me_d * per + me_y, me_z)

    def arrival(ref, rs):
        return send(ref, ref, rs, rs, 0, 0)

    def sent(ref, ss):
        send(ref, ref, ss, ss, 0, 0).wait_send()

    def fold(tall):
        return jnp.concatenate([tall[: rows_d // 2], tall[rows_d // 2 :]], axis=1)

    lane_group = lax.broadcasted_iota(jnp.int32, (rows_d, width), 1) // chans
    group_eye = lax.broadcasted_iota(jnp.int32, (groups, groups), 0) == lax.broadcasted_iota(jnp.int32, (groups, groups), 1)
    wide_0 = lax.broadcasted_iota(jnp.int32, (width, width), 0)
    wide_1 = lax.broadcasted_iota(jnp.int32, (width, width), 1)

    def prepare(l):
        step_size = jnp.exp(jnp.sum(jnp.where(group_eye, log_dt_ref[l : l + 1, :], 0.0), axis=1, keepdims=True))
        lam_re, lam_im = lam_re_ref[l], lam_im_ref[l]
        decay = jnp.exp(lam_re * step_size)
        angle = lam_im * step_size
        keep_re = decay * jnp.cos(angle)
        keep_im = decay * jnp.sin(angle)
        denom = lam_re * lam_re + lam_im * lam_im
        ratio_re = ((keep_re - 1.0) * lam_re + keep_im * lam_im) / denom
        ratio_im = (keep_im * lam_re - (keep_re - 1.0) * lam_im) / denom
        keep_a = jnp.concatenate([keep_re, keep_re], axis=1)
        keep_b = jnp.concatenate([-keep_im, keep_im], axis=1)
        if l == 0:
            for i in range(2, 7):
                loads[i].wait()
        for g in range(groups):
            t_re, t_im = b_re[l, g], b_im[l, g]
            r_re, r_im = ratio_re[g : g + 1, :], ratio_im[g : g + 1, :]
            drive[l, pl.ds(g * chans, chans), :] = jnp.concatenate(
                [r_re * t_re - r_im * t_im, r_re * t_im + r_im * t_re], axis=1
            )
        read[l] = jnp.concatenate([c_re[l].reshape(width, half), -c_im[l].reshape(width, half)], axis=1)
        for g in range(groups):
            old = state[l, pl.ds(g, rows_d, stride=groups), :]
            kept[l, pl.ds(g * rows_d, rows_d), :] = (
                keep_a[g : g + 1, :] * old + keep_b[g : g + 1, :] * pltpu.roll(old, lanes // 2, 1)
            )
        proj[...] = lax.dot_general(kept[l], read[l], NT, precision=HIGHEST, preferred_element_type=F32)
        total = jnp.zeros((rows_d, width), F32)
        for g in range(groups):
            total = jnp.where(lane_group == g, proj[pl.ds(g * rows_d, rows_d), :], total)
        full = lax.dot_general(drive[l], read[l], NT, precision=HIGHEST, preferred_element_type=F32)
        mixer = jnp.where(wide_0 // chans == wide_1 // chans, full, 0.0)
        mixer = mixer + jnp.where(wide_0 == wide_1, skip_ref[l : l + 1, :], 0.0)
        return total, mixer

    def update(l, u):
        for g in range(groups):
            masked[pl.ds(g * rows_d, rows_d), :] = jnp.where(lane_group == g, u, 0.0)
        kept[l] = kept[l] + jnp.dot(masked[...], drive[l], precision=HIGHEST, preferred_element_type=F32)
        for g in range(groups):
            state[l, pl.ds(g, rows_d, stride=groups), :] = kept[l, pl.ds(g * rows_d, rows_d), :]

    pl.semaphore_wait(barrier, per * dp - 1 + 4 + (dp - 1) * per)

    smalls[0].wait()
    for a, b in ring_far_first(dp, per):
        x_copy(lax.rem(me_z + a, dp) * per + lax.rem(me_y + b, per)).start()

    @pl.when(me_z != me_d)
    def _():
        x_copy(me_t).start()

    @pl.when(me_z == me_d)
    def _():
        x_all[me_d * per + me_y] = stream_ref[...]

    smalls[1].wait()
    gain_all[me_d] = jnp.broadcast_to(gain_ref[0:1, :], (rows_t, feats))
    loads[0].wait()
    for k in PLANE_FAR_FIRST:
        if k:
            gain_copy(partner(me_d, k, dp)).start()
            in_copy(partner(me_d, k, dp)).start()
    x_old[me_y] = stream_ref[...]
    for j in ROW_FAR_FIRST:
        if j:
            old_copy(partner(me_y, j, per)).start()
    loads[7].wait()
    loads[8].wait()
    col_start(2, 1)
    col_start(3, 1)
    for small in smalls[2:]:
        small.wait()
    from_old[...], mix_w[...] = prepare(0)

    for what in (2, 3):
        col_wait(what, 1)
        col_start(what, 2)
    loads[1].wait()
    col_start(0, 1)

    acc = jnp.zeros((rows_d, width), F32)
    squares = jnp.zeros((rows_d, feats), F32)
    for k in reversed(PLANE_FAR_FIRST):
        by = partner(me_d, k, dp, True)
        if k:
            arrival(x_all.at[pl.ds(0, per)], x_rs.at[by]).wait_recv()
        else:

            @pl.when(me_z != me_d)
            def _():
                arrival(x_all.at[pl.ds(0, per)], x_rs.at[by]).wait_recv()

            @pl.when(me_z == me_d)
            def _():
                arrival(x_all.at[pl.ds(0, per - 1)], x_rs.at[by]).wait_recv()

            arrival(gain_all.at[pl.ds(0, dp - 1)], gain_rs).wait_recv()
            arrival(near_in.at[pl.ds(0, dp - 1)], in_rs).wait_recv()
        weights = near_in.at[by] if k else own_w
        x = x_all[pl.ds(by * per, per)].astype(F32)
        normed = (x * gain_all[by][None]).astype(BF16).reshape(rows_d, feats)
        x = x.reshape(rows_d, feats)
        squares = squares + x * x
        acc = acc + lax.dot_general(normed, weights[...], NT, preferred_element_type=F32)
    u = lax.rsqrt(jnp.sum(squares, axis=1, keepdims=True) / (feats * dp) + EPS) * acc
    u_keep[...] = u
    pre = from_old[...] + jnp.dot(u, mix_w[...], precision=HIGHEST, preferred_element_type=F32)
    mix_out[...] = fold(jax.nn.gelu(pre).astype(BF16))
    for k in PLANE_FAR_FIRST[:-1]:
        mix_copy(partner(me_d, k, dp)).start()

    @pl.when(me_z != me_d)
    def _():
        mix_copy(me_d).start()

    @pl.when(me_z == me_d)
    def _():
        mix_all[me_z] = mix_out[...]

    for what in (2, 3):
        col_wait(what, 2)
        col_start(what, 3, 4)
    col_wait(0, 1)
    col_start(0, 2)
    loads[9].wait()
    loads[10].wait()
    col_start(1, 1)

    def project(blocks, weights, arrive):
        value = jnp.zeros((rows_d, feats), F32)
        gate = jnp.zeros((rows_d, feats), F32)
        for i, (block, held) in enumerate(blocks):
            arrive(i, block)
            mixed = held[block]
            mixed = jnp.concatenate([mixed[:, :width], mixed[:, width:]], axis=0)
            value = value + jnp.dot(mixed, weights[block, 0], preferred_element_type=F32)
            gate = gate + jnp.dot(mixed, weights[block, 1], preferred_element_type=F32)
        return value, gate

    def arrive_now(i, block):
        if i == 5:
            col_wait(2, 3)
            col_wait(3, 3)
            col_wait(0, 2)
            col_start(0, 3, 4)
        if i:
            arrival(mix_all.at[block], mix_rs.at[block]).wait_recv()
        else:

            @pl.when(me_z != me_d)
            def _():
                arrival(mix_all.at[block], mix_rs.at[block]).wait_recv()

    nearest = [lax.rem(me_z + hop + dp, dp) for hop in (0, 1, -1, 2, -2, 3, -3, 4)]
    value, gate = project([(z, mix_all) for z in nearest], col_now, arrive_now)
    near_recv[me_y, :, :feats] = value.astype(BF16)
    near_recv[me_y, :, feats:] = gate.astype(BF16)
    for j in ROW_FAR_FIRST:
        if j:
            near_copy(partner(me_y, j, per)).start()
    update(0, u_keep[...])
    total, mixer = prepare(1)
    tight = mixer[:, :chans]
    for g in range(1, groups):
        tight = tight + mixer[:, g * chans : (g + 1) * chans]
    blank = jnp.zeros((rows_d, width - width // rows_d * chans), F32)
    swap_send[...] = jnp.concatenate(
        [total] + [tight[i : i + rows_d] for i in range(0, width, rows_d)] + [blank], axis=1
    )

    @pl.when(me_z != me_d)
    def _():
        swap_copy().start()

    @pl.when(me_z == me_d)
    def _():
        swap_recv[...] = swap_send[...]

    col_wait(1, 1)
    col_start(1, 2)

    @pl.when(me_z != me_d)
    def _():
        sent(x_all, x_ss)
        sent(mix_all, mix_ss)

    @pl.when(me_z == me_d)
    def _():
        sent(x_all.at[pl.ds(0, tp - 1)], x_ss)
        sent(mix_all.at[pl.ds(0, dp - 1)], mix_ss)

    sent(near_in.at[pl.ds(0, dp - 1)], in_ss)
    sent(gain_all.at[pl.ds(0, dp - 1)], gain_ss)
    sent(x_old.at[pl.ds(0, per - 1)], old_ss)
    sent(col_now.at[pl.ds(0, 7), 0], col_ss.at[2])
    sent(col_now.at[pl.ds(0, 7), 1], col_ss.at[3])
    arrival(x_old.at[pl.ds(0, per - 1)], old_rs).wait_recv()
    arrival(near_recv.at[pl.ds(0, per - 1)], near_rs).wait_recv()
    combined = near_recv[0].astype(F32)
    for y in range(1, per):
        combined = combined + near_recv[y].astype(F32)
    fresh = (
        x_old[...].astype(F32).reshape(rows_d, feats) + combined[:, :feats] * jax.nn.sigmoid(combined[:, feats:])
    ).astype(BF16)

    x_keep[...] = fresh.reshape(per, rows_t, feats)
    x = fresh.astype(F32)
    normed = (x * gain_ref[1:2, :]).astype(BF16)
    squares = jnp.sum(x * x, axis=1, keepdims=True)
    upper = squares.astype(BF16).astype(F32)
    middle = (squares - upper).astype(BF16).astype(F32)
    lower = squares - upper - middle
    tail_lane = lax.broadcasted_iota(jnp.int32, (rows_d, 128 - width), 1)
    tail = jnp.where(tail_lane == 0, upper, jnp.where(tail_lane == 1, middle, jnp.where(tail_lane == 2, lower, 0.0)))
    col_wait(0, 3)
    own = None
    for k in PLANE_FAR_FIRST:
        to = partner(me_d, k, dp)
        product = lax.dot_general(normed, col_in[to], NT, preferred_element_type=F32)
        whole = jnp.concatenate([product, tail], axis=1)
        if k:
            part_send[to] = whole.astype(BF16)
            part_copy(to).start()
        else:
            own = whole
    col_wait(1, 2)
    col_start(1, 3, 4)
    sent(near_recv.at[pl.ds(0, per - 1)], near_ss)
    sent(col_in.at[pl.ds(0, 7)], col_ss.at[0])

    @pl.when(me_z != me_d)
    def _():
        swap_copy().wait_send()
        arrival(swap_recv, swap_rs).wait_recv()

    swapped = swap_recv[...]
    tight = jnp.concatenate(
        [swapped[:, width + i * chans : width + (i + 1) * chans] for i in range(width // rows_d)], axis=0
    )
    mixer = jnp.where(wide_0 // chans == wide_1 // chans, jnp.concatenate([tight] * groups, axis=1), 0.0)
    arrival(part_recv.at[pl.ds(0, dp - 1)], part_rs).wait_recv()
    for k in range(1, dp):
        own = own + part_recv[partner(me_d, k, dp)].astype(F32)
    squares = own[:, width : width + 1] + own[:, width + 1 : width + 2] + own[:, width + 2 : width + 3]
    u = lax.rsqrt(squares / (feats * dp) + EPS) * own[:, :width]
    u_send[...] = jnp.concatenate([u, u], axis=1)

    @pl.when(me_z != me_d)
    def _():
        u_copy().start()

    @pl.when(me_z == me_d)
    def _():
        u_recv[...] = u_send[...]

    pre = swapped[:, :width] + jnp.dot(u, mixer, precision=HIGHEST, preferred_element_type=F32)
    mix_far[me_d] = fold(jax.nn.gelu(pre).astype(BF16))
    for k in PLANE_FAR_FIRST:
        if k:
            mf_copy(partner(me_d, k, dp)).start()
    col_wait(1, 3)
    sent(part_send.at[pl.ds(0, dp - 1)], part_ss)
    sent(col_out.at[pl.ds(0, 7)], col_ss.at[1])

    def arrive_far(i, block):
        if i:
            arrival(mix_far.at[block], mix_rs.at[block]).wait_recv()

    value, gate = project(
        [(partner(me_d, k, dp, True), mix_far) for k in reversed(PLANE_FAR_FIRST)], col_out, arrive_far
    )
    out_own[:, :, :feats] = value.reshape(per, rows_t, feats)
    out_own[:, :, feats:] = gate.reshape(per, rows_t, feats)
    out_send[:, :, :feats] = value.astype(BF16).reshape(per, rows_t, feats)
    out_send[:, :, feats:] = gate.astype(BF16).reshape(per, rows_t, feats)
    for j in ROW_FAR_FIRST:
        if j:
            of_copy(partner(me_y, j, per)).start()

    @pl.when(me_z != me_d)
    def _():
        arrival(u_recv, u_rs).wait_recv()

    update(1, u_recv[:, :width])
    combined = out_own[me_y]
    arrival(out_recv.at[pl.ds(0, per - 1)], of_rs).wait_recv()
    for j in range(1, per):
        combined = combined + out_recv[partner(me_y, j, per)].astype(F32)
    out_ref[...] = (
        x_keep[me_y].astype(F32) + combined[:, :feats] * jax.nn.sigmoid(combined[:, feats:])
    ).astype(BF16)

    sent(mix_far.at[pl.ds(0, dp - 1)], mf_ss)
    sent(out_send.at[pl.ds(0, per - 1)], of_ss)

    @pl.when(me_z != me_d)
    def _():
        u_copy().wait_send()


def put(out_ref, states_ref, out_hbm, states_hbm, sems):
    copies = [
        pltpu.make_async_copy(states_ref, states_hbm, sems.at[0]),
        pltpu.make_async_copy(out_ref, out_hbm, sems.at[1]),
    ]
    for copy in copies:
        copy.start()
    for copy in copies:
        copy.wait()


def per_device(
    tp, dp,
    stream, norm_gain, w_input, lam_re, lam_im, log_dt, b_re, b_im, readout_real, readout_imaginary, d_skip,
    w_val, w_gate, state,
):
    layers, feats, width = w_input.shape
    rows_t = stream.shape[0]
    rows_d, groups, lanes = state.shape[1:]
    chans = b_re.shape[-1]
    per = rows_d // rows_t

    turned_in = w_input.swapaxes(1, 2)
    turned_re, turned_im = b_re.swapaxes(2, 3), b_im.swapaxes(2, 3)

    limit = 67043328 - 4 * layers * rows_d * groups * lanes - (256 << 10)
    vmem = pl.BlockSpec(memory_space=pltpu.VMEM)
    hbm = pl.BlockSpec(memory_space=pltpu.HBM)
    one = pltpu.SemaphoreType.DMA
    dma = lambda *shape: one(shape)
    out, states = pl.pallas_call(
        functools.partial(kernel, tp, dp, chans),
        out_shape=(pltpu.VMEM(stream.shape, BF16), pltpu.VMEM((layers, rows_d * groups, lanes), F32)),
        in_specs=[hbm] * 14,
        out_specs=(vmem, vmem),
        scratch_shapes=[
            pltpu.VMEM(stream.shape, BF16),
            pltpu.VMEM(norm_gain.shape, F32),
            pltpu.VMEM(lam_re.shape, F32),
            pltpu.VMEM(lam_im.shape, F32),
            pltpu.VMEM(log_dt.shape, F32),
            pltpu.VMEM(d_skip.shape, F32),
            pltpu.VMEM((width, feats), BF16),
            pltpu.VMEM(turned_re.shape, F32),
            pltpu.VMEM(turned_im.shape, F32),
            pltpu.VMEM(readout_real.shape, F32),
            pltpu.VMEM(readout_imaginary.shape, F32),
            pltpu.VMEM((layers, width, lanes), F32),
            pltpu.VMEM((layers, width, lanes), F32),
            pltpu.VMEM((layers, rows_d * groups, lanes), F32),
            pltpu.VMEM((rows_d * groups, width), F32),
            pltpu.VMEM((rows_d, width), F32),
            pltpu.VMEM((rows_d * groups, width), F32),
            pltpu.VMEM((rows_d, width), F32),
            pltpu.VMEM((width, width), F32),
            pltpu.VMEM((tp, rows_t, feats), BF16),
            pltpu.VMEM((per, rows_t, feats), BF16),
            pltpu.VMEM((dp, width, feats), BF16),
            pltpu.VMEM((rows_d // 2, 2 * width), BF16),
            pltpu.VMEM((dp, rows_d // 2, 2 * width), BF16),
            pltpu.VMEM((per, rows_d, 2 * feats), BF16),
            pltpu.VMEM((per, rows_t, 2 * feats), F32),
            pltpu.VMEM((dp, rows_t, feats), F32),
            pltpu.VMEM((dp, width, feats), BF16),
            pltpu.VMEM((dp, 2, width, feats), BF16),
            pltpu.VMEM((dp, 2, width, feats), BF16),
            pltpu.VMEM((per, rows_t, feats), BF16),
            pltpu.VMEM((dp, rows_d, 128), BF16),
            pltpu.VMEM((dp, rows_d, 128), BF16),
            pltpu.VMEM((rows_d, 2 * width), F32),
            pltpu.VMEM((rows_d, 2 * width), F32),
            pltpu.VMEM((rows_d, 128), F32),
            pltpu.VMEM((rows_d, 128), F32),
            pltpu.VMEM((dp, rows_d // 2, 2 * width), BF16),
            pltpu.VMEM((per, rows_t, 2 * feats), BF16),
            pltpu.VMEM((per, rows_t, 2 * feats), BF16),
            dma(6), dma(11),
            one, dma(dp),
            one, one,
            one, one,
            one, dma(dp),
            one, one,
            one, one,
            dma(4), dma(4, 3),
            one, one,
            one, one,
            one, one,
            one, one, one,
        ],
        compiler_params=pltpu.CompilerParams(collective_id=0, has_side_effects=True, vmem_limit_bytes=limit),
    )(
        stream, norm_gain, turned_in, lam_re, lam_im, log_dt, turned_re, turned_im, readout_real,
        readout_imaginary, d_skip, w_val, w_gate,
        state.reshape(layers, rows_d * groups, lanes),
    )
    out, states = pl.pallas_call(
        put,
        out_shape=(jax.ShapeDtypeStruct(out.shape, BF16), jax.ShapeDtypeStruct(states.shape, F32)),
        in_specs=[vmem, vmem],
        out_specs=(hbm, hbm),
        scratch_shapes=[dma(2)],
        compiler_params=pltpu.CompilerParams(vmem_limit_bytes=1 << 20),
    )(out, states)
    return out, states.reshape(state.shape)


def solution(mesh):
    return jax.shard_map(
        functools.partial(per_device, mesh.shape["tp"], mesh.shape["dp"]),
        mesh=mesh,
        in_specs=(
            P("tp", "dp"),
            P(None, "dp"),
            P(None, "dp", "tp"),
            P(None, "tp", None),
            P(None, "tp", None),
            P(None, "tp"),
            P(None, "tp", None, None),
            P(None, "tp", None, None),
            P(None, "tp", None, None),
            P(None, "tp", None, None),
            P(None, "tp"),
            P(None, "tp", "dp"),
            P(None, "tp", "dp"),
            P(None, "dp", "tp", None),
        ),
        out_specs=(P("tp", "dp"), P(None, "dp", "tp", None)),
        check_vma=False,
    )
```

```python
import functools

import jax
import jax.numpy as jnp
from jax import lax
from jax.experimental import pallas as pl
from jax.experimental.pallas import tpu as pltpu
from jax.sharding import PartitionSpec as P

EPS = 1e-06
F32 = jnp.float32
BF16 = jnp.bfloat16
HIGHEST = lax.Precision.HIGHEST
NT = (((1,), (1,)), ((), ()))
PLANE_FAR_FIRST = (4, 5, 6, 7, 2, 3, 1, 0)
ROW_FAR_FIRST = (2, 1, 3, 0)


def partner(me, k, n, back=False):
    if n & (n - 1):
        return (me + (n - k if back else k)) % n
    found, bit = 0, 1
    while bit < n:
        mine = (me // bit) % 2
        found = found + (bit * (1 - mine) if k & bit else bit * mine)
        bit *= 2
    return found


def ring_far_first(n, m):
    others = [(a, b) for a in range(n) for b in range(m) if a or b]
    return sorted(others, key=lambda o: -min(o[0], n - o[0]) - min(o[1], m - o[1]))


def kernel(
    tp, dp, chans,
    stream_hbm, gain_hbm, w_in_hbm, lam_re_hbm, lam_im_hbm, log_dt_hbm, b_re_hbm, b_im_hbm, c_re_hbm, c_im_hbm, skip_hbm,
    w_val_hbm, w_gate_hbm, state_hbm,
    out_ref, state,
    stream_ref, gain_ref, lam_re_ref, lam_im_ref, log_dt_ref, skip_ref, own_w, b_re, b_im, c_re, c_im, drive, read,
    kept, proj, u_keep, masked, from_old, mix_w,
    x_all, x_old, near_in, mix_out, mix_all, near_recv, out_own,
    gain_all, col_in, col_out, col_now, x_keep, part_send, part_recv, swap_send, swap_recv, u_send, u_recv, mix_far, out_send, out_recv,
    small_sem, load_sem, x_ss, x_rs, old_ss, old_rs, in_ss, in_rs, mix_ss, mix_rs, near_ss, near_rs,
    gain_ss, gain_rs, col_ss, col_rs, part_ss, part_rs, swap_ss, swap_rs, u_ss, u_rs, mf_ss, of_ss, of_rs,
):
    layers = w_in_hbm.shape[0]
    me_t, me_d = lax.axis_index("tp"), lax.axis_index("dp")
    rows_t, feats = stream_ref.shape
    rows_d, width = u_keep.shape
    per = rows_d // rows_t
    groups, half = lam_re_ref.shape[1:]
    lanes = state.shape[2]
    me_z, me_y = me_t // per, me_t % per

    barrier = pltpu.get_barrier_semaphore()

    def greet(t, d):
        pl.semaphore_signal(barrier, inc=1, device_id={"tp": t, "dp": d}, device_id_type=pl.DeviceIdType.MESH)

    @pl.when(me_z != me_d)
    def _():
        for k in range(dp):
            for j in range(per):
                greet(me_d * per + j, partner(me_d, k, dp))

    for hop in (1, -1, 2, -2):
        greet(lax.rem(me_z + hop + dp, dp) * per + me_y, me_d)
    for k in range(dp):
        for j in range(per):
            if k or j:
                greet(me_z * per + partner(me_y, j, per), partner(me_d, k, dp))

    smalls = []
    for i, (src, dst) in enumerate(
        (
            (stream_hbm, stream_ref), (gain_hbm, gain_ref), (lam_re_hbm, lam_re_ref), (lam_im_hbm, lam_im_ref),
            (log_dt_hbm, log_dt_ref), (skip_hbm, skip_ref),
        )
    ):
        smalls.append(pltpu.make_async_copy(src, dst, small_sem.at[i]))
        smalls[i].start()
    loads = {}
    for i, (src, dst) in enumerate(
        (
            (w_in_hbm.at[0], own_w), (w_in_hbm.at[1], col_in.at[me_z]), (b_re_hbm, b_re), (b_im_hbm, b_im),
            (c_re_hbm, c_re), (c_im_hbm, c_im), (state_hbm, state), (w_val_hbm.at[0], col_now.at[me_z, 0]),
            (w_gate_hbm.at[0], col_now.at[me_z, 1]), (w_val_hbm.at[1], col_out.at[me_z, 0]),
            (w_gate_hbm.at[1], col_out.at[me_z, 1]),
        )
    ):
        loads[i] = pltpu.make_async_copy(src, dst, load_sem.at[i])
        loads[i].start()

    def send(src, dst, ss, rs, t, d):
        return pltpu.make_async_remote_copy(
            src_ref=src, dst_ref=dst, send_sem=ss, recv_sem=rs, device_id={"tp": t, "dp": d},
            device_id_type=pl.DeviceIdType.MESH,
        )

    def x_copy(t):
        return send(stream_ref, x_all.at[me_d * per + me_y], x_ss, x_rs.at[me_d], t, me_z)

    def in_copy(to):
        return send(own_w, near_in.at[me_d], in_ss, in_rs, me_t, to)

    def old_copy(y):
        return send(stream_ref, x_old.at[me_y], old_ss, old_rs, me_z * per + y, me_d)

    def mix_copy(to):
        return send(mix_out, mix_all.at[me_z], mix_ss, mix_rs.at[me_z], me_d * per + me_y, to)

    def near_copy(y):
        return send(near_recv.at[me_y], near_recv.at[me_y], near_ss, near_rs, me_z * per + y, me_d)

    def gain_copy(to):
        return send(gain_all.at[me_d], gain_all.at[me_d], gain_ss, gain_rs, me_t, to)

    def col_part(what, home, side, i):
        rows = pl.ds(side * (width // 2), width // 2)
        held = (col_in.at[home], col_out.at[home, 0], col_now.at[home, 0], col_now.at[home, 1], col_out.at[home, 1])[what]
        return held.at[rows] if i == 4 else held

    def col_copy(what, side, i):
        sign = 1 - 2 * side
        home = lax.rem(me_z - sign * min(i - 1, 2) + 2 * dp, dp)
        to = lax.rem(me_z + sign * (2 if i == 4 else 1) + dp, dp)
        part = col_part(what, home, side, i)
        return send(part, part, col_ss.at[what], col_rs.at[what, min(i, 3) - 1], to * per + me_y, me_d)

    def col_start(what, *hops):
        for i in hops:
            for side in range(2):
                col_copy(what, side, i).start()

    def col_wait(what, hop):
        blocks = pl.ds(0, 3 if hop == 3 else 2)
        held = (
            col_in.at[blocks], col_out.at[blocks, 0], col_now.at[blocks, 0], col_now.at[blocks, 1], col_out.at[blocks, 1]
        )[what]
        arrival(held, col_rs.at[what, hop - 1]).wait_recv()

    def part_copy(to):
        return send(part_send.at[to], part_recv.at[me_d], part_ss, part_rs, me_t, to)

    def mf_copy(to):
        return send(mix_far.at[me_d], mix_far.at[me_d], mf_ss, mix_rs.at[me_d], me_t, to)

    def of_copy(y):
        return send(out_send.at[y], out_recv.at[me_y], of_ss, of_rs, me_z * per + y, me_d)

    def swap_copy():
        return send(swap_send, swap_recv, swap_ss, swap_rs, me_d * per + me_y, me_z)

    def u_copy():
        return send(u_send, u_recv, u_ss, u_rs, me_d * per + me_y, me_z)

    def arrival(ref, rs):
        return send(ref, ref, rs, rs, 0, 0)

    def sent(ref, ss):
        send(ref, ref, ss, ss, 0, 0).wait_send()

    def fold(tall):
        return jnp.concatenate([tall[: rows_d // 2], tall[rows_d // 2 :]], axis=1)

    lane_group = lax.broadcasted_iota(jnp.int32, (rows_d, width), 1) // chans
    group_eye = lax.broadcasted_iota(jnp.int32, (groups, groups), 0) == lax.broadcasted_iota(jnp.int32, (groups, groups), 1)
    wide_0 = lax.broadcasted_iota(jnp.int32, (width, width), 0)
    wide_1 = lax.broadcasted_iota(jnp.int32, (width, width), 1)

    def prepare(l):
        step_size = jnp.exp(jnp.sum(jnp.where(group_eye, log_dt_ref[l : l + 1, :], 0.0), axis=1, keepdims=True))
        lam_re, lam_im = lam_re_ref[l], lam_im_ref[l]
        decay = jnp.exp(lam_re * step_size)
        angle = lam_im * step_size
        keep_re = decay * jnp.cos(angle)
        keep_im = decay * jnp.sin(angle)
        denom = lam_re * lam_re + lam_im * lam_im
        ratio_re = ((keep_re - 1.0) * lam_re + keep_im * lam_im) / denom
        ratio_im = (keep_im * lam_re - (keep_re - 1.0) * lam_im) / denom
        keep_a = jnp.concatenate([keep_re, keep_re], axis=1)
        keep_b = jnp.concatenate([-keep_im, keep_im], axis=1)
        if l == 0:
            for i in range(2, 7):
                loads[i].wait()
        for g in range(groups):
            t_re, t_im = b_re[l, g], b_im[l, g]
            r_re, r_im = ratio_re[g : g + 1, :], ratio_im[g : g + 1, :]
            drive[l, pl.ds(g * chans, chans), :] = jnp.concatenate(
                [r_re * t_re - r_im * t_im, r_re * t_im + r_im * t_re], axis=1
            )
        read[l] = jnp.concatenate([c_re[l].reshape(width, half), -c_im[l].reshape(width, half)], axis=1)
        for g in range(groups):
            old = state[l, pl.ds(g, rows_d, stride=groups), :]
            kept[l, pl.ds(g * rows_d, rows_d), :] = (
                keep_a[g : g + 1, :] * old + keep_b[g : g + 1, :] * pltpu.roll(old, lanes // 2, 1)
            )
        proj[...] = lax.dot_general(kept[l], read[l], NT, precision=HIGHEST, preferred_element_type=F32)
        total = jnp.zeros((rows_d, width), F32)
        for g in range(groups):
            total = jnp.where(lane_group == g, proj[pl.ds(g * rows_d, rows_d), :], total)
        full = lax.dot_general(drive[l], read[l], NT, precision=HIGHEST, preferred_element_type=F32)
        mixer = jnp.where(wide_0 // chans == wide_1 // chans, full, 0.0)
        mixer = mixer + jnp.where(wide_0 == wide_1, skip_ref[l : l + 1, :], 0.0)
        return total, mixer

    def update(l, u):
        for g in range(groups):
            masked[pl.ds(g * rows_d, rows_d), :] = jnp.where(lane_group == g, u, 0.0)
        kept[l] = kept[l] + jnp.dot(masked[...], drive[l], precision=HIGHEST, preferred_element_type=F32)
        for g in range(groups):
            state[l, pl.ds(g, rows_d, stride=groups), :] = kept[l, pl.ds(g * rows_d, rows_d), :]

    pl.semaphore_wait(barrier, per * dp - 1 + 4 + (dp - 1) * per)

    smalls[0].wait()
    for a, b in ring_far_first(dp, per):
        x_copy(lax.rem(me_z + a, dp) * per + lax.rem(me_y + b, per)).start()

    @pl.when(me_z != me_d)
    def _():
        x_copy(me_t).start()

    @pl.when(me_z == me_d)
    def _():
        x_all[me_d * per + me_y] = stream_ref[...]

    smalls[1].wait()
    gain_all[me_d] = jnp.broadcast_to(gain_ref[0:1, :], (rows_t, feats))
    loads[0].wait()
    for k in PLANE_FAR_FIRST:
        if k:
            gain_copy(partner(me_d, k, dp)).start()
            in_copy(partner(me_d, k, dp)).start()
    x_old[me_y] = stream_ref[...]
    for j in ROW_FAR_FIRST:
        if j:
            old_copy(partner(me_y, j, per)).start()
    loads[7].wait()
    loads[8].wait()
    col_start(2, 1)
    col_start(3, 1)
    for small in smalls[2:]:
        small.wait()
    from_old[...], mix_w[...] = prepare(0)

    for what in (2, 3):
        col_wait(what, 1)
        col_start(what, 2)
    loads[1].wait()
    col_start(0, 1)

    acc = jnp.zeros((rows_d, width), F32)
    squares = jnp.zeros((rows_d, feats), F32)
    for k in reversed(PLANE_FAR_FIRST):
        by = partner(me_d, k, dp, True)
        if k:
            arrival(x_all.at[pl.ds(0, per)], x_rs.at[by]).wait_recv()
        else:

            @pl.when(me_z != me_d)
            def _():
                arrival(x_all.at[pl.ds(0, per)], x_rs.at[by]).wait_recv()

            @pl.when(me_z == me_d)
            def _():
                arrival(x_all.at[pl.ds(0, per - 1)], x_rs.at[by]).wait_recv()

            arrival(gain_all.at[pl.ds(0, dp - 1)], gain_rs).wait_recv()
            arrival(near_in.at[pl.ds(0, dp - 1)], in_rs).wait_recv()
        weights = near_in.at[by] if k else own_w
        x = x_all[pl.ds(by * per, per)].astype(F32)
        normed = (x * gain_all[by][None]).astype(BF16).reshape(rows_d, feats)
        x = x.reshape(rows_d, feats)
        squares = squares + x * x
        acc = acc + lax.dot_general(normed, weights[...], NT, preferred_element_type=F32)
    u = lax.rsqrt(jnp.sum(squares, axis=1, keepdims=True) / (feats * dp) + EPS) * acc
    u_keep[...] = u
    pre = from_old[...] + jnp.dot(u, mix_w[...], precision=HIGHEST, preferred_element_type=F32)
    mix_out[...] = fold(jax.nn.gelu(pre).astype(BF16))
    for k in PLANE_FAR_FIRST[:-1]:
        mix_copy(partner(me_d, k, dp)).start()

    @pl.when(me_z != me_d)
    def _():
        mix_copy(me_d).start()

    @pl.when(me_z == me_d)
    def _():
        mix_all[me_z] = mix_out[...]

    for what in (2, 3):
        col_wait(what, 2)
        col_start(what, 4, 3)
    col_wait(0, 1)
    col_start(0, 2)
    loads[9].wait()
    loads[10].wait()
    col_start(1, 1)
    col_start(4, 1)

    def project(blocks, weights, arrive):
        value = jnp.zeros((rows_d, feats), F32)
        gate = jnp.zeros((rows_d, feats), F32)
        for i, (block, held) in enumerate(blocks):
            arrive(i, block)
            mixed = held[block]
            mixed = jnp.concatenate([mixed[:, :width], mixed[:, width:]], axis=0)
            value = value + jnp.dot(mixed, weights[block, 0], preferred_element_type=F32)
            gate = gate + jnp.dot(mixed, weights[block, 1], preferred_element_type=F32)
        return value, gate

    def arrive_now(i, block):
        if i == 5:
            col_wait(2, 3)
            col_wait(3, 3)
            col_wait(0, 2)
            col_start(0, 4, 3)
        if i:
            arrival(mix_all.at[block], mix_rs.at[block]).wait_recv()
        else:

            @pl.when(me_z != me_d)
            def _():
                arrival(mix_all.at[block], mix_rs.at[block]).wait_recv()

    nearest = [lax.rem(me_z + hop + dp, dp) for hop in (0, 1, -1, 2, -2, 3, -3, 4)]
    value, gate = project([(z, mix_all) for z in nearest], col_now, arrive_now)
    near_recv[me_y, :, :feats] = value.astype(BF16)
    near_recv[me_y, :, feats:] = gate.astype(BF16)
    for j in ROW_FAR_FIRST:
        if j:
            near_copy(partner(me_y, j, per)).start()
    update(0, u_keep[...])
    total, mixer = prepare(1)
    tight = mixer[:, :chans]
    for g in range(1, groups):
        tight = tight + mixer[:, g * chans : (g + 1) * chans]
    blank = jnp.zeros((rows_d, width - width // rows_d * chans), F32)
    swap_send[...] = jnp.concatenate(
        [total] + [tight[i : i + rows_d] for i in range(0, width, rows_d)] + [blank], axis=1
    )

    @pl.when(me_z != me_d)
    def _():
        swap_copy().start()

    @pl.when(me_z == me_d)
    def _():
        swap_recv[...] = swap_send[...]

    for what in (1, 4):
        col_wait(what, 1)
        col_start(what, 2)

    @pl.when(me_z != me_d)
    def _():
        sent(x_all, x_ss)
        sent(mix_all, mix_ss)

    @pl.when(me_z == me_d)
    def _():
        sent(x_all.at[pl.ds(0, tp - 1)], x_ss)
        sent(mix_all.at[pl.ds(0, dp - 1)], mix_ss)

    sent(near_in.at[pl.ds(0, dp - 1)], in_ss)
    sent(gain_all.at[pl.ds(0, dp - 1)], gain_ss)
    sent(x_old.at[pl.ds(0, per - 1)], old_ss)
    sent(col_now.at[pl.ds(0, 7), 0], col_ss.at[2])
    sent(col_now.at[pl.ds(0, 7), 1], col_ss.at[3])
    arrival(x_old.at[pl.ds(0, per - 1)], old_rs).wait_recv()
    arrival(near_recv.at[pl.ds(0, per - 1)], near_rs).wait_recv()
    combined = near_recv[0].astype(F32)
    for y in range(1, per):
        combined = combined + near_recv[y].astype(F32)
    fresh = (
        x_old[...].astype(F32).reshape(rows_d, feats) + combined[:, :feats] * jax.nn.sigmoid(combined[:, feats:])
    ).astype(BF16)

    x_keep[...] = fresh.reshape(per, rows_t, feats)
    x = fresh.astype(F32)
    normed = (x * gain_ref[1:2, :]).astype(BF16)
    squares = jnp.sum(x * x, axis=1, keepdims=True)
    upper = squares.astype(BF16).astype(F32)
    middle = (squares - upper).astype(BF16).astype(F32)
    lower = squares - upper - middle
    tail_lane = lax.broadcasted_iota(jnp.int32, (rows_d, 128 - width), 1)
    tail = jnp.where(tail_lane == 0, upper, jnp.where(tail_lane == 1, middle, jnp.where(tail_lane == 2, lower, 0.0)))
    col_wait(0, 3)
    own = None
    for k in PLANE_FAR_FIRST:
        to = partner(me_d, k, dp)
        product = lax.dot_general(normed, col_in[to], NT, preferred_element_type=F32)
        whole = jnp.concatenate([product, tail], axis=1)
        if k:
            part_send[to] = whole.astype(BF16)
            part_copy(to).start()
        else:
            own = whole
    for what in (1, 4):
        col_wait(what, 2)
        col_start(what, 4, 3)
    sent(near_recv.at[pl.ds(0, per - 1)], near_ss)
    sent(col_in.at[pl.ds(0, 7)], col_ss.at[0])

    @pl.when(me_z != me_d)
    def _():
        swap_copy().wait_send()
        arrival(swap_recv, swap_rs).wait_recv()

    swapped = swap_recv[...]
    tight = jnp.concatenate(
        [swapped[:, width + i * chans : width + (i + 1) * chans] for i in range(width // rows_d)], axis=0
    )
    mixer = jnp.where(wide_0 // chans == wide_1 // chans, jnp.concatenate([tight] * groups, axis=1), 0.0)
    arrival(part_recv.at[pl.ds(0, dp - 1)], part_rs).wait_recv()
    for k in range(1, dp):
        own = own + part_recv[partner(me_d, k, dp)].astype(F32)
    squares = own[:, width : width + 1] + own[:, width + 1 : width + 2] + own[:, width + 2 : width + 3]
    u = lax.rsqrt(squares / (feats * dp) + EPS) * own[:, :width]
    u_send[...] = jnp.concatenate([u, u], axis=1)

    @pl.when(me_z != me_d)
    def _():
        u_copy().start()

    @pl.when(me_z == me_d)
    def _():
        u_recv[...] = u_send[...]

    pre = swapped[:, :width] + jnp.dot(u, mixer, precision=HIGHEST, preferred_element_type=F32)
    mix_far[me_d] = fold(jax.nn.gelu(pre).astype(BF16))
    for k in PLANE_FAR_FIRST:
        if k:
            mf_copy(partner(me_d, k, dp)).start()
    col_wait(1, 3)
    col_wait(4, 3)
    sent(part_send.at[pl.ds(0, dp - 1)], part_ss)
    sent(col_out.at[pl.ds(0, 7), 0], col_ss.at[1])
    sent(col_out.at[pl.ds(0, 7), 1], col_ss.at[4])

    def arrive_far(i, block):
        if i:
            arrival(mix_far.at[block], mix_rs.at[block]).wait_recv()

    value, gate = project(
        [(partner(me_d, k, dp, True), mix_far) for k in reversed(PLANE_FAR_FIRST)], col_out, arrive_far
    )
    out_own[:, :, :feats] = value.reshape(per, rows_t, feats)
    out_own[:, :, feats:] = gate.reshape(per, rows_t, feats)
    out_send[:, :, :feats] = value.astype(BF16).reshape(per, rows_t, feats)
    out_send[:, :, feats:] = gate.astype(BF16).reshape(per, rows_t, feats)
    for j in ROW_FAR_FIRST:
        if j:
            of_copy(partner(me_y, j, per)).start()

    @pl.when(me_z != me_d)
    def _():
        arrival(u_recv, u_rs).wait_recv()

    update(1, u_recv[:, :width])
    combined = out_own[me_y]
    arrival(out_recv.at[pl.ds(0, per - 1)], of_rs).wait_recv()
    for j in range(1, per):
        combined = combined + out_recv[partner(me_y, j, per)].astype(F32)
    out_ref[...] = (
        x_keep[me_y].astype(F32) + combined[:, :feats] * jax.nn.sigmoid(combined[:, feats:])
    ).astype(BF16)

    sent(mix_far.at[pl.ds(0, dp - 1)], mf_ss)
    sent(out_send.at[pl.ds(0, per - 1)], of_ss)

    @pl.when(me_z != me_d)
    def _():
        u_copy().wait_send()


def put(out_ref, states_ref, out_hbm, states_hbm, sems):
    copies = [
        pltpu.make_async_copy(states_ref, states_hbm, sems.at[0]),
        pltpu.make_async_copy(out_ref, out_hbm, sems.at[1]),
    ]
    for copy in copies:
        copy.start()
    for copy in copies:
        copy.wait()


def per_device(
    tp, dp,
    stream, norm_gain, w_input, lam_re, lam_im, log_dt, b_re, b_im, readout_real, readout_imaginary, d_skip,
    w_val, w_gate, state,
):
    layers, feats, width = w_input.shape
    rows_t = stream.shape[0]
    rows_d, groups, lanes = state.shape[1:]
    chans = b_re.shape[-1]
    per = rows_d // rows_t

    turned_in = w_input.swapaxes(1, 2)
    turned_re, turned_im = b_re.swapaxes(2, 3), b_im.swapaxes(2, 3)

    limit = 67043328 - 4 * layers * rows_d * groups * lanes - (256 << 10)
    vmem = pl.BlockSpec(memory_space=pltpu.VMEM)
    hbm = pl.BlockSpec(memory_space=pltpu.HBM)
    one = pltpu.SemaphoreType.DMA
    dma = lambda *shape: one(shape)
    out, states = pl.pallas_call(
        functools.partial(kernel, tp, dp, chans),
        out_shape=(pltpu.VMEM(stream.shape, BF16), pltpu.VMEM((layers, rows_d * groups, lanes), F32)),
        in_specs=[hbm] * 14,
        out_specs=(vmem, vmem),
        scratch_shapes=[
            pltpu.VMEM(stream.shape, BF16),
            pltpu.VMEM(norm_gain.shape, F32),
            pltpu.VMEM(lam_re.shape, F32),
            pltpu.VMEM(lam_im.shape, F32),
            pltpu.VMEM(log_dt.shape, F32),
            pltpu.VMEM(d_skip.shape, F32),
            pltpu.VMEM((width, feats), BF16),
            pltpu.VMEM(turned_re.shape, F32),
            pltpu.VMEM(turned_im.shape, F32),
            pltpu.VMEM(readout_real.shape, F32),
            pltpu.VMEM(readout_imaginary.shape, F32),
            pltpu.VMEM((layers, width, lanes), F32),
            pltpu.VMEM((layers, width, lanes), F32),
            pltpu.VMEM((layers, rows_d * groups, lanes), F32),
            pltpu.VMEM((rows_d * groups, width), F32),
            pltpu.VMEM((rows_d, width), F32),
            pltpu.VMEM((rows_d * groups, width), F32),
            pltpu.VMEM((rows_d, width), F32),
            pltpu.VMEM((width, width), F32),
            pltpu.VMEM((tp, rows_t, feats), BF16),
            pltpu.VMEM((per, rows_t, feats), BF16),
            pltpu.VMEM((dp, width, feats), BF16),
            pltpu.VMEM((rows_d // 2, 2 * width), BF16),
            pltpu.VMEM((dp, rows_d // 2, 2 * width), BF16),
            pltpu.VMEM((per, rows_d, 2 * feats), BF16),
            pltpu.VMEM((per, rows_t, 2 * feats), F32),
            pltpu.VMEM((dp, rows_t, feats), F32),
            pltpu.VMEM((dp, width, feats), BF16),
            pltpu.VMEM((dp, 2, width, feats), BF16),
            pltpu.VMEM((dp, 2, width, feats), BF16),
            pltpu.VMEM((per, rows_t, feats), BF16),
            pltpu.VMEM((dp, rows_d, 128), BF16),
            pltpu.VMEM((dp, rows_d, 128), BF16),
            pltpu.VMEM((rows_d, 2 * width), F32),
            pltpu.VMEM((rows_d, 2 * width), F32),
            pltpu.VMEM((rows_d, 128), F32),
            pltpu.VMEM((rows_d, 128), F32),
            pltpu.VMEM((dp, rows_d // 2, 2 * width), BF16),
            pltpu.VMEM((per, rows_t, 2 * feats), BF16),
            pltpu.VMEM((per, rows_t, 2 * feats), BF16),
            dma(6), dma(11),
            one, dma(dp),
            one, one,
            one, one,
            one, dma(dp),
            one, one,
            one, one,
            dma(5), dma(5, 3),
            one, one,
            one, one,
            one, one,
            one, one, one,
        ],
        compiler_params=pltpu.CompilerParams(collective_id=0, has_side_effects=True, vmem_limit_bytes=limit),
    )(
        stream, norm_gain, turned_in, lam_re, lam_im, log_dt, turned_re, turned_im, readout_real,
        readout_imaginary, d_skip, w_val, w_gate,
        state.reshape(layers, rows_d * groups, lanes),
    )
    out, states = pl.pallas_call(
        put,
        out_shape=(jax.ShapeDtypeStruct(out.shape, BF16), jax.ShapeDtypeStruct(states.shape, F32)),
        in_specs=[vmem, vmem],
        out_specs=(hbm, hbm),
        scratch_shapes=[dma(2)],
        compiler_params=pltpu.CompilerParams(vmem_limit_bytes=1 << 20),
    )(out, states)
    return out, states.reshape(state.shape)


def solution(mesh):
    return jax.shard_map(
        functools.partial(per_device, mesh.shape["tp"], mesh.shape["dp"]),
        mesh=mesh,
        in_specs=(
            P("tp", "dp"),
            P(None, "dp"),
            P(None, "dp", "tp"),
            P(None, "tp", None),
            P(None, "tp", None),
            P(None, "tp"),
            P(None, "tp", None, None),
            P(None, "tp", None, None),
            P(None, "tp", None, None),
            P(None, "tp", None, None),
            P(None, "tp"),
            P(None, "tp", "dp"),
            P(None, "tp", "dp"),
            P(None, "dp", "tp", None),
        ),
        out_specs=(P("tp", "dp"), P(None, "dp", "tp", None)),
        check_vma=False,
    )
```

```python
import functools

import jax
import jax.numpy as jnp
from jax import lax
from jax.experimental import pallas as pl
from jax.experimental.pallas import tpu as pltpu
from jax.sharding import PartitionSpec as P

EPS = 1e-06
F32 = jnp.float32
BF16 = jnp.bfloat16
HIGHEST = lax.Precision.HIGHEST
NT = (((1,), (1,)), ((), ()))
PLANE_FAR_FIRST = (4, 5, 6, 7, 2, 3, 1, 0)
ROW_FAR_FIRST = (2, 1, 3, 0)


def partner(me, k, n, back=False):
    if n & (n - 1):
        return (me + (n - k if back else k)) % n
    found, bit = 0, 1
    while bit < n:
        mine = (me // bit) % 2
        found = found + (bit * (1 - mine) if k & bit else bit * mine)
        bit *= 2
    return found


def ring_far_first(n, m):
    others = [(a, b) for a in range(n) for b in range(m) if a or b]
    return sorted(others, key=lambda o: -min(o[0], n - o[0]) - min(o[1], m - o[1]))


def kernel(
    tp, dp, chans,
    stream_hbm, gain_hbm, w_in_hbm, lam_re_hbm, lam_im_hbm, log_dt_hbm, b_re_hbm, b_im_hbm, c_re_hbm, c_im_hbm, skip_hbm,
    w_val_hbm, w_gate_hbm, state_hbm,
    out_ref, state,
    stream_ref, gain_ref, lam_re_ref, lam_im_ref, log_dt_ref, skip_ref, own_w, b_re, b_im, c_re, c_im, drive, read,
    kept, proj, u_keep, masked, from_old, mix_w,
    x_all, x_old, near_in, mix_out, mix_all, near_recv, out_own,
    gain_all, col_in, col_out, col_now, x_keep, part_send, part_recv, swap_send, swap_recv, u_send, u_recv, mix_far, out_send, out_recv,
    small_sem, load_sem, x_ss, x_rs, old_ss, old_rs, in_ss, in_rs, mix_ss, mix_rs, near_ss, near_rs,
    gain_ss, gain_rs, col_ss, col_rs, part_ss, part_rs, swap_ss, swap_rs, u_ss, u_rs, mf_ss, of_ss, of_rs,
):
    layers = w_in_hbm.shape[0]
    me_t, me_d = lax.axis_index("tp"), lax.axis_index("dp")
    rows_t, feats = stream_ref.shape
    rows_d, width = u_keep.shape
    per = rows_d // rows_t
    groups, half = lam_re_ref.shape[1:]
    lanes = state.shape[2]
    me_z, me_y = me_t // per, me_t % per

    barrier = pltpu.get_barrier_semaphore()

    def greet(t, d):
        pl.semaphore_signal(barrier, inc=1, device_id={"tp": t, "dp": d}, device_id_type=pl.DeviceIdType.MESH)

    @pl.when(me_z != me_d)
    def _():
        for k in range(dp):
            for j in range(per):
                greet(me_d * per + j, partner(me_d, k, dp))

    for hop in (1, -1, 2, -2):
        greet(lax.rem(me_z + hop + dp, dp) * per + me_y, me_d)
    for k in range(dp):
        for j in range(per):
            if k or j:
                greet(me_z * per + partner(me_y, j, per), partner(me_d, k, dp))

    smalls = []
    for i, (src, dst) in enumerate(
        (
            (stream_hbm, stream_ref), (gain_hbm, gain_ref), (lam_re_hbm, lam_re_ref), (lam_im_hbm, lam_im_ref),
            (log_dt_hbm, log_dt_ref), (skip_hbm, skip_ref),
        )
    ):
        smalls.append(pltpu.make_async_copy(src, dst, small_sem.at[i]))
        smalls[i].start()
    loads = {}
    for i, (src, dst) in enumerate(
        (
            (w_in_hbm.at[0], own_w), (w_in_hbm.at[1], col_in.at[me_z]), (b_re_hbm, b_re), (b_im_hbm, b_im),
            (c_re_hbm, c_re), (c_im_hbm, c_im), (state_hbm, state), (w_val_hbm.at[0], col_now.at[me_z, 0]),
            (w_gate_hbm.at[0], col_now.at[me_z, 1]), (w_val_hbm.at[1], col_out.at[me_z, 0]),
            (w_gate_hbm.at[1], col_out.at[me_z, 1]),
        )
    ):
        loads[i] = pltpu.make_async_copy(src, dst, load_sem.at[i])
        loads[i].start()

    def send(src, dst, ss, rs, t, d):
        return pltpu.make_async_remote_copy(
            src_ref=src, dst_ref=dst, send_sem=ss, recv_sem=rs, device_id={"tp": t, "dp": d},
            device_id_type=pl.DeviceIdType.MESH,
        )

    def x_copy(t):
        return send(stream_ref, x_all.at[me_d * per + me_y], x_ss, x_rs.at[me_d], t, me_z)

    def in_copy(to):
        return send(own_w, near_in.at[me_d], in_ss, in_rs, me_t, to)

    def old_copy(y):
        return send(stream_ref, x_old.at[me_y], old_ss, old_rs, me_z * per + y, me_d)

    def mix_copy(to):
        return send(mix_out, mix_all.at[me_z], mix_ss, mix_rs.at[me_z], me_d * per + me_y, to)

    def near_copy(y):
        return send(near_recv.at[me_y], near_recv.at[me_y], near_ss, near_rs, me_z * per + y, me_d)

    def gain_copy(to):
        return send(gain_all.at[me_d], gain_all.at[me_d], gain_ss, gain_rs, me_t, to)

    now = (3, 4, 5, 6)

    def col_stream(what, home):
        if what < 3:
            return (col_in.at[home], col_out.at[home, 0], col_out.at[home, 1])[what]
        return col_now.at[home, (what - 3) // 2, pl.ds((what - 3) % 2 * (width // 2), width // 2)]

    def col_part(what, home, side, i):
        held = col_stream(what, home)
        rows = held.shape[0] // 2
        return held.at[pl.ds(side * rows, rows)] if i == 4 else held

    def col_copy(what, side, i):
        sign = 1 - 2 * side
        home = lax.rem(me_z - sign * min(i - 1, 2) + 2 * dp, dp)
        to = lax.rem(me_z + sign * (2 if i == 4 else 1) + dp, dp)
        part = col_part(what, home, side, i)
        return send(part, part, col_ss.at[(0, 1, 1, 2, 2, 2, 2)[what]], col_rs.at[what, min(i, 3) - 1], to * per + me_y, me_d)

    def col_start(what, *hops):
        for i in hops:
            for side in range(2):
                col_copy(what, side, i).start()

    def col_wait(what, hop):
        blocks = pl.ds(0, 3 if hop == 3 else 2)
        held = col_stream(what, blocks)
        arrival(held, col_rs.at[what, hop - 1]).wait_recv()

    def part_copy(to):
        return send(part_send.at[to], part_recv.at[me_d], part_ss, part_rs, me_t, to)

    def mf_copy(to):
        return send(mix_far.at[me_d], mix_far.at[me_d], mf_ss, mix_rs.at[me_d], me_t, to)

    def of_copy(y):
        return send(out_send.at[y], out_recv.at[me_y], of_ss, of_rs, me_z * per + y, me_d)

    def swap_copy():
        return send(swap_send, swap_recv, swap_ss, swap_rs, me_d * per + me_y, me_z)

    def u_copy():
        return send(u_send, u_recv, u_ss, u_rs, me_d * per + me_y, me_z)

    def arrival(ref, rs):
        return send(ref, ref, rs, rs, 0, 0)

    def sent(ref, ss):
        send(ref, ref, ss, ss, 0, 0).wait_send()

    def fold(tall):
        return jnp.concatenate([tall[: rows_d // 2], tall[rows_d // 2 :]], axis=1)

    lane_group = lax.broadcasted_iota(jnp.int32, (rows_d, width), 1) // chans
    group_eye = lax.broadcasted_iota(jnp.int32, (groups, groups), 0) == lax.broadcasted_iota(jnp.int32, (groups, groups), 1)
    wide_0 = lax.broadcasted_iota(jnp.int32, (width, width), 0)
    wide_1 = lax.broadcasted_iota(jnp.int32, (width, width), 1)

    def prepare(l):
        step_size = jnp.exp(jnp.sum(jnp.where(group_eye, log_dt_ref[l : l + 1, :], 0.0), axis=1, keepdims=True))
        lam_re, lam_im = lam_re_ref[l], lam_im_ref[l]
        decay = jnp.exp(lam_re * step_size)
        angle = lam_im * step_size
        keep_re = decay * jnp.cos(angle)
        keep_im = decay * jnp.sin(angle)
        denom = lam_re * lam_re + lam_im * lam_im
        ratio_re = ((keep_re - 1.0) * lam_re + keep_im * lam_im) / denom
        ratio_im = (keep_im * lam_re - (keep_re - 1.0) * lam_im) / denom
        keep_a = jnp.concatenate([keep_re, keep_re], axis=1)
        keep_b = jnp.concatenate([-keep_im, keep_im], axis=1)
        if l == 0:
            for i in range(2, 7):
                loads[i].wait()
        for g in range(groups):
            t_re, t_im = b_re[l, g], b_im[l, g]
            r_re, r_im = ratio_re[g : g + 1, :], ratio_im[g : g + 1, :]
            drive[l, pl.ds(g * chans, chans), :] = jnp.concatenate(
                [r_re * t_re - r_im * t_im, r_re * t_im + r_im * t_re], axis=1
            )
        read[l] = jnp.concatenate([c_re[l].reshape(width, half), -c_im[l].reshape(width, half)], axis=1)
        for g in range(groups):
            old = state[l, pl.ds(g, rows_d, stride=groups), :]
            kept[l, pl.ds(g * rows_d, rows_d), :] = (
                keep_a[g : g + 1, :] * old + keep_b[g : g + 1, :] * pltpu.roll(old, lanes // 2, 1)
            )
        proj[...] = lax.dot_general(kept[l], read[l], NT, precision=HIGHEST, preferred_element_type=F32)
        total = jnp.zeros((rows_d, width), F32)
        for g in range(groups):
            total = jnp.where(lane_group == g, proj[pl.ds(g * rows_d, rows_d), :], total)
        full = lax.dot_general(drive[l], read[l], NT, precision=HIGHEST, preferred_element_type=F32)
        mixer = jnp.where(wide_0 // chans == wide_1 // chans, full, 0.0)
        mixer = mixer + jnp.where(wide_0 == wide_1, skip_ref[l : l + 1, :], 0.0)
        return total, mixer

    def update(l, u):
        for g in range(groups):
            masked[pl.ds(g * rows_d, rows_d), :] = jnp.where(lane_group == g, u, 0.0)
        kept[l] = kept[l] + jnp.dot(masked[...], drive[l], precision=HIGHEST, preferred_element_type=F32)
        for g in range(groups):
            state[l, pl.ds(g, rows_d, stride=groups), :] = kept[l, pl.ds(g * rows_d, rows_d), :]

    pl.semaphore_wait(barrier, per * dp - 1 + 4 + (dp - 1) * per)

    smalls[0].wait()
    for a, b in ring_far_first(dp, per):
        x_copy(lax.rem(me_z + a, dp) * per + lax.rem(me_y + b, per)).start()

    @pl.when(me_z != me_d)
    def _():
        x_copy(me_t).start()

    @pl.when(me_z == me_d)
    def _():
        x_all[me_d * per + me_y] = stream_ref[...]

    smalls[1].wait()
    gain_all[me_d] = jnp.broadcast_to(gain_ref[0:1, :], (rows_t, feats))
    loads[0].wait()
    for k in PLANE_FAR_FIRST:
        if k:
            gain_copy(partner(me_d, k, dp)).start()
            in_copy(partner(me_d, k, dp)).start()
    x_old[me_y] = stream_ref[...]
    for j in ROW_FAR_FIRST:
        if j:
            old_copy(partner(me_y, j, per)).start()
    loads[7].wait()
    loads[8].wait()
    for what in now:
        col_start(what, 1)
    for small in smalls[2:]:
        small.wait()
    from_old[...], mix_w[...] = prepare(0)

    for what in now:
        col_wait(what, 1)
        col_start(what, 2)
    loads[1].wait()
    col_start(0, 1)

    acc = jnp.zeros((rows_d, width), F32)
    squares = jnp.zeros((rows_d, feats), F32)
    for k in reversed(PLANE_FAR_FIRST):
        by = partner(me_d, k, dp, True)
        if k:
            arrival(x_all.at[pl.ds(0, per)], x_rs.at[by]).wait_recv()
        else:

            @pl.when(me_z != me_d)
            def _():
                arrival(x_all.at[pl.ds(0, per)], x_rs.at[by]).wait_recv()

            @pl.when(me_z == me_d)
            def _():
                arrival(x_all.at[pl.ds(0, per - 1)], x_rs.at[by]).wait_recv()

            arrival(gain_all.at[pl.ds(0, dp - 1)], gain_rs).wait_recv()
            arrival(near_in.at[pl.ds(0, dp - 1)], in_rs).wait_recv()
        weights = near_in.at[by] if k else own_w
        x = x_all[pl.ds(by * per, per)].astype(F32)
        normed = (x * gain_all[by][None]).astype(BF16).reshape(rows_d, feats)
        x = x.reshape(rows_d, feats)
        squares = squares + x * x
        acc = acc + lax.dot_general(normed, weights[...], NT, preferred_element_type=F32)
    u = lax.rsqrt(jnp.sum(squares, axis=1, keepdims=True) / (feats * dp) + EPS) * acc
    u_keep[...] = u
    pre = from_old[...] + jnp.dot(u, mix_w[...], precision=HIGHEST, preferred_element_type=F32)
    mix_out[...] = fold(jax.nn.gelu(pre).astype(BF16))
    for k in PLANE_FAR_FIRST[:-1]:
        mix_copy(partner(me_d, k, dp)).start()

    @pl.when(me_z != me_d)
    def _():
        mix_copy(me_d).start()

    @pl.when(me_z == me_d)
    def _():
        mix_all[me_z] = mix_out[...]

    for what in now:
        col_wait(what, 2)
        col_start(what, 4, 3)
    col_wait(0, 1)
    col_start(0, 2)
    loads[9].wait()
    loads[10].wait()
    col_start(1, 1)
    col_start(2, 1)

    def project(blocks, weights, arrive):
        value = jnp.zeros((rows_d, feats), F32)
        gate = jnp.zeros((rows_d, feats), F32)
        for i, (block, held) in enumerate(blocks):
            arrive(i, block)
            mixed = held[block]
            mixed = jnp.concatenate([mixed[:, :width], mixed[:, width:]], axis=0)
            value = value + jnp.dot(mixed, weights[block, 0], preferred_element_type=F32)
            gate = gate + jnp.dot(mixed, weights[block, 1], preferred_element_type=F32)
        return value, gate

    def arrive_now(i, block):
        if i == 5:
            for what in now:
                col_wait(what, 3)
            col_wait(0, 2)
            col_start(0, 4, 3)
        if i:
            arrival(mix_all.at[block], mix_rs.at[block]).wait_recv()
        else:

            @pl.when(me_z != me_d)
            def _():
                arrival(mix_all.at[block], mix_rs.at[block]).wait_recv()

    nearest = [lax.rem(me_z + hop + dp, dp) for hop in (0, 1, -1, 2, -2, 3, -3, 4)]
    value, gate = project([(z, mix_all) for z in nearest], col_now, arrive_now)
    near_recv[me_y, :, :feats] = value.astype(BF16)
    near_recv[me_y, :, feats:] = gate.astype(BF16)
    for j in ROW_FAR_FIRST:
        if j:
            near_copy(partner(me_y, j, per)).start()
    update(0, u_keep[...])
    total, mixer = prepare(1)
    tight = mixer[:, :chans]
    for g in range(1, groups):
        tight = tight + mixer[:, g * chans : (g + 1) * chans]
    blank = jnp.zeros((rows_d, width - width // rows_d * chans), F32)
    swap_send[...] = jnp.concatenate(
        [total] + [tight[i : i + rows_d] for i in range(0, width, rows_d)] + [blank], axis=1
    )

    @pl.when(me_z != me_d)
    def _():
        swap_copy().start()

    @pl.when(me_z == me_d)
    def _():
        swap_recv[...] = swap_send[...]

    for what in (1, 2):
        col_wait(what, 1)
        col_start(what, 2)

    @pl.when(me_z != me_d)
    def _():
        sent(x_all, x_ss)
        sent(mix_all, mix_ss)

    @pl.when(me_z == me_d)
    def _():
        sent(x_all.at[pl.ds(0, tp - 1)], x_ss)
        sent(mix_all.at[pl.ds(0, dp - 1)], mix_ss)

    sent(near_in.at[pl.ds(0, dp - 1)], in_ss)
    sent(gain_all.at[pl.ds(0, dp - 1)], gain_ss)
    sent(x_old.at[pl.ds(0, per - 1)], old_ss)
    sent(col_now.at[pl.ds(0, 7)], col_ss.at[2])
    arrival(x_old.at[pl.ds(0, per - 1)], old_rs).wait_recv()
    arrival(near_recv.at[pl.ds(0, per - 1)], near_rs).wait_recv()
    combined = near_recv[0].astype(F32)
    for y in range(1, per):
        combined = combined + near_recv[y].astype(F32)
    fresh = (
        x_old[...].astype(F32).reshape(rows_d, feats) + combined[:, :feats] * jax.nn.sigmoid(combined[:, feats:])
    ).astype(BF16)

    x_keep[...] = fresh.reshape(per, rows_t, feats)
    x = fresh.astype(F32)
    normed = (x * gain_ref[1:2, :]).astype(BF16)
    squares = jnp.sum(x * x, axis=1, keepdims=True)
    upper = squares.astype(BF16).astype(F32)
    middle = (squares - upper).astype(BF16).astype(F32)
    lower = squares - upper - middle
    tail_lane = lax.broadcasted_iota(jnp.int32, (rows_d, 128 - width), 1)
    tail = jnp.where(tail_lane == 0, upper, jnp.where(tail_lane == 1, middle, jnp.where(tail_lane == 2, lower, 0.0)))
    col_wait(0, 3)
    own = None
    for k in PLANE_FAR_FIRST:
        to = partner(me_d, k, dp)
        product = lax.dot_general(normed, col_in[to], NT, preferred_element_type=F32)
        whole = jnp.concatenate([product, tail], axis=1)
        if k:
            part_send[to] = whole.astype(BF16)
            part_copy(to).start()
        else:
            own = whole
    for what in (1, 2):
        col_wait(what, 2)
        col_start(what, 4, 3)
    sent(near_recv.at[pl.ds(0, per - 1)], near_ss)
    sent(col_in.at[pl.ds(0, 7)], col_ss.at[0])

    @pl.when(me_z != me_d)
    def _():
        swap_copy().wait_send()
        arrival(swap_recv, swap_rs).wait_recv()

    swapped = swap_recv[...]
    tight = jnp.concatenate(
        [swapped[:, width + i * chans : width + (i + 1) * chans] for i in range(width // rows_d)], axis=0
    )
    mixer = jnp.where(wide_0 // chans == wide_1 // chans, jnp.concatenate([tight] * groups, axis=1), 0.0)
    arrival(part_recv.at[pl.ds(0, dp - 1)], part_rs).wait_recv()
    for k in range(1, dp):
        own = own + part_recv[partner(me_d, k, dp)].astype(F32)
    squares = own[:, width : width + 1] + own[:, width + 1 : width + 2] + own[:, width + 2 : width + 3]
    u = lax.rsqrt(squares / (feats * dp) + EPS) * own[:, :width]
    u_send[...] = jnp.concatenate([u, u], axis=1)

    @pl.when(me_z != me_d)
    def _():
        u_copy().start()

    @pl.when(me_z == me_d)
    def _():
        u_recv[...] = u_send[...]

    pre = swapped[:, :width] + jnp.dot(u, mixer, precision=HIGHEST, preferred_element_type=F32)
    mix_far[me_d] = fold(jax.nn.gelu(pre).astype(BF16))
    for k in PLANE_FAR_FIRST:
        if k:
            mf_copy(partner(me_d, k, dp)).start()
    col_wait(1, 3)
    col_wait(2, 3)
    sent(part_send.at[pl.ds(0, dp - 1)], part_ss)
    sent(col_out.at[pl.ds(0, 7)], col_ss.at[1])

    def arrive_far(i, block):
        if i:
            arrival(mix_far.at[block], mix_rs.at[block]).wait_recv()

    value, gate = project(
        [(partner(me_d, k, dp, True), mix_far) for k in reversed(PLANE_FAR_FIRST)], col_out, arrive_far
    )
    out_own[:, :, :feats] = value.reshape(per, rows_t, feats)
    out_own[:, :, feats:] = gate.reshape(per, rows_t, feats)
    out_send[:, :, :feats] = value.astype(BF16).reshape(per, rows_t, feats)
    out_send[:, :, feats:] = gate.astype(BF16).reshape(per, rows_t, feats)
    for j in ROW_FAR_FIRST:
        if j:
            of_copy(partner(me_y, j, per)).start()

    @pl.when(me_z != me_d)
    def _():
        arrival(u_recv, u_rs).wait_recv()

    update(1, u_recv[:, :width])
    combined = out_own[me_y]
    arrival(out_recv.at[pl.ds(0, per - 1)], of_rs).wait_recv()
    for j in range(1, per):
        combined = combined + out_recv[partner(me_y, j, per)].astype(F32)
    out_ref[...] = (
        x_keep[me_y].astype(F32) + combined[:, :feats] * jax.nn.sigmoid(combined[:, feats:])
    ).astype(BF16)

    sent(mix_far.at[pl.ds(0, dp - 1)], mf_ss)
    sent(out_send.at[pl.ds(0, per - 1)], of_ss)

    @pl.when(me_z != me_d)
    def _():
        u_copy().wait_send()


def put(out_ref, states_ref, out_hbm, states_hbm, sems):
    copies = [
        pltpu.make_async_copy(states_ref, states_hbm, sems.at[0]),
        pltpu.make_async_copy(out_ref, out_hbm, sems.at[1]),
    ]
    for copy in copies:
        copy.start()
    for copy in copies:
        copy.wait()


def per_device(
    tp, dp,
    stream, norm_gain, w_input, lam_re, lam_im, log_dt, b_re, b_im, readout_real, readout_imaginary, d_skip,
    w_val, w_gate, state,
):
    layers, feats, width = w_input.shape
    rows_t = stream.shape[0]
    rows_d, groups, lanes = state.shape[1:]
    chans = b_re.shape[-1]
    per = rows_d // rows_t

    turned_in = w_input.swapaxes(1, 2)
    turned_re, turned_im = b_re.swapaxes(2, 3), b_im.swapaxes(2, 3)

    limit = 67043328 - 4 * layers * rows_d * groups * lanes - (256 << 10)
    vmem = pl.BlockSpec(memory_space=pltpu.VMEM)
    hbm = pl.BlockSpec(memory_space=pltpu.HBM)
    one = pltpu.SemaphoreType.DMA
    dma = lambda *shape: one(shape)
    out, states = pl.pallas_call(
        functools.partial(kernel, tp, dp, chans),
        out_shape=(pltpu.VMEM(stream.shape, BF16), pltpu.VMEM((layers, rows_d * groups, lanes), F32)),
        in_specs=[hbm] * 14,
        out_specs=(vmem, vmem),
        scratch_shapes=[
            pltpu.VMEM(stream.shape, BF16),
            pltpu.VMEM(norm_gain.shape, F32),
            pltpu.VMEM(lam_re.shape, F32),
            pltpu.VMEM(lam_im.shape, F32),
            pltpu.VMEM(log_dt.shape, F32),
            pltpu.VMEM(d_skip.shape, F32),
            pltpu.VMEM((width, feats), BF16),
            pltpu.VMEM(turned_re.shape, F32),
            pltpu.VMEM(turned_im.shape, F32),
            pltpu.VMEM(readout_real.shape, F32),
            pltpu.VMEM(readout_imaginary.shape, F32),
            pltpu.VMEM((layers, width, lanes), F32),
            pltpu.VMEM((layers, width, lanes), F32),
            pltpu.VMEM((layers, rows_d * groups, lanes), F32),
            pltpu.VMEM((rows_d * groups, width), F32),
            pltpu.VMEM((rows_d, width), F32),
            pltpu.VMEM((rows_d * groups, width), F32),
            pltpu.VMEM((rows_d, width), F32),
            pltpu.VMEM((width, width), F32),
            pltpu.VMEM((tp, rows_t, feats), BF16),
            pltpu.VMEM((per, rows_t, feats), BF16),
            pltpu.VMEM((dp, width, feats), BF16),
            pltpu.VMEM((rows_d // 2, 2 * width), BF16),
            pltpu.VMEM((dp, rows_d // 2, 2 * width), BF16),
            pltpu.VMEM((per, rows_d, 2 * feats), BF16),
            pltpu.VMEM((per, rows_t, 2 * feats), F32),
            pltpu.VMEM((dp, rows_t, feats), F32),
            pltpu.VMEM((dp, width, feats), BF16),
            pltpu.VMEM((dp, 2, width, feats), BF16),
            pltpu.VMEM((dp, 2, width, feats), BF16),
            pltpu.VMEM((per, rows_t, feats), BF16),
            pltpu.VMEM((dp, rows_d, 128), BF16),
            pltpu.VMEM((dp, rows_d, 128), BF16),
            pltpu.VMEM((rows_d, 2 * width), F32),
            pltpu.VMEM((rows_d, 2 * width), F32),
            pltpu.VMEM((rows_d, 128), F32),
            pltpu.VMEM((rows_d, 128), F32),
            pltpu.VMEM((dp, rows_d // 2, 2 * width), BF16),
            pltpu.VMEM((per, rows_t, 2 * feats), BF16),
            pltpu.VMEM((per, rows_t, 2 * feats), BF16),
            dma(6), dma(11),
            one, dma(dp),
            one, one,
            one, one,
            one, dma(dp),
            one, one,
            one, one,
            dma(3), dma(7, 3),
            one, one,
            one, one,
            one, one,
            one, one, one,
        ],
        compiler_params=pltpu.CompilerParams(collective_id=0, has_side_effects=True, vmem_limit_bytes=limit),
    )(
        stream, norm_gain, turned_in, lam_re, lam_im, log_dt, turned_re, turned_im, readout_real,
        readout_imaginary, d_skip, w_val, w_gate,
        state.reshape(layers, rows_d * groups, lanes),
    )
    out, states = pl.pallas_call(
        put,
        out_shape=(jax.ShapeDtypeStruct(out.shape, BF16), jax.ShapeDtypeStruct(states.shape, F32)),
        in_specs=[vmem, vmem],
        out_specs=(hbm, hbm),
        scratch_shapes=[dma(2)],
        compiler_params=pltpu.CompilerParams(vmem_limit_bytes=1 << 20),
    )(out, states)
    return out, states.reshape(state.shape)


def solution(mesh):
    return jax.shard_map(
        functools.partial(per_device, mesh.shape["tp"], mesh.shape["dp"]),
        mesh=mesh,
        in_specs=(
            P("tp", "dp"),
            P(None, "dp"),
            P(None, "dp", "tp"),
            P(None, "tp", None),
            P(None, "tp", None),
            P(None, "tp"),
            P(None, "tp", None, None),
            P(None, "tp", None, None),
            P(None, "tp", None, None),
            P(None, "tp", None, None),
            P(None, "tp"),
            P(None, "tp", "dp"),
            P(None, "tp", "dp"),
            P(None, "dp", "tp", None),
        ),
        out_specs=(P("tp", "dp"), P(None, "dp", "tp", None)),
        check_vma=False,
    )
```
